32 devices in a mesh: sp: 16 (over z, y, x), tp: 2 (over core).
Axes of the slice: x: 2, y: 2, z: 4, core: 2. Of those that a mesh axis runs over, the one named last changes fastest.
Arguments:
- queries: bfloat16 [4096, 1024], P('sp', 'tp'), may hold values from -6 to 6
- keys: bfloat16 [4096, 512], P('sp', 'tp'), may hold values from -6 to 6
- values: bfloat16 [4096, 512], P('sp', 'tp'), may hold values from -6 to 6
- q_gain: float32 [64], replicated, may hold values from 1.6 to 4.5
- key_norm_gain: float32 [64], replicated, may hold values from 1.6 to 4.5
- out_weight: bfloat16 [1024, 2048], P('tp'), may hold values from -0.1875 to 0.1875
- residual: bfloat16 [4096, 2048], P('sp'), may hold values from -6 to 6
- ln1_gain: float32 [2048], replicated, may hold values from 0.1 to 1.9
- ln1_bias: float32 [2048], replicated, may hold values from -3 to 3
- up_weight: bfloat16 [2048, 8192], P('sp', 'tp'), may hold values from -0.125 to 0.125
- down_weight: bfloat16 [8192, 2048], P('tp', 'sp'), may hold values from -0.0625 to 0.0625
- ln2_gain: float32 [2048], replicated, may hold values from 0.1 to 1.9
- ln2_bias: float32 [2048], replicated, may hold values from -3 to 3
Outputs:
- encoded: bfloat16 [4096, 2048], P('sp', 'tp')
The draws below stay inside these ranges and needn't reach their ends.
All inputs are finite; a program needn't handle non-finite values.
Results may differ from the reference program's by a relative error of at most 0.014.
Values may be sent and summed in bfloat16 or wider, within the bound.
A program may use at most 128 MiB of HBM per device.

```python
import math
import jax
import jax.numpy as jnp
from jax import lax

D = 2048
FF = 8192
QUERY_HEADS = 16
KEY_VALUE_HEADS = 8
HEAD_SIZE = 64
GRID_W = 64
SEQUENCE_TOKENS = 4096
N_TP = 2


def random_base_keys(key):
    return jnp.clip(jax.random.normal(jax.random.fold_in(key, 11), (SEQUENCE_TOKENS, KEY_VALUE_HEADS * HEAD_SIZE), jnp.float32), -6.0, 6.0)


def draw_keys(key, part):
    return random_base_keys(key).astype(jnp.bfloat16)


def draw_queries(key, part):
    drawn_q = jnp.clip(jax.random.normal(jax.random.fold_in(key, 12), (SEQUENCE_TOKENS, QUERY_HEADS * HEAD_SIZE), jnp.float32), -6.0, 6.0)
    return drawn_q.astype(jnp.bfloat16)


def draw_q_gain(key, part):
    return jax.random.uniform(jax.random.fold_in(key, 21), (HEAD_SIZE,), jnp.float32, 1.6, 2.4)


def draw_key_norm_gain(key, part):
    return jax.random.uniform(jax.random.fold_in(key, 22), (HEAD_SIZE,), jnp.float32, 1.6, 2.4)


def block_levels(rng, extent, cuts, least, high):
    level, own = 1.0, jax.random.fold_in(rng, 6)
    for dim, blocks in cuts:
        heights = jnp.exp(jax.random.uniform(jax.random.fold_in(own, dim), (blocks,), jnp.float32, least / len(cuts), high / len(cuts)))
        level = level * jnp.repeat(heights, extent[dim] // blocks).reshape([-1 if axis == dim else 1 for axis in range(len(extent))])
    return level


def gaussian(key, extent, scale, limit, shards=(), kind=jnp.bfloat16):
    values = jax.random.normal(key, extent, jnp.float32) * scale
    if len(shards) > 0:
        values = block_levels(key, extent, shards, -0.22, 0.18) * values
    return jnp.clip(values, min=-limit, max=limit).astype(kind)


def setup_inputs(seed: int = 0) -> dict:
    key_list = jax.random.split(jax.random.key(seed), 14)
    return {
        "queries": draw_queries(jax.random.fold_in(key_list[13], 71), 0),
        "keys": draw_keys(jax.random.fold_in(key_list[13], 71), 0),
        "values": gaussian(key_list[2], (SEQUENCE_TOKENS, KEY_VALUE_HEADS * HEAD_SIZE), 1.0, 6.0, ((0, 16), (1, 2))),
        "q_gain": draw_q_gain(jax.random.fold_in(key_list[13], 71), 0),
        "key_norm_gain": draw_key_norm_gain(jax.random.fold_in(key_list[13], 71), 0),
        "out_weight": gaussian(key_list[5], (QUERY_HEADS * HEAD_SIZE, D), (QUERY_HEADS * HEAD_SIZE) ** -0.5, 0.1875, ((0, 2),)),
        "residual": gaussian(key_list[6], (SEQUENCE_TOKENS, D), 1.0, 6.0, ((0, 16),)),
        "ln1_gain": jnp.clip(1.0 + 0.18 * jax.random.normal(key_list[7], (D,), jnp.float32), 0.1, 1.9),
        "ln1_bias": gaussian(key_list[8], (D,), 0.3, 3.0, (), jnp.float32),
        "up_weight": gaussian(key_list[9], (D, FF), D ** -0.5, 0.125, ((0, 16), (1, 2))),
        "down_weight": gaussian(key_list[10], (FF, D), FF ** -0.5, 0.0625, ((0, 2), (1, 16))),
        "ln2_gain": jnp.clip(1.0 + 0.18 * jax.random.normal(key_list[11], (D,), jnp.float32), 0.1, 1.9),
        "ln2_bias": gaussian(key_list[12], (D,), 0.3, 3.0, (), jnp.float32),
    }


ALPHA = 8.0 ** 0.25
ROTARY_BASE = 10000.0
RMS_EPSILON = 1e-06
NORM_EPSILON = 1e-05

def rotate_grid(heads_in, grid_places):
    half_dim = heads_in.shape[-1] // 2
    quarter = half_dim // 2
    inverse = ROTARY_BASE ** (-jnp.arange(quarter, dtype=jnp.float32) / quarter)

    def spin(segment, coords):
        angles = coords.astype(jnp.float32)[:, None] * inverse[None, :]
        cos_val = jnp.cos(angles)[:, None, :]
        sin_val = jnp.sin(angles)[:, None, :]
        lead_half = segment[..., :quarter]
        tail_half = segment[..., quarter:]
        return jnp.concatenate([lead_half * cos_val - tail_half * sin_val, tail_half * cos_val + lead_half * sin_val], -1)
    return jnp.concatenate([spin(heads_in[..., :half_dim], grid_places // GRID_W), spin(heads_in[..., half_dim:], grid_places % GRID_W)], -1)

def prepare_inputs(heads_in, gain_vec, grid_places, factor):
    values32 = heads_in.astype(jnp.float32)
    normed = values32 * lax.rsqrt(lax.optimization_barrier(jnp.mean(values32 * values32, -1, keepdims=True)) + RMS_EPSILON) * gain_vec
    return (rotate_grid(normed, grid_places) * factor).astype(jnp.bfloat16)

def layer_norm(pre_norm, gain_vec, bias_vec):
    row_mean = lax.optimization_barrier(jnp.mean(pre_norm, -1, keepdims=True))
    centred = pre_norm - row_mean
    spread = lax.optimization_barrier(jnp.mean(centred * centred, -1, keepdims=True))
    return centred * lax.rsqrt(spread + NORM_EPSILON) * gain_vec + bias_vec

def sum_partials(left_side, right_side):
    group_width = left_side.shape[1] // N_TP
    totals = jnp.zeros((left_side.shape[0], right_side.shape[1]), jnp.float32)
    for member in range(N_TP):
        partial_value = jnp.dot(left_side[:, member * group_width:(member + 1) * group_width], right_side[member * group_width:(member + 1) * group_width], preferred_element_type=jnp.float32)
        totals = totals + lax.optimization_barrier(partial_value.astype(jnp.bfloat16)).astype(jnp.float32)
    return totals

def reference(queries, keys, values, q_gain, key_norm_gain, out_weight, residual, ln1_gain, ln1_bias, up_weight, down_weight, ln2_gain, ln2_bias):
    sequence_length = queries.shape[0]
    grid_places = jnp.arange(sequence_length, dtype=jnp.int32)
    group_count_size = QUERY_HEADS // KEY_VALUE_HEADS
    single_query_block = math.gcd(sequence_length, 128)
    query_head_rows = prepare_inputs(queries.reshape(sequence_length, QUERY_HEADS, HEAD_SIZE), q_gain, grid_places, HEAD_SIZE ** (-0.5))
    key_head_rows = prepare_inputs(keys.reshape(sequence_length, KEY_VALUE_HEADS, HEAD_SIZE), key_norm_gain, grid_places, 1.0).astype(jnp.float32)
    value_head_rows = values.reshape(sequence_length, KEY_VALUE_HEADS, HEAD_SIZE).astype(jnp.float32)
    query_block_list = query_head_rows.reshape(sequence_length // single_query_block, single_query_block, KEY_VALUE_HEADS, group_count_size, HEAD_SIZE)

    def attend(q_block):
        scores = jnp.einsum('qhgd,khd->hgqk', q_block.astype(jnp.float32), key_head_rows)
        maxima = lax.optimization_barrier(jnp.max(scores, -1, keepdims=True))
        weights = jnp.exp(scores - maxima)
        totals = lax.optimization_barrier(jnp.sum(weights, -1))
        rounded = lax.optimization_barrier(weights.astype(jnp.bfloat16)).astype(jnp.float32)
        summed = jnp.einsum('hgqk,khd->qhgd', rounded, value_head_rows)
        return summed / jnp.transpose(totals, (2, 0, 1))[..., None]
    attended = lax.map(attend, query_block_list).reshape(sequence_length, QUERY_HEADS * HEAD_SIZE).astype(jnp.bfloat16)
    mixed_sum = sum_partials(attended, out_weight)
    normed = layer_norm(ALPHA * residual.astype(jnp.float32) + mixed_sum, ln1_gain, ln1_bias).astype(jnp.bfloat16)
    up_acts = jnp.dot(normed, up_weight, preferred_element_type=jnp.float32)
    hidden = jnp.square(jnp.maximum(up_acts, 0.0)).astype(jnp.bfloat16)
    ffn_out = sum_partials(hidden, down_weight)
    return layer_norm(ALPHA * normed.astype(jnp.float32) + ffn_out, ln2_gain, ln2_bias).astype(jnp.bfloat16)
```

```python
import functools
import math

import jax
import jax.numpy as jnp
from jax import lax
from jax.experimental import pallas as pl
from jax.experimental.pallas import tpu as pltpu
from jax.sharding import Mesh, PartitionSpec as P

D = 2048
HEAD_SIZE = 64
GRID_W = 64


ALPHA = 8.0**0.25
ROTARY_BASE = 10000.0
RMS_EPSILON = 1e-06
NORM_EPSILON = 1e-05


def rotate_grid(heads_in, grid_places):
    half_dim = heads_in.shape[-1] // 2
    quarter = half_dim // 2
    inverse = ROTARY_BASE ** (-jnp.arange(quarter, dtype=jnp.float32) / quarter)

    def spin(segment, coords):
        angles = coords.astype(jnp.float32)[:, None] * inverse[None, :]
        cos_val = jnp.cos(angles)[:, None, :]
        sin_val = jnp.sin(angles)[:, None, :]
        lead_half = segment[..., :quarter]
        tail_half = segment[..., quarter:]
        return jnp.concatenate(
            [lead_half * cos_val - tail_half * sin_val, tail_half * cos_val + lead_half * sin_val],
            -1,
        )

    return jnp.concatenate(
        [
            spin(heads_in[..., :half_dim], grid_places // GRID_W),
            spin(heads_in[..., half_dim:], grid_places % GRID_W),
        ],
        -1,
    )


def prepare_inputs(heads_in, gain_vec, grid_places, factor):
    values32 = heads_in.astype(jnp.float32)
    normed = (
        values32
        * lax.rsqrt(jnp.mean(values32 * values32, -1, keepdims=True) + RMS_EPSILON)
        * gain_vec
    )
    return (rotate_grid(normed, grid_places) * factor).astype(jnp.bfloat16)


def layer_norm(pre_norm, gain_vec, bias_vec):
    row_mean = jnp.mean(pre_norm, -1, keepdims=True)
    centred = pre_norm - row_mean
    spread = jnp.mean(centred * centred, -1, keepdims=True)
    return centred * lax.rsqrt(spread + NORM_EPSILON) * gain_vec + bias_vec


def line_gather(block, axis):
    n, me = lax.axis_size(axis), lax.axis_index(axis)
    up = [(i, i + 1) for i in range(n - 1)]
    down = [(i + 1, i) for i in range(n - 1)]
    from_left, from_right = [block], [block]
    for _ in range(n - 1):
        from_left.append(lax.ppermute(from_left[-1], axis, up))
        from_right.append(lax.ppermute(from_right[-1], axis, down))
    stacked = jnp.zeros((n, *block.shape), block.dtype)
    for k in range(n):
        piece = block if k == 0 else jnp.where(me >= k, from_left[k], from_right[n - k])
        stacked = lax.dynamic_update_index_in_dim(stacked, piece, (me - k + n) % n, 0)
    return stacked


def swap_blocks(blocks, axis):
    n, me = lax.axis_size(axis), lax.axis_index(axis)
    stacked = jnp.zeros_like(blocks)
    for k in range(n):
        piece = lax.dynamic_index_in_dim(blocks, (me + k) % n, 0, keepdims=False)
        if k:
            piece = lax.ppermute(piece, axis, [(i, (i + k) % n) for i in range(n)])
        stacked = lax.dynamic_update_index_in_dim(stacked, piece, (me - k + n) % n, 0)
    return stacked


def turn_cols(block, outer, inner):
    width = block.shape[1] // (outer * inner)
    starts = [(o * inner + i) * width for i in range(inner) for o in range(outer)]
    return jnp.concatenate([block[:, c : c + width] for c in starts], -1)


def attend_kernel(chunk, q_ref, kv_ref, out_ref, vals_ref):
    width = 2 * HEAD_SIZE
    key_count = kv_ref.shape[0]
    rows = q_ref.shape[0]

    @pl.when(pl.program_id(1) == 0)
    def _():
        lane_kv = lax.broadcasted_iota(jnp.int32, (chunk, width), 1)

        @pl.loop(0, key_count // chunk)
        def _(c):
            at = pl.ds(pl.multiple_of(c * chunk, chunk), chunk)
            vals_ref[at, :] = jnp.where(
                lane_kv < HEAD_SIZE, 1.0, kv_ref[at, :].astype(jnp.float32)
            ).astype(jnp.bfloat16)

    lane = lax.broadcasted_iota(jnp.int32, (rows, width), 1)
    both = q_ref[...].astype(jnp.float32)
    results = []
    for head in range(2):
        own = both if head == 0 else pltpu.roll(both, HEAD_SIZE, 1)
        q = jnp.where(lane < HEAD_SIZE, own, 0.0).astype(jnp.bfloat16)
        top = None
        for c in range(key_count // chunk):
            at = pl.ds(c * chunk, chunk)
            scores = lax.dot_general(
                q, kv_ref[at, :], (((1,), (1,)), ((), ())), preferred_element_type=jnp.float32
            )
            peak = jnp.max(scores, -1, keepdims=True)
            new_top = peak if top is None else jnp.maximum(top, peak)
            weights = jnp.exp(scores - new_top).astype(jnp.bfloat16)
            part = jnp.dot(weights, vals_ref[at, :], preferred_element_type=jnp.float32)
            total = part if top is None else total * jnp.exp(top - new_top) + part
            top = new_top
        results.append(total)
    first, second = (t / pltpu.roll(t, HEAD_SIZE, 1) for t in results)
    out_ref[...] = jnp.where(
        lane < HEAD_SIZE, pltpu.roll(first, HEAD_SIZE, 1), second
    ).astype(jnp.bfloat16)


def attend(q, kv, block=256, chunk=2048):
    heads, rows, width = q.shape
    key_count = kv.shape[1]
    block, chunk = math.gcd(rows, block), math.gcd(key_count, chunk)
    return pl.pallas_call(
        functools.partial(attend_kernel, chunk),
        grid=(heads, rows // block),
        in_specs=[
            pl.BlockSpec((None, block, width), lambda h, i: (h, i, 0)),
            pl.BlockSpec((None, key_count, width), lambda h, i: (h, 0, 0)),
        ],
        out_specs=pl.BlockSpec((None, block, width), lambda h, i: (h, i, 0)),
        out_shape=jax.ShapeDtypeStruct(q.shape, jnp.bfloat16),
        scratch_shapes=[pltpu.VMEM((key_count, width), jnp.bfloat16)],
        compiler_params=pltpu.CompilerParams(dimension_semantics=("arbitrary", "arbitrary")),
        cost_estimate=pl.CostEstimate(
            flops=heads * rows * key_count * 16 * HEAD_SIZE,
            bytes_accessed=2 * (2 * q.size + kv.size),
            transcendentals=heads * rows * key_count * 2,
        ),
    )(q, kv)


def local(
    queries,
    keys,
    values,
    q_gain,
    key_norm_gain,
    out_weight,
    residual,
    ln1_gain,
    ln1_bias,
    up_weight,
    down_weight,
    ln2_gain,
    ln2_bias,
):
    tok_rows = queries.shape[0]
    n_a, n_tp = lax.axis_size("a"), lax.axis_size("tp")
    grid_places = lax.axis_index(("a", "w")) * tok_rows + jnp.arange(tok_rows, dtype=jnp.int32)
    kv_heads = keys.shape[1] // HEAD_SIZE
    q_count = queries.shape[1] // HEAD_SIZE
    own_heads = kv_heads // n_a
    query_rows = prepare_inputs(
        queries.reshape(tok_rows, q_count, HEAD_SIZE), q_gain, grid_places, HEAD_SIZE ** (-0.5)
    ).reshape(tok_rows, kv_heads, 2 * HEAD_SIZE)
    key_rows = prepare_inputs(
        keys.reshape(tok_rows, kv_heads, HEAD_SIZE), key_norm_gain, grid_places, 1.0
    )
    value_rows = values.reshape(tok_rows, kv_heads, HEAD_SIZE)
    packed = jnp.concatenate([query_rows, key_rows, value_rows], -1)
    packed = jnp.transpose(packed, (1, 0, 2)).reshape(n_a, own_heads, tok_rows, 4 * HEAD_SIZE)
    packed = lax.all_to_all(packed, "a", 0, 0, tiled=True)
    packed = jnp.transpose(packed, (1, 0, 2, 3)).reshape(
        own_heads, n_a * tok_rows, 4 * HEAD_SIZE
    )
    q = packed[..., : 2 * HEAD_SIZE]
    kv = lax.all_gather(packed[..., 2 * HEAD_SIZE :], "w", axis=1, tiled=True)
    kv, down_weight = lax.optimization_barrier((kv, down_weight))

    out_full = line_gather(out_weight, "tp").reshape(-1, D)
    up_own = lax.all_to_all(up_weight, "a", 1, 0, tiled=True)
    up_full = lax.all_gather(up_own, "w", axis=0, tiled=True)
    down_own = swap_blocks(down_weight.reshape(n_a, -1, down_weight.shape[1]), "a")
    down_own = down_own.swapaxes(0, 1).reshape(down_weight.shape[0] // n_a, -1)

    attended = attend(q, kv)
    rows = tok_rows // n_tp
    sent = attended.reshape(own_heads, n_a * n_tp, rows, 2 * HEAD_SIZE)
    sent = jnp.transpose(sent, (1, 0, 2, 3))
    got = lax.all_to_all(sent, ("a", "tp"), 0, 0, tiled=True)
    got, down_own = lax.optimization_barrier((got, down_own))
    down_full = lax.all_gather(down_own, "w", axis=0)
    got = got.reshape(n_a, n_tp, own_heads, rows, 2 * HEAD_SIZE)
    group_cols = jnp.transpose(got, (1, 3, 0, 2, 4)).reshape(n_tp, rows, -1)
    out_groups = out_full.reshape(2, -1, D)
    both = jnp.transpose(group_cols, (1, 0, 2)).reshape(rows, 2, -1)
    mixed = sum(
        jnp.dot(both[:, g], out_groups[g], preferred_element_type=jnp.float32)
        .astype(jnp.bfloat16)
        .astype(jnp.float32)
        for g in range(2)
    )
    own_residual = lax.dynamic_slice_in_dim(residual, lax.axis_index("tp") * rows, rows, 0)
    normed = layer_norm(
        ALPHA * own_residual.astype(jnp.float32) + mixed, ln1_gain, ln1_bias
    ).astype(jnp.bfloat16)
    n_w = lax.axis_size("w")
    turned = turn_cols(normed, n_a, n_w)
    full_rows = line_gather(line_gather(turned, "a"), "tp").reshape(-1, D)
    up_acts = jnp.dot(full_rows, up_full, preferred_element_type=jnp.float32)
    hidden = jnp.square(jnp.maximum(up_acts, 0.0)).astype(jnp.bfloat16)
    partial_ffn = jnp.concatenate(
        [
            jnp.dot(hidden, down_full[i], preferred_element_type=jnp.float32).astype(jnp.bfloat16)
            for i in range(down_full.shape[0])
        ],
        -1,
    )
    ffn_out = lax.psum_scatter(partial_ffn, "tp", scatter_dimension=0, tiled=True)
    ffn_out = lax.psum_scatter(ffn_out, "a", scatter_dimension=0, tiled=True)
    ffn_out = (
        ffn_out.reshape(rows, n_w, n_a, -1).swapaxes(1, 2).reshape(rows, D).astype(jnp.float32)
    )
    encoded = layer_norm(
        ALPHA * normed.astype(jnp.float32) + ffn_out, ln2_gain, ln2_bias
    ).astype(jnp.bfloat16)
    return lax.all_to_all(encoded, "tp", 1, 0, tiled=True)


MESH = pl.DeviceIdType.MESH
BF16, F32 = jnp.bfloat16, jnp.float32


def scaled(index, size):
    return pl.ds(pl.multiple_of(index * size, size), size)


def layer_kernel(
    n_a,
    n_w,
    packed,
    up_own,
    down_own,
    out_own,
    res_all,
    gain1,
    bias1,
    gain2,
    bias2,
    out,
    qkv,
    kv,
    vals,
    att_out,
    att_in,
    out_full,
    res,
    mixed,
    up,
    down,
    toks,
    hid,
    part,
    sib_out,
    sib_in,
    rs_out,
    rs_in,
    enc_out,
    loc_sem,
    qkv_s,
    qkv_r,
    kv_s,
    kv_r,
    att_s,
    att_r,
    wz_s,
    wz_r,
    wf_s,
    wf_r,
    wd_s,
    wd_r,
    tz_s,
    tz_r,
    pair_s,
    pair_r,
    sib_s,
    sib_r,
    rs_s,
    rs_r,
):
    place, core = lax.axis_index("sp"), lax.axis_index("tp")
    a, w = place // n_w, place % n_w
    other = 1 - core
    x_side = w + 1 - 2 * (w % 2)
    y_side = w + 2 - 4 * (w // 2)
    sides = (x_side, y_side)
    rows = toks.shape[2]
    tok_rows = 2 * rows
    width = 2 * HEAD_SIZE
    up_rows, up_cols = up_own.shape[0], up.shape[1]
    down_rows, down_cols = down.shape[0], down_own.shape[1]

    def at(a_, w_, core_):
        return (a_ * n_w + w_, core_)

    sibling = at(a, w, other)

    def remote(src, dst, send, recv, target):
        return pltpu.make_async_remote_copy(
            src_ref=src,
            dst_ref=dst,
            send_sem=send,
            recv_sem=recv,
            device_id=target,
            device_id_type=MESH,
        )

    def landed(dst, recv, send):
        remote(dst, dst, send, recv, sibling).wait_recv()

    def sent(src, send, recv):
        remote(src, src, send, recv, sibling).wait_send()

    def cyc(k):
        return lax.rem(a + k + 2 * n_a, n_a)

    def w_slot(kind, a_, w_):
        if kind == 0:
            return up.at[scaled(a_ * n_w + w_, up_rows), :]
        return down.at[:, scaled(a_ * n_w + w_, down_cols)]

    def w_half(kind, a_, w_, h):
        if kind == 0:
            half = up_rows // 2
            return up.at[scaled((a_ * n_w + w_) * 2 + h, half), :]
        half = down_rows // 2
        return down.at[pl.ds(h * half, half), scaled(a_ * n_w + w_, down_cols)]

    def w_src(kind, a_):
        if kind == 0:
            return up_own.at[:, scaled(a_, up_cols)]
        return down_own.at[scaled(a_, down_rows), :]

    def w_exchange(kind):
        for k in range(1, n_a):
            to = cyc(k)
            remote(
                w_src(kind, to),
                w_slot(kind, a, w),
                wz_s.at[kind, to],
                wz_r.at[kind, a],
                at(to, w, core),
            ).start()

    def w_forward(kind, frm):
        for j in range(2):
            remote(
                w_slot(kind, frm, w),
                w_slot(kind, frm, w),
                wf_s.at[kind, frm, j],
                wf_r.at[kind, frm, j],
                at(a, sides[j], core),
            ).start()

    def w_arrive(kind, frm):
        landed(w_slot(kind, frm, w), wz_r.at[kind, frm], wz_s.at[kind, frm])

    def w_corner(kind, frm):
        for j in range(2):
            landed(w_slot(kind, frm, sides[j]), wf_r.at[kind, frm, j], wf_s.at[kind, frm, j])
            part_ref = w_half(kind, frm, sides[j], j)
            remote(
                part_ref,
                part_ref,
                wd_s.at[kind, frm, j],
                wd_r.at[kind, frm, j],
                at(a, sides[1 - j], core),
            ).start()

    def w_complete(kind):
        for k in range(n_a):
            frm = cyc(-k)
            for j in range(2):
                landed(
                    w_half(kind, frm, n_w - 1 - w, j),
                    wd_r.at[kind, frm, j],
                    wd_s.at[kind, frm, j],
                )

    def w_drain(kind):
        for k in range(1, n_a):
            to = cyc(k)
            sent(w_src(kind, to), wz_s.at[kind, to], wz_r.at[kind, to])
        for k in range(n_a):
            frm = cyc(-k)
            for j in range(2):
                sent(w_slot(kind, frm, w), wf_s.at[kind, frm, j], wf_r.at[kind, frm, j])
                sent(w_half(kind, frm, sides[j], j), wd_s.at[kind, frm, j], wd_r.at[kind, frm, j])

    local_copies = [
        pltpu.make_async_copy(up_own.at[:, scaled(a, up_cols)], w_slot(0, a, w), loc_sem.at[0]),
        pltpu.make_async_copy(
            down_own.at[scaled(a, down_rows), :], w_slot(1, a, w), loc_sem.at[1]
        ),
        pltpu.make_async_copy(out_own, out_full.at[core], loc_sem.at[2]),
        pltpu.make_async_copy(res_all.at[scaled(core, rows), :], res, loc_sem.at[3]),
    ]
    for copy in local_copies:
        copy.start()

    barrier = pltpu.get_barrier_semaphore()
    peers = [at(cyc(k), w, core_) for k in range(n_a) for core_ in (core, other)][1:]
    peers += [at(a, side, core) for side in (x_side, y_side, n_w - 1 - w)]
    for peer in peers:
        pl.semaphore_signal(barrier, inc=1, device_id=peer, device_id_type=MESH)
    pl.semaphore_wait(barrier, len(peers))

    for k in range(1, n_a):
        to = cyc(k)
        remote(packed.at[to], qkv.at[a], qkv_s.at[to], qkv_r.at[a], at(to, w, core)).start()
    local_copies[0].wait()
    w_forward(0, a)
    w_exchange(0)
    remote(out_own, out_full.at[core], pair_s.at[0], pair_r.at[0], sibling).start()
    qkv[a] = packed[a]

    w_peers = (x_side, y_side, n_w - 1 - w)

    def kv_slot(w_, a_):
        return kv.at[w_ * n_a + a_]

    for k in range(n_a):
        frm = cyc(-k)
        if k:
            landed(qkv.at[frm], qkv_r.at[frm], qkv_s.at[frm])
        kv[w * n_a + frm] = qkv[frm, :, width:]
        for j, peer in enumerate(w_peers):
            remote(
                qkv.at[frm, :, pl.ds(width, width)],
                kv_slot(w, frm),
                kv_s.at[j, frm],
                kv_r.at[j, frm],
                at(a, peer, core),
            ).start()
    for k in range(n_a):
        for j, peer in enumerate(w_peers):
            frm = cyc(-k)
            landed(kv_slot(peer, frm), kv_r.at[j, frm], kv_s.at[j, frm])

    slots = n_w * n_a
    lane_kv = lax.broadcasted_iota(jnp.int32, (tok_rows, width), 1)

    @pl.loop(0, slots)
    def _(i):
        vals[i] = jnp.where(lane_kv < HEAD_SIZE, 1.0, kv[i].astype(F32)).astype(BF16)

    lane = lax.broadcasted_iota(jnp.int32, (tok_rows, width), 1)
    chunks = 2
    per = slots // chunks

    @pl.loop(0, n_a)
    def _(i):
        block = cyc(1 + i)
        both = qkv[block, :, :width].astype(F32)
        results = []
        for head in range(2):
            own = both if head == 0 else pltpu.roll(both, HEAD_SIZE, 1)
            q = jnp.where(lane < HEAD_SIZE, own, 0.0).astype(BF16)
            top = None
            for c in range(chunks):
                keys = kv[pl.ds(c * per, per)].reshape(per * tok_rows, width)
                scores = lax.dot_general(
                    q, keys, (((1,), (1,)), ((), ())), preferred_element_type=F32
                )
                peak = jnp.max(scores, -1, keepdims=True)
                new_top = peak if top is None else jnp.maximum(top, peak)
                weights = jnp.exp(scores - new_top).astype(BF16)
                held = vals[pl.ds(c * per, per)].reshape(per * tok_rows, width)
                add = jnp.dot(weights, held, preferred_element_type=F32)
                total = add if top is None else total * jnp.exp(top - new_top) + add
                top = new_top
            results.append(total)
        first, second = (t / pltpu.roll(t, HEAD_SIZE, 1) for t in results)
        att_out[block] = jnp.where(
            lane < HEAD_SIZE, pltpu.roll(first, HEAD_SIZE, 1), second
        ).astype(BF16)
        mine = core * n_a + a
        remote(
            att_out.at[block, scaled(other, rows), :],
            att_in.at[mine],
            att_s.at[block, 0],
            att_r.at[mine],
            at(block, w, other),
        ).start()

        @pl.when(i < n_a - 1)
        def _():
            remote(
                att_out.at[block, scaled(core, rows), :],
                att_in.at[mine],
                att_s.at[block, 1],
                att_r.at[mine],
                at(block, w, core),
            ).start()
            frm = cyc(-1 - i)
            w_arrive(0, frm)
            w_forward(0, frm)

    att_in[core * n_a + a] = att_out[a, scaled(core, rows), :]
    w_exchange(1)
    local_copies[1].wait()
    w_forward(1, a)
    local_copies[2].wait()
    local_copies[3].wait()
    landed(out_full.at[other], pair_r.at[0], pair_s.at[0])
    for core_ in (core, other):
        for k in range(n_a):
            frm = cyc(-k)
            if k == 0 and core_ is core:
                continue
            frm_slot = core_ * n_a + frm
            landed(att_in.at[frm_slot], att_r.at[frm_slot], att_s.at[frm, 0])

    tile = 256

    @pl.loop(0, D // tile)
    def _(t):
        cols = scaled(t, tile)
        total = None
        for g in range(2):
            lhs = jnp.concatenate([att_in[g * n_a + k] for k in range(n_a)], -1)
            add = jnp.dot(lhs, out_full[g, :, cols], preferred_element_type=F32)
            add = add.astype(BF16).astype(F32)
            total = add if total is None else total + add
        mixed[:, cols] = total

    step = 16

    @pl.loop(0, rows // step)
    def _(t):
        r = scaled(t, step)
        toks[a, 0, r, :] = layer_norm(
            ALPHA * res[r, :].astype(F32) + mixed[r, :], gain1[...], bias1[...]
        ).astype(BF16)

    def tok_send(b, dest, way):
        remote(
            toks.at[b, 0], toks.at[b, 0], tz_s.at[b, way], tz_r.at[b], at(dest, w, core)
        ).start()

    def tok_pair(b):
        remote(toks.at[b, 0], toks.at[b, 1], pair_s.at[1 + b], pair_r.at[1 + b], sibling).start()

    last = n_a - 1

    @pl.when(a < last)
    def _():
        tok_send(a, a + 1, 0)

    @pl.when(a > 0)
    def _():
        tok_send(a, a - 1, 1)

    tok_pair(a)
    for k in range(n_a):
        w_corner(0, cyc(-k))
    w_complete(0)

    low = jnp.minimum(a, last - a)
    toward = jnp.where(2 * a < n_a, 1, -1)

    def order(k):
        near = a + jnp.where(k % 2 == 1, 1, -1) * ((k + 1) // 2)
        return jnp.where(k <= 2 * low, near, a + toward * (k - low))

    @pl.loop(0, n_a)
    def _(k):
        b = order(k)

        @pl.when(k > 0)
        def _():
            landed(toks.at[b, 0], tz_r.at[b], tz_s.at[b, 0])

            @pl.when((b > a) & (a > 0))
            def _():
                tok_send(b, a - 1, 1)

            @pl.when((b < a) & (a < last))
            def _():
                tok_send(b, a + 1, 0)

            tok_pair(b)
            frm = cyc(-k)
            w_arrive(1, frm)
            w_forward(1, frm)
            w_corner(1, cyc(1 - k))

        landed(toks.at[b, 1], pair_r.at[1 + b], pair_s.at[1 + b])

        @pl.loop(0, up_cols // tile)
        def _(t):
            cols = scaled(t, tile)
            acts = jnp.dot(
                toks[b].reshape(tok_rows, D), up[:, cols], preferred_element_type=F32
            )
            hid[b, :, cols] = jnp.square(jnp.maximum(acts, 0.0)).astype(BF16)

    w_corner(1, cyc(1 - n_a))
    w_complete(1)

    @pl.loop(0, n_a + 1)
    def _(i):
        @pl.when(i < n_a)
        def _():
            b = cyc(1 + i)

            @pl.loop(0, D // tile)
            def _(t):
                cols = scaled(t, tile)
                acts = jnp.dot(hid[b], down[:, cols], preferred_element_type=F32)
                part[b, :, cols] = acts[:rows]
                sib_out[b, :, cols] = acts[rows:].astype(BF16)

            remote(sib_out.at[b], sib_in.at[b], sib_s.at[b], sib_r.at[b], sibling).start()

        @pl.when(i > 0)
        def _():
            b = cyc(i)
            landed(sib_in.at[b], sib_r.at[b], sib_s.at[b])

            @pl.when(b != a)
            def _():
                @pl.loop(0, rows // step)
                def _(t):
                    r = scaled(t, step)
                    rs_out[b, r, :] = (part[b, r, :] + sib_in[b, r, :].astype(F32)).astype(BF16)

                remote(
                    rs_out.at[b], rs_in.at[a], rs_s.at[b], rs_r.at[a], at(b, w, core)
                ).start()

    for k in range(1, n_a):
        frm = cyc(-k)
        landed(rs_in.at[frm], rs_r.at[frm], rs_s.at[frm])

    half = D // 2

    @pl.loop(0, rows // step)
    def _(t):
        r = scaled(t, step)
        total = part[a, r, :] + sib_in[a, r, :].astype(F32)
        for k in range(1, n_a):
            total = total + rs_in[cyc(-k), r, :].astype(F32)
        encoded = layer_norm(
            ALPHA * toks[a, 0, r, :].astype(F32) + total, gain2[...], bias2[...]
        )
        left, right = encoded[:, :half].astype(BF16), encoded[:, half:].astype(BF16)
        out[pl.ds(pl.multiple_of(core * rows + t * step, step), step), :] = jnp.where(
            core == 0, left, right
        )
        enc_out[r, :] = jnp.where(core == 0, right, left)

    swap = remote(enc_out, out.at[scaled(core, rows), :], pair_s.at[n_a + 1], pair_r.at[n_a + 1], sibling)
    swap.start()
    for k in range(1, n_a):
        to = cyc(k)
        sent(packed.at[to], qkv_s.at[to], qkv_r.at[to])
    for k in range(n_a):
        for j in range(3):
            sent(kv_slot(w, k), kv_s.at[j, k], kv_r.at[j, k])
    sent(out_own, pair_s.at[0], pair_r.at[0])
    for kind in range(2):
        w_drain(kind)
    for k in range(n_a):
        b = cyc(k)
        sent(att_out.at[b, pl.ds(0, rows), :], att_s.at[b, 0], att_r.at[b])
        if k:
            sent(att_out.at[b, pl.ds(0, rows), :], att_s.at[b, 1], att_r.at[b])
            sent(rs_out.at[b], rs_s.at[b], rs_r.at[b])
        sent(sib_out.at[b], sib_s.at[b], sib_r.at[b])
        sent(toks.at[b, 0], pair_s.at[1 + b], pair_r.at[1 + b])

        @pl.when((a < last) & (b <= a))
        def _():
            sent(toks.at[b, 0], tz_s.at[b, 0], tz_r.at[b])

        @pl.when((a > 0) & (b >= a))
        def _():
            sent(toks.at[b, 0], tz_s.at[b, 1], tz_r.at[b])

    swap.wait_send()
    landed(out.at[scaled(other, rows), :], pair_r.at[n_a + 1], pair_s.at[n_a + 1])


def fused(n_a, n_w, *args):
    (queries, keys, values, q_gain, key_norm_gain, out_weight, residual, *rest) = args
    ln1_gain, ln1_bias, up_weight, down_weight, ln2_gain, ln2_bias = rest
    tok_rows = queries.shape[0]
    rows = tok_rows // 2
    places = lax.axis_index("sp") * tok_rows + jnp.arange(tok_rows, dtype=jnp.int32)
    heads = keys.shape[1] // HEAD_SIZE
    query_rows = prepare_inputs(
        queries.reshape(tok_rows, 2 * heads, HEAD_SIZE), q_gain, places, HEAD_SIZE ** (-0.5)
    ).reshape(tok_rows, heads, 2 * HEAD_SIZE)
    key_rows = prepare_inputs(
        keys.reshape(tok_rows, heads, HEAD_SIZE), key_norm_gain, places, 1.0
    )
    packed = jnp.concatenate(
        [query_rows, key_rows, values.reshape(tok_rows, heads, HEAD_SIZE)], -1
    )
    packed = jnp.transpose(packed, (1, 0, 2))
    width = 2 * HEAD_SIZE
    up_cols = up_weight.shape[1] // n_a
    down_rows = down_weight.shape[0] // n_a
    dma, vmem = pltpu.SemaphoreType.DMA, pltpu.VMEM
    whole, hbm = pl.BlockSpec(memory_space=pltpu.VMEM), pl.BlockSpec(memory_space=pl.ANY)
    return pl.pallas_call(
        functools.partial(layer_kernel, n_a, n_w),
        out_shape=jax.ShapeDtypeStruct((tok_rows, D // 2), BF16),
        in_specs=[whole] + [hbm] * 4 + [whole] * 4,
        out_specs=whole,
        scratch_shapes=[
            vmem((n_a, tok_rows, 2 * width), BF16),
            vmem((n_w * n_a, tok_rows, width), BF16),
            vmem((n_w * n_a, tok_rows, width), BF16),
            vmem((n_a, tok_rows, width), BF16),
            vmem((2 * n_a, rows, width), BF16),
            vmem((2, *out_weight.shape), BF16),
            vmem((rows, D), BF16),
            vmem((rows, D), F32),
            vmem((D, up_cols), BF16),
            vmem((down_rows, D), BF16),
            vmem((n_a, 2, rows, D), BF16),
            vmem((n_a, tok_rows, up_cols), BF16),
            vmem((n_a, rows, D), F32),
            vmem((n_a, rows, D), BF16),
            vmem((n_a, rows, D), BF16),
            vmem((n_a, rows, D), BF16),
            vmem((n_a, rows, D), BF16),
            vmem((rows, D // 2), BF16),
            dma((4,)),
            dma((n_a,)),
            dma((n_a,)),
            dma((3, n_a)),
            dma((3, n_a)),
            dma((n_a, 2)),
            dma((2 * n_a,)),
            dma((2, n_a)),
            dma((2, n_a)),
            dma((2, n_a, 2)),
            dma((2, n_a, 2)),
            dma((2, n_a, 2)),
            dma((2, n_a, 2)),
            dma((n_a, 2)),
            dma((n_a,)),
            dma((n_a + 2,)),
            dma((n_a + 2,)),
            dma((n_a,)),
            dma((n_a,)),
            dma((n_a,)),
            dma((n_a,)),
        ],
        compiler_params=pltpu.CompilerParams(
            collective_id=0, has_side_effects=True, vmem_limit_bytes=60 * 2**20
        ),
    )(
        packed,
        up_weight,
        down_weight,
        out_weight,
        residual,
        *(v.reshape(1, D) for v in (ln1_gain, ln1_bias, ln2_gain, ln2_bias)),
    )


def solution(mesh):
    n_sp, n_tp = mesh.shape["sp"], mesh.shape["tp"]

    def layer(queries, keys, *others):
        n_a = math.gcd(n_sp, keys.shape[1] // (HEAD_SIZE * n_tp))
        n_w = n_sp // n_a
        sp = ("a", "w")
        if n_tp == 2 and n_w == 4 and n_a * HEAD_SIZE * n_tp == keys.shape[1]:
            cut = P("sp", "tp")
            return jax.shard_map(
                functools.partial(fused, n_a, n_w),
                mesh=mesh,
                in_specs=(cut, cut, cut, P(), P(), P("tp", None), P("sp", None), P(), P())
                + (cut, P("tp", "sp"), P(), P()),
                out_specs=cut,
                check_vma=False,
            )(queries, keys, *others)
        groups = Mesh(mesh.devices.reshape(n_a, n_w, n_tp), ("a", "w", "tp"))
        cut = P(sp, "tp")
        return jax.shard_map(
            local,
            mesh=groups,
            in_specs=(cut, cut, cut, P(), P(), P("tp", None), P(sp, None), P(), P())
            + (cut, P("tp", sp), P(), P()),
            out_specs=cut,
            check_vma=False,
        )(queries, keys, *others)

    return layer
```

```python
import functools
import math

import jax
import jax.numpy as jnp
from jax import lax
from jax.experimental import pallas as pl
from jax.experimental.pallas import tpu as pltpu
from jax.sharding import Mesh, PartitionSpec as P

D = 2048
HEAD_SIZE = 64
GRID_W = 64


ALPHA = 8.0**0.25
ROTARY_BASE = 10000.0
RMS_EPSILON = 1e-06
NORM_EPSILON = 1e-05


def rotate_grid(heads_in, grid_places):
    half_dim = heads_in.shape[-1] // 2
    quarter = half_dim // 2
    inverse = ROTARY_BASE ** (-jnp.arange(quarter, dtype=jnp.float32) / quarter)

    def spin(segment, coords):
        angles = coords.astype(jnp.float32)[:, None] * inverse[None, :]
        cos_val = jnp.cos(angles)[:, None, :]
        sin_val = jnp.sin(angles)[:, None, :]
        lead_half = segment[..., :quarter]
        tail_half = segment[..., quarter:]
        return jnp.concatenate(
            [lead_half * cos_val - tail_half * sin_val, tail_half * cos_val + lead_half * sin_val],
            -1,
        )

    return jnp.concatenate(
        [
            spin(heads_in[..., :half_dim], grid_places // GRID_W),
            spin(heads_in[..., half_dim:], grid_places % GRID_W),
        ],
        -1,
    )


def prepare_inputs(heads_in, gain_vec, grid_places, factor):
    values32 = heads_in.astype(jnp.float32)
    normed = (
        values32
        * lax.rsqrt(jnp.mean(values32 * values32, -1, keepdims=True) + RMS_EPSILON)
        * gain_vec
    )
    return (rotate_grid(normed, grid_places) * factor).astype(jnp.bfloat16)


def layer_norm(pre_norm, gain_vec, bias_vec):
    row_mean = jnp.mean(pre_norm, -1, keepdims=True)
    centred = pre_norm - row_mean
    spread = jnp.mean(centred * centred, -1, keepdims=True)
    return centred * lax.rsqrt(spread + NORM_EPSILON) * gain_vec + bias_vec


def line_gather(block, axis):
    n, me = lax.axis_size(axis), lax.axis_index(axis)
    up = [(i, i + 1) for i in range(n - 1)]
    down = [(i + 1, i) for i in range(n - 1)]
    from_left, from_right = [block], [block]
    for _ in range(n - 1):
        from_left.append(lax.ppermute(from_left[-1], axis, up))
        from_right.append(lax.ppermute(from_right[-1], axis, down))
    stacked = jnp.zeros((n, *block.shape), block.dtype)
    for k in range(n):
        piece = block if k == 0 else jnp.where(me >= k, from_left[k], from_right[n - k])
        stacked = lax.dynamic_update_index_in_dim(stacked, piece, (me - k + n) % n, 0)
    return stacked


def swap_blocks(blocks, axis):
    n, me = lax.axis_size(axis), lax.axis_index(axis)
    stacked = jnp.zeros_like(blocks)
    for k in range(n):
        piece = lax.dynamic_index_in_dim(blocks, (me + k) % n, 0, keepdims=False)
        if k:
            piece = lax.ppermute(piece, axis, [(i, (i + k) % n) for i in range(n)])
        stacked = lax.dynamic_update_index_in_dim(stacked, piece, (me - k + n) % n, 0)
    return stacked


def turn_cols(block, outer, inner):
    width = block.shape[1] // (outer * inner)
    starts = [(o * inner + i) * width for i in range(inner) for o in range(outer)]
    return jnp.concatenate([block[:, c : c + width] for c in starts], -1)


def attend_kernel(chunk, q_ref, kv_ref, out_ref, vals_ref):
    width = 2 * HEAD_SIZE
    key_count = kv_ref.shape[0]
    rows = q_ref.shape[0]

    @pl.when(pl.program_id(1) == 0)
    def _():
        lane_kv = lax.broadcasted_iota(jnp.int32, (chunk, width), 1)

        @pl.loop(0, key_count // chunk)
        def _(c):
            at = pl.ds(pl.multiple_of(c * chunk, chunk), chunk)
            vals_ref[at, :] = jnp.where(
                lane_kv < HEAD_SIZE, 1.0, kv_ref[at, :].astype(jnp.float32)
            ).astype(jnp.bfloat16)

    lane = lax.broadcasted_iota(jnp.int32, (rows, width), 1)
    both = q_ref[...].astype(jnp.float32)
    results = []
    for head in range(2):
        own = both if head == 0 else pltpu.roll(both, HEAD_SIZE, 1)
        q = jnp.where(lane < HEAD_SIZE, own, 0.0).astype(jnp.bfloat16)
        top = None
        for c in range(key_count // chunk):
            at = pl.ds(c * chunk, chunk)
            scores = lax.dot_general(
                q, kv_ref[at, :], (((1,), (1,)), ((), ())), preferred_element_type=jnp.float32
            )
            peak = jnp.max(scores, -1, keepdims=True)
            new_top = peak if top is None else jnp.maximum(top, peak)
            weights = jnp.exp(scores - new_top).astype(jnp.bfloat16)
            part = jnp.dot(weights, vals_ref[at, :], preferred_element_type=jnp.float32)
            total = part if top is None else total * jnp.exp(top - new_top) + part
            top = new_top
        results.append(total)
    first, second = (t / pltpu.roll(t, HEAD_SIZE, 1) for t in results)
    out_ref[...] = jnp.where(
        lane < HEAD_SIZE, pltpu.roll(first, HEAD_SIZE, 1), second
    ).astype(jnp.bfloat16)


def attend(q, kv, block=256, chunk=2048):
    heads, rows, width = q.shape
    key_count = kv.shape[1]
    block, chunk = math.gcd(rows, block), math.gcd(key_count, chunk)
    return pl.pallas_call(
        functools.partial(attend_kernel, chunk),
        grid=(heads, rows // block),
        in_specs=[
            pl.BlockSpec((None, block, width), lambda h, i: (h, i, 0)),
            pl.BlockSpec((None, key_count, width), lambda h, i: (h, 0, 0)),
        ],
        out_specs=pl.BlockSpec((None, block, width), lambda h, i: (h, i, 0)),
        out_shape=jax.ShapeDtypeStruct(q.shape, jnp.bfloat16),
        scratch_shapes=[pltpu.VMEM((key_count, width), jnp.bfloat16)],
        compiler_params=pltpu.CompilerParams(dimension_semantics=("arbitrary", "arbitrary")),
        cost_estimate=pl.CostEstimate(
            flops=heads * rows * key_count * 16 * HEAD_SIZE,
            bytes_accessed=2 * (2 * q.size + kv.size),
            transcendentals=heads * rows * key_count * 2,
        ),
    )(q, kv)


def local(
    queries,
    keys,
    values,
    q_gain,
    key_norm_gain,
    out_weight,
    residual,
    ln1_gain,
    ln1_bias,
    up_weight,
    down_weight,
    ln2_gain,
    ln2_bias,
):
    tok_rows = queries.shape[0]
    n_a, n_tp = lax.axis_size("a"), lax.axis_size("tp")
    grid_places = lax.axis_index(("a", "w")) * tok_rows + jnp.arange(tok_rows, dtype=jnp.int32)
    kv_heads = keys.shape[1] // HEAD_SIZE
    q_count = queries.shape[1] // HEAD_SIZE
    own_heads = kv_heads // n_a
    query_rows = prepare_inputs(
        queries.reshape(tok_rows, q_count, HEAD_SIZE), q_gain, grid_places, HEAD_SIZE ** (-0.5)
    ).reshape(tok_rows, kv_heads, 2 * HEAD_SIZE)
    key_rows = prepare_inputs(
        keys.reshape(tok_rows, kv_heads, HEAD_SIZE), key_norm_gain, grid_places, 1.0
    )
    value_rows = values.reshape(tok_rows, kv_heads, HEAD_SIZE)
    packed = jnp.concatenate([query_rows, key_rows, value_rows], -1)
    packed = jnp.transpose(packed, (1, 0, 2)).reshape(n_a, own_heads, tok_rows, 4 * HEAD_SIZE)
    packed = lax.all_to_all(packed, "a", 0, 0, tiled=True)
    packed = jnp.transpose(packed, (1, 0, 2, 3)).reshape(
        own_heads, n_a * tok_rows, 4 * HEAD_SIZE
    )
    q = packed[..., : 2 * HEAD_SIZE]
    kv = lax.all_gather(packed[..., 2 * HEAD_SIZE :], "w", axis=1, tiled=True)
    kv, down_weight = lax.optimization_barrier((kv, down_weight))

    out_full = line_gather(out_weight, "tp").reshape(-1, D)
    up_own = lax.all_to_all(up_weight, "a", 1, 0, tiled=True)
    up_full = lax.all_gather(up_own, "w", axis=0, tiled=True)
    down_own = swap_blocks(down_weight.reshape(n_a, -1, down_weight.shape[1]), "a")
    down_own = down_own.swapaxes(0, 1).reshape(down_weight.shape[0] // n_a, -1)

    attended = attend(q, kv)
    rows = tok_rows // n_tp
    sent = attended.reshape(own_heads, n_a * n_tp, rows, 2 * HEAD_SIZE)
    sent = jnp.transpose(sent, (1, 0, 2, 3))
    got = lax.all_to_all(sent, ("a", "tp"), 0, 0, tiled=True)
    got, down_own = lax.optimization_barrier((got, down_own))
    down_full = lax.all_gather(down_own, "w", axis=0)
    got = got.reshape(n_a, n_tp, own_heads, rows, 2 * HEAD_SIZE)
    group_cols = jnp.transpose(got, (1, 3, 0, 2, 4)).reshape(n_tp, rows, -1)
    out_groups = out_full.reshape(2, -1, D)
    both = jnp.transpose(group_cols, (1, 0, 2)).reshape(rows, 2, -1)
    mixed = sum(
        jnp.dot(both[:, g], out_groups[g], preferred_element_type=jnp.float32)
        .astype(jnp.bfloat16)
        .astype(jnp.float32)
        for g in range(2)
    )
    own_residual = lax.dynamic_slice_in_dim(residual, lax.axis_index("tp") * rows, rows, 0)
    normed = layer_norm(
        ALPHA * own_residual.astype(jnp.float32) + mixed, ln1_gain, ln1_bias
    ).astype(jnp.bfloat16)
    n_w = lax.axis_size("w")
    turned = turn_cols(normed, n_a, n_w)
    full_rows = line_gather(line_gather(turned, "a"), "tp").reshape(-1, D)
    up_acts = jnp.dot(full_rows, up_full, preferred_element_type=jnp.float32)
    hidden = jnp.square(jnp.maximum(up_acts, 0.0)).astype(jnp.bfloat16)
    partial_ffn = jnp.concatenate(
        [
            jnp.dot(hidden, down_full[i], preferred_element_type=jnp.float32).astype(jnp.bfloat16)
            for i in range(down_full.shape[0])
        ],
        -1,
    )
    ffn_out = lax.psum_scatter(partial_ffn, "tp", scatter_dimension=0, tiled=True)
    ffn_out = lax.psum_scatter(ffn_out, "a", scatter_dimension=0, tiled=True)
    ffn_out = (
        ffn_out.reshape(rows, n_w, n_a, -1).swapaxes(1, 2).reshape(rows, D).astype(jnp.float32)
    )
    encoded = layer_norm(
        ALPHA * normed.astype(jnp.float32) + ffn_out, ln2_gain, ln2_bias
    ).astype(jnp.bfloat16)
    return lax.all_to_all(encoded, "tp", 1, 0, tiled=True)


MESH = pl.DeviceIdType.MESH
BF16, F32 = jnp.bfloat16, jnp.float32


def scaled(index, size):
    return pl.ds(pl.multiple_of(index * size, size), size)


def layer_kernel(
    n_a,
    n_w,
    packed,
    up_own,
    down_own,
    out_own,
    res_all,
    gain1,
    bias1,
    gain2,
    bias2,
    out,
    qkv,
    kv,
    vals,
    att_out,
    att_in,
    out_full,
    res,
    mixed,
    up,
    down,
    toks,
    hid,
    part,
    sib_out,
    sib_in,
    rs_out,
    rs_in,
    enc_out,
    loc_sem,
    qkv_s,
    qkv_r,
    kv_s,
    kv_r,
    att_s,
    att_r,
    wz_s,
    wz_r,
    wf_s,
    wf_r,
    wd_s,
    wd_r,
    tz_s,
    tz_r,
    pair_s,
    pair_r,
    sib_s,
    sib_r,
    rs_s,
    rs_r,
):
    place, core = lax.axis_index("sp"), lax.axis_index("tp")
    a, w = place // n_w, place % n_w
    other = 1 - core
    x_side = w + 1 - 2 * (w % 2)
    y_side = w + 2 - 4 * (w // 2)
    sides = (x_side, y_side)
    rows = toks.shape[2]
    tok_rows = 2 * rows
    width = 2 * HEAD_SIZE
    up_rows, up_cols = up_own.shape[0], up.shape[1]
    down_rows, down_cols = down.shape[0], down_own.shape[1]

    def at(a_, w_, core_):
        return (a_ * n_w + w_, core_)

    sibling = at(a, w, other)

    def remote(src, dst, send, recv, target):
        return pltpu.make_async_remote_copy(
            src_ref=src,
            dst_ref=dst,
            send_sem=send,
            recv_sem=recv,
            device_id=target,
            device_id_type=MESH,
        )

    def landed(dst, recv, send):
        remote(dst, dst, send, recv, sibling).wait_recv()

    def sent(src, send, recv):
        remote(src, src, send, recv, sibling).wait_send()

    def cyc(k):
        return lax.rem(a + k + 2 * n_a, n_a)

    def w_slot(kind, a_, w_):
        if kind == 0:
            return up.at[scaled(a_ * n_w + w_, up_rows), :]
        return down.at[:, scaled(a_ * n_w + w_, down_cols)]

    def w_half(kind, a_, w_, h):
        if kind == 0:
            half = up_rows // 2
            return up.at[scaled((a_ * n_w + w_) * 2 + h, half), :]
        half = down_rows // 2
        return down.at[pl.ds(h * half, half), scaled(a_ * n_w + w_, down_cols)]

    def w_src(kind, a_):
        if kind == 0:
            return up_own.at[:, scaled(a_, up_cols)]
        return down_own.at[scaled(a_, down_rows), :]

    def w_exchange(kind, to):
        remote(
            w_src(kind, to),
            w_slot(kind, a, w),
            wz_s.at[kind, to],
            wz_r.at[kind, a],
            at(to, w, core),
        ).start()

    def w_forward(kind, frm):
        for j in range(2):
            remote(
                w_slot(kind, frm, w),
                w_slot(kind, frm, w),
                wf_s.at[kind, frm, j],
                wf_r.at[kind, frm, j],
                at(a, sides[j], core),
            ).start()

    def w_arrive(kind, frm):
        landed(w_slot(kind, frm, w), wz_r.at[kind, frm], wz_s.at[kind, frm])

    def w_pass(kind, frm):
        w_arrive(kind, frm)
        w_forward(kind, frm)

    def w_corner(kind, frm):
        for j in range(2):
            landed(w_slot(kind, frm, sides[j]), wf_r.at[kind, frm, j], wf_s.at[kind, frm, j])
            part_ref = w_half(kind, frm, sides[j], j)
            remote(
                part_ref,
                part_ref,
                wd_s.at[kind, frm, j],
                wd_r.at[kind, frm, j],
                at(a, sides[1 - j], core),
            ).start()

    def w_complete(kind):
        for k in range(n_a):
            frm = cyc(-k)
            for j in range(2):
                landed(
                    w_half(kind, frm, n_w - 1 - w, j),
                    wd_r.at[kind, frm, j],
                    wd_s.at[kind, frm, j],
                )

    def w_drain(kind):
        for k in range(1, n_a):
            to = cyc(k)
            sent(w_src(kind, to), wz_s.at[kind, to], wz_r.at[kind, to])
        for k in range(n_a):
            frm = cyc(-k)
            for j in range(2):
                sent(w_slot(kind, frm, w), wf_s.at[kind, frm, j], wf_r.at[kind, frm, j])
                sent(w_half(kind, frm, sides[j], j), wd_s.at[kind, frm, j], wd_r.at[kind, frm, j])

    local_copies = [
        pltpu.make_async_copy(up_own.at[:, scaled(a, up_cols)], w_slot(0, a, w), loc_sem.at[0]),
        pltpu.make_async_copy(
            down_own.at[scaled(a, down_rows), :], w_slot(1, a, w), loc_sem.at[1]
        ),
        pltpu.make_async_copy(out_own, out_full.at[core], loc_sem.at[2]),
        pltpu.make_async_copy(res_all.at[scaled(core, rows), :], res, loc_sem.at[3]),
    ]
    for copy in local_copies:
        copy.start()

    barrier = pltpu.get_barrier_semaphore()
    peers = [at(cyc(k), w, core_) for k in range(n_a) for core_ in (core, other)][1:]
    peers += [at(a, side, core) for side in (x_side, y_side, n_w - 1 - w)]
    for peer in peers:
        pl.semaphore_signal(barrier, inc=1, device_id=peer, device_id_type=MESH)
    pl.semaphore_wait(barrier, len(peers))

    w_peers = (x_side, y_side, n_w - 1 - w)

    def kv_slot(w_, a_):
        return kv.at[w_ * n_a + a_]

    def kv_forward(src, frm):
        for j, peer in enumerate(w_peers):
            remote(
                src,
                kv_slot(w, frm),
                kv_s.at[j, frm],
                kv_r.at[j, frm],
                at(a, peer, core),
            ).start()

    for k in range(1, n_a):
        to = cyc(k)
        remote(packed.at[to], qkv.at[a], qkv_s.at[to], qkv_r.at[a], at(to, w, core)).start()
    kv_forward(packed.at[a, :, pl.ds(width, width)], a)
    local_copies[0].wait()
    w_forward(0, a)
    local_copies[1].wait()
    w_forward(1, a)
    for k in range(1, n_a):
        w_exchange(0, cyc(k))
    remote(out_own, out_full.at[core], pair_s.at[0], pair_r.at[0], sibling).start()
    qkv[a] = packed[a]
    kv[w * n_a + a] = packed[a, :, width:]

    for k in range(1, n_a):
        frm = cyc(-k)
        landed(qkv.at[frm], qkv_r.at[frm], qkv_s.at[frm])
        kv_forward(qkv.at[frm, :, pl.ds(width, width)], frm)
        kv[w * n_a + frm] = qkv[frm, :, width:]
    w_corner(0, a)
    w_corner(1, a)
    for k in range(n_a):
        for j, peer in enumerate(w_peers):
            frm = cyc(-k)
            landed(kv_slot(peer, frm), kv_r.at[j, frm], kv_s.at[j, frm])

    slots = n_w * n_a
    lane_kv = lax.broadcasted_iota(jnp.int32, (tok_rows, width), 1)

    @pl.loop(0, slots)
    def _(i):
        vals[i] = jnp.where(lane_kv < HEAD_SIZE, 1.0, kv[i].astype(F32)).astype(BF16)

    lane = lax.broadcasted_iota(jnp.int32, (tok_rows, width), 1)
    chunks = 2
    per = slots // chunks

    @pl.loop(0, n_a)
    def _(i):
        block = cyc(1 + i)
        both = qkv[block, :, :width].astype(F32)
        results = []
        for head in range(2):
            own = both if head == 0 else pltpu.roll(both, HEAD_SIZE, 1)
            q = jnp.where(lane < HEAD_SIZE, own, 0.0).astype(BF16)
            top = None
            for c in range(chunks):
                keys = kv[pl.ds(c * per, per)].reshape(per * tok_rows, width)
                scores = lax.dot_general(
                    q, keys, (((1,), (1,)), ((), ())), preferred_element_type=F32
                )
                peak = jnp.max(scores, -1, keepdims=True)
                new_top = peak if top is None else jnp.maximum(top, peak)
                weights = jnp.exp(scores - new_top).astype(BF16)
                held = vals[pl.ds(c * per, per)].reshape(per * tok_rows, width)
                add = jnp.dot(weights, held, preferred_element_type=F32)
                total = add if top is None else total * jnp.exp(top - new_top) + add
                top = new_top
            results.append(total)
        first, second = (t / pltpu.roll(t, HEAD_SIZE, 1) for t in results)
        att_out[block] = jnp.where(
            lane < HEAD_SIZE, pltpu.roll(first, HEAD_SIZE, 1), second
        ).astype(BF16)
        mine = core * n_a + a
        remote(
            att_out.at[block, scaled(other, rows), :],
            att_in.at[mine],
            att_s.at[block, 0],
            att_r.at[mine],
            at(block, w, other),
        ).start()

        @pl.when(i < n_a - 1)
        def _():
            remote(
                att_out.at[block, scaled(core, rows), :],
                att_in.at[mine],
                att_s.at[block, 1],
                att_r.at[mine],
                at(block, w, core),
            ).start()
            w_exchange(1, block)

        @pl.when((i > 0) & (i < n_a - 1))
        def _():
            w_pass(0, cyc(-i))


    w_corner(0, cyc(-1))
    w_pass(0, cyc(1 - n_a))
    att_in[core * n_a + a] = att_out[a, scaled(core, rows), :]
    local_copies[2].wait()
    local_copies[3].wait()
    landed(out_full.at[other], pair_r.at[0], pair_s.at[0])
    for core_ in (core, other):
        for k in range(n_a):
            frm = cyc(-k)
            if k == 0 and core_ is core:
                continue
            frm_slot = core_ * n_a + frm
            landed(att_in.at[frm_slot], att_r.at[frm_slot], att_s.at[frm, 0])

    tile = 256

    @pl.loop(0, D // tile)
    def _(t):
        cols = scaled(t, tile)
        total = None
        for g in range(2):
            lhs = jnp.concatenate([att_in[g * n_a + k] for k in range(n_a)], -1)
            add = jnp.dot(lhs, out_full[g, :, cols], preferred_element_type=F32)
            add = add.astype(BF16).astype(F32)
            total = add if total is None else total + add
        mixed[:, cols] = total

    step = 16

    @pl.loop(0, rows // step)
    def _(t):
        r = scaled(t, step)
        toks[a, 0, r, :] = layer_norm(
            ALPHA * res[r, :].astype(F32) + mixed[r, :], gain1[...], bias1[...]
        ).astype(BF16)

    def tok_send(b, dest, way):
        remote(
            toks.at[b, 0], toks.at[b, 0], tz_s.at[b, way], tz_r.at[b], at(dest, w, core)
        ).start()

    def tok_pair(b):
        remote(toks.at[b, 0], toks.at[b, 1], pair_s.at[1 + b], pair_r.at[1 + b], sibling).start()

    last = n_a - 1

    @pl.when(a < last)
    def _():
        tok_send(a, a + 1, 0)

    @pl.when(a > 0)
    def _():
        tok_send(a, a - 1, 1)

    tok_pair(a)
    low = jnp.minimum(a, last - a)
    toward = jnp.where(2 * a < n_a, 1, -1)

    def order(k):
        near = a + (1 if k % 2 else -1) * ((k + 1) // 2)
        return jnp.where(k <= 2 * low, near, a + toward * (k - low))

    def relay(k):
        b = order(k)
        landed(toks.at[b, 0], tz_r.at[b], tz_s.at[b, 0])

        @pl.when((b > a) & (a > 0))
        def _():
            tok_send(b, a - 1, 1)

        @pl.when((b < a) & (a < last))
        def _():
            tok_send(b, a + 1, 0)

        tok_pair(b)

    def up_part(k):
        b = order(k)
        landed(toks.at[b, 1], pair_r.at[1 + b], pair_s.at[1 + b])

        @pl.loop(0, up_cols // tile)
        def _(t):
            cols = scaled(t, tile)
            acts = jnp.dot(
                toks[b].reshape(tok_rows, D), up[:, cols], preferred_element_type=F32
            )
            hid[b, :, cols] = jnp.square(jnp.maximum(acts, 0.0)).astype(BF16)

    for k in range(2, n_a):
        w_corner(0, cyc(-k))
        w_pass(1, cyc(1 - k))
    w_complete(0)
    up_part(0)
    for k in range(1, n_a - 1):
        relay(k)
        w_corner(1, cyc(-k))
        if k == 1:
            w_pass(1, cyc(1 - n_a))
        up_part(k)

    @pl.when(low > 0)
    def _():
        relay(n_a - 1)

    w_corner(1, cyc(1 - n_a))
    w_complete(1)

    groups = n_a
    g_cols = D // groups
    ahead = last - low

    def target(k):
        far = jnp.where(low > 0, k + 1, lax.rem(k + 1, last) + 1)
        dest = jnp.where(k < ahead, a + toward * far, a - toward * (k - ahead + 1))
        return jnp.where(k < last, dest, a)

    def piece(ref, g):
        return ref.at[:, scaled(g, g_cols)]

    def hop(b):
        return a + jnp.where(b > a, 1, -1)

    def inbox(p, b):
        return jnp.where((b == p) & (p < a), n_a, b)

    @pl.loop(0, n_a * groups + 1)
    def _(i):
        @pl.when(i == groups)
        def _():
            @pl.when(low == 0)
            def _():
                relay(n_a - 1)

            up_part(n_a - 1)

        @pl.when(i < n_a * groups)
        def _():
            b, g = target(i // groups), lax.rem(i, groups)

            @pl.loop(0, g_cols // tile)
            def _(t):
                cols = scaled(g * (g_cols // tile) + t, tile)
                acts = jnp.dot(hid[b], down[:, cols], preferred_element_type=F32)
                part[b, :, cols] = acts[:rows]
                sib_out[b, :, cols] = acts[rows:].astype(BF16)

            remote(
                piece(sib_out.at[b], g),
                piece(sib_in.at[b], g),
                sib_s.at[b, g],
                sib_r.at[b, g],
                sibling,
            ).start()

        @pl.when((i > 0) & (i <= last * groups))
        def _():
            b, g = target((i - 1) // groups), lax.rem(i - 1, groups)
            cols = scaled(g, g_cols)
            landed(piece(sib_in.at[b], g), sib_r.at[b, g], sib_s.at[b, g])

            @pl.when(low > 0)
            def _():
                landed(piece(rs_in.at[b], g), rs_r.at[b, g], rs_s.at[b, g])

            @pl.loop(0, rows // step)
            def _(t):
                r = scaled(t, step)
                total = part[b, r, cols] + sib_in[b, r, cols].astype(F32)
                total = jnp.where(low > 0, total + rs_in[b, r, cols].astype(F32), total)
                rs_out[b, r, cols] = total.astype(BF16)

            p = hop(b)
            slot = inbox(p, b)
            remote(
                piece(rs_out.at[b], g),
                piece(rs_in.at[slot], g),
                rs_s.at[b, g],
                rs_r.at[slot, g],
                at(p, w, core),
            ).start()

    for g in range(groups):
        landed(piece(sib_in.at[a], g), sib_r.at[a, g], sib_s.at[a, g])

        @pl.when(a > 0)
        def _(g=g):
            landed(piece(rs_in.at[a], g), rs_r.at[a, g], rs_s.at[a, g])

        @pl.when(a < last)
        def _(g=g):
            landed(piece(rs_in.at[n_a], g), rs_r.at[n_a, g], rs_s.at[a, g])

    half = D // 2

    @pl.loop(0, rows // step)
    def _(t):
        r = scaled(t, step)
        total = part[a, r, :] + sib_in[a, r, :].astype(F32)
        total = jnp.where(a > 0, total + rs_in[a, r, :].astype(F32), total)
        total = jnp.where(a < last, total + rs_in[n_a, r, :].astype(F32), total)
        encoded = layer_norm(
            ALPHA * toks[a, 0, r, :].astype(F32) + total, gain2[...], bias2[...]
        )
        left, right = encoded[:, :half].astype(BF16), encoded[:, half:].astype(BF16)
        out[pl.ds(pl.multiple_of(core * rows + t * step, step), step), :] = jnp.where(
            core == 0, left, right
        )
        enc_out[r, :] = jnp.where(core == 0, right, left)

    swap = remote(enc_out, out.at[scaled(core, rows), :], pair_s.at[n_a + 1], pair_r.at[n_a + 1], sibling)
    swap.start()
    for k in range(1, n_a):
        to = cyc(k)
        sent(packed.at[to], qkv_s.at[to], qkv_r.at[to])
    for k in range(n_a):
        for j in range(3):
            sent(kv_slot(w, k), kv_s.at[j, k], kv_r.at[j, k])
    sent(out_own, pair_s.at[0], pair_r.at[0])
    for kind in range(2):
        w_drain(kind)
    for k in range(n_a):
        b = cyc(k)
        sent(att_out.at[b, pl.ds(0, rows), :], att_s.at[b, 0], att_r.at[b])
        if k:
            sent(att_out.at[b, pl.ds(0, rows), :], att_s.at[b, 1], att_r.at[b])
            for g in range(groups):
                sent(piece(rs_out.at[b], g), rs_s.at[b, g], rs_r.at[b, g])
        for g in range(groups):
            sent(piece(sib_out.at[b], g), sib_s.at[b, g], sib_r.at[b, g])
        sent(toks.at[b, 0], pair_s.at[1 + b], pair_r.at[1 + b])

        @pl.when((a < last) & (b <= a))
        def _():
            sent(toks.at[b, 0], tz_s.at[b, 0], tz_r.at[b])

        @pl.when((a > 0) & (b >= a))
        def _():
            sent(toks.at[b, 0], tz_s.at[b, 1], tz_r.at[b])

    swap.wait_send()
    landed(out.at[scaled(other, rows), :], pair_r.at[n_a + 1], pair_s.at[n_a + 1])


def fused(n_a, n_w, *args):
    (queries, keys, values, q_gain, key_norm_gain, out_weight, residual, *rest) = args
    ln1_gain, ln1_bias, up_weight, down_weight, ln2_gain, ln2_bias = rest
    tok_rows = queries.shape[0]
    rows = tok_rows // 2
    places = lax.axis_index("sp") * tok_rows + jnp.arange(tok_rows, dtype=jnp.int32)
    heads = keys.shape[1] // HEAD_SIZE
    query_rows = prepare_inputs(
        queries.reshape(tok_rows, 2 * heads, HEAD_SIZE), q_gain, places, HEAD_SIZE ** (-0.5)
    ).reshape(tok_rows, heads, 2 * HEAD_SIZE)
    key_rows = prepare_inputs(
        keys.reshape(tok_rows, heads, HEAD_SIZE), key_norm_gain, places, 1.0
    )
    packed = jnp.concatenate(
        [query_rows, key_rows, values.reshape(tok_rows, heads, HEAD_SIZE)], -1
    )
    packed = jnp.transpose(packed, (1, 0, 2))
    width = 2 * HEAD_SIZE
    up_cols = up_weight.shape[1] // n_a
    down_rows = down_weight.shape[0] // n_a
    dma, vmem = pltpu.SemaphoreType.DMA, pltpu.VMEM
    whole, hbm = pl.BlockSpec(memory_space=pltpu.VMEM), pl.BlockSpec(memory_space=pl.ANY)
    return pl.pallas_call(
        functools.partial(layer_kernel, n_a, n_w),
        out_shape=jax.ShapeDtypeStruct((tok_rows, D // 2), BF16),
        in_specs=[whole] + [hbm] * 4 + [whole] * 4,
        out_specs=whole,
        scratch_shapes=[
            vmem((n_a, tok_rows, 2 * width), BF16),
            vmem((n_w * n_a, tok_rows, width), BF16),
            vmem((n_w * n_a, tok_rows, width), BF16),
            vmem((n_a, tok_rows, width), BF16),
            vmem((2 * n_a, rows, width), BF16),
            vmem((2, *out_weight.shape), BF16),
            vmem((rows, D), BF16),
            vmem((rows, D), F32),
            vmem((D, up_cols), BF16),
            vmem((down_rows, D), BF16),
            vmem((n_a, 2, rows, D), BF16),
            vmem((n_a, tok_rows, up_cols), BF16),
            vmem((n_a, rows, D), F32),
            vmem((n_a, rows, D), BF16),
            vmem((n_a, rows, D), BF16),
            vmem((n_a, rows, D), BF16),
            vmem((n_a + 1, rows, D), BF16),
            vmem((rows, D // 2), BF16),
            dma((4,)),
            dma((n_a,)),
            dma((n_a,)),
            dma((3, n_a)),
            dma((3, n_a)),
            dma((n_a, 2)),
            dma((2 * n_a,)),
            dma((2, n_a)),
            dma((2, n_a)),
            dma((2, n_a, 2)),
            dma((2, n_a, 2)),
            dma((2, n_a, 2)),
            dma((2, n_a, 2)),
            dma((n_a, 2)),
            dma((n_a,)),
            dma((n_a + 2,)),
            dma((n_a + 2,)),
            dma((n_a, n_a)),
            dma((n_a, n_a)),
            dma((n_a, n_a)),
            dma((n_a + 1, n_a)),
        ],
        compiler_params=pltpu.CompilerParams(
            collective_id=0, has_side_effects=True, vmem_limit_bytes=60 * 2**20
        ),
    )(
        packed,
        up_weight,
        down_weight,
        out_weight,
        residual,
        *(v.reshape(1, D) for v in (ln1_gain, ln1_bias, ln2_gain, ln2_bias)),
    )


def solution(mesh):
    n_sp, n_tp = mesh.shape["sp"], mesh.shape["tp"]

    def layer(queries, keys, *others):
        n_a = math.gcd(n_sp, keys.shape[1] // (HEAD_SIZE * n_tp))
        n_w = n_sp // n_a
        sp = ("a", "w")
        if n_tp == 2 and n_w == 4 and n_a * HEAD_SIZE * n_tp == keys.shape[1]:
            cut = P("sp", "tp")
            return jax.shard_map(
                functools.partial(fused, n_a, n_w),
                mesh=mesh,
                in_specs=(cut, cut, cut, P(), P(), P("tp", None), P("sp", None), P(), P())
                + (cut, P("tp", "sp"), P(), P()),
                out_specs=cut,
                check_vma=False,
            )(queries, keys, *others)
        groups = Mesh(mesh.devices.reshape(n_a, n_w, n_tp), ("a", "w", "tp"))
        cut = P(sp, "tp")
        return jax.shard_map(
            local,
            mesh=groups,
            in_specs=(cut, cut, cut, P(), P(), P("tp", None), P(sp, None), P(), P())
            + (cut, P("tp", sp), P(), P()),
            out_specs=cut,
            check_vma=False,
        )(queries, keys, *others)

    return layer
```

```python
import functools
import math

import jax
import jax.numpy as jnp
from jax import lax
from jax.experimental import pallas as pl
from jax.experimental.pallas import tpu as pltpu
from jax.sharding import Mesh, PartitionSpec as P

D = 2048
HEAD_SIZE = 64
GRID_W = 64


ALPHA = 8.0**0.25
ROTARY_BASE = 10000.0
RMS_EPSILON = 1e-06
NORM_EPSILON = 1e-05


def rotate_grid(heads_in, grid_places):
    half_dim = heads_in.shape[-1] // 2
    quarter = half_dim // 2
    inverse = ROTARY_BASE ** (-jnp.arange(quarter, dtype=jnp.float32) / quarter)

    def spin(segment, coords):
        angles = coords.astype(jnp.float32)[:, None] * inverse[None, :]
        cos_val = jnp.cos(angles)[:, None, :]
        sin_val = jnp.sin(angles)[:, None, :]
        lead_half = segment[..., :quarter]
        tail_half = segment[..., quarter:]
        return jnp.concatenate(
            [lead_half * cos_val - tail_half * sin_val, tail_half * cos_val + lead_half * sin_val],
            -1,
        )

    return jnp.concatenate(
        [
            spin(heads_in[..., :half_dim], grid_places // GRID_W),
            spin(heads_in[..., half_dim:], grid_places % GRID_W),
        ],
        -1,
    )


def prepare_inputs(heads_in, gain_vec, grid_places, factor):
    values32 = heads_in.astype(jnp.float32)
    normed = (
        values32
        * lax.rsqrt(jnp.mean(values32 * values32, -1, keepdims=True) + RMS_EPSILON)
        * gain_vec
    )
    return (rotate_grid(normed, grid_places) * factor).astype(jnp.bfloat16)


def layer_norm(pre_norm, gain_vec, bias_vec):
    row_mean = jnp.mean(pre_norm, -1, keepdims=True)
    centred = pre_norm - row_mean
    spread = jnp.mean(centred * centred, -1, keepdims=True)
    return centred * lax.rsqrt(spread + NORM_EPSILON) * gain_vec + bias_vec


def line_gather(block, axis):
    n, me = lax.axis_size(axis), lax.axis_index(axis)
    up = [(i, i + 1) for i in range(n - 1)]
    down = [(i + 1, i) for i in range(n - 1)]
    from_left, from_right = [block], [block]
    for _ in range(n - 1):
        from_left.append(lax.ppermute(from_left[-1], axis, up))
        from_right.append(lax.ppermute(from_right[-1], axis, down))
    stacked = jnp.zeros((n, *block.shape), block.dtype)
    for k in range(n):
        piece = block if k == 0 else jnp.where(me >= k, from_left[k], from_right[n - k])
        stacked = lax.dynamic_update_index_in_dim(stacked, piece, (me - k + n) % n, 0)
    return stacked


def swap_blocks(blocks, axis):
    n, me = lax.axis_size(axis), lax.axis_index(axis)
    stacked = jnp.zeros_like(blocks)
    for k in range(n):
        piece = lax.dynamic_index_in_dim(blocks, (me + k) % n, 0, keepdims=False)
        if k:
            piece = lax.ppermute(piece, axis, [(i, (i + k) % n) for i in range(n)])
        stacked = lax.dynamic_update_index_in_dim(stacked, piece, (me - k + n) % n, 0)
    return stacked


def turn_cols(block, outer, inner):
    width = block.shape[1] // (outer * inner)
    starts = [(o * inner + i) * width for i in range(inner) for o in range(outer)]
    return jnp.concatenate([block[:, c : c + width] for c in starts], -1)


def attend_kernel(chunk, q_ref, kv_ref, out_ref, vals_ref):
    width = 2 * HEAD_SIZE
    key_count = kv_ref.shape[0]
    rows = q_ref.shape[0]

    @pl.when(pl.program_id(1) == 0)
    def _():
        lane_kv = lax.broadcasted_iota(jnp.int32, (chunk, width), 1)

        @pl.loop(0, key_count // chunk)
        def _(c):
            at = pl.ds(pl.multiple_of(c * chunk, chunk), chunk)
            vals_ref[at, :] = jnp.where(
                lane_kv < HEAD_SIZE, 1.0, kv_ref[at, :].astype(jnp.float32)
            ).astype(jnp.bfloat16)

    lane = lax.broadcasted_iota(jnp.int32, (rows, width), 1)
    both = q_ref[...].astype(jnp.float32)
    results = []
    for head in range(2):
        own = both if head == 0 else pltpu.roll(both, HEAD_SIZE, 1)
        q = jnp.where(lane < HEAD_SIZE, own, 0.0).astype(jnp.bfloat16)
        top = None
        for c in range(key_count // chunk):
            at = pl.ds(c * chunk, chunk)
            scores = lax.dot_general(
                q, kv_ref[at, :], (((1,), (1,)), ((), ())), preferred_element_type=jnp.float32
            )
            peak = jnp.max(scores, -1, keepdims=True)
            new_top = peak if top is None else jnp.maximum(top, peak)
            weights = jnp.exp(scores - new_top).astype(jnp.bfloat16)
            part = jnp.dot(weights, vals_ref[at, :], preferred_element_type=jnp.float32)
            total = part if top is None else total * jnp.exp(top - new_top) + part
            top = new_top
        results.append(total)
    first, second = (t / pltpu.roll(t, HEAD_SIZE, 1) for t in results)
    out_ref[...] = jnp.where(
        lane < HEAD_SIZE, pltpu.roll(first, HEAD_SIZE, 1), second
    ).astype(jnp.bfloat16)


def attend(q, kv, block=256, chunk=2048):
    heads, rows, width = q.shape
    key_count = kv.shape[1]
    block, chunk = math.gcd(rows, block), math.gcd(key_count, chunk)
    return pl.pallas_call(
        functools.partial(attend_kernel, chunk),
        grid=(heads, rows // block),
        in_specs=[
            pl.BlockSpec((None, block, width), lambda h, i: (h, i, 0)),
            pl.BlockSpec((None, key_count, width), lambda h, i: (h, 0, 0)),
        ],
        out_specs=pl.BlockSpec((None, block, width), lambda h, i: (h, i, 0)),
        out_shape=jax.ShapeDtypeStruct(q.shape, jnp.bfloat16),
        scratch_shapes=[pltpu.VMEM((key_count, width), jnp.bfloat16)],
        compiler_params=pltpu.CompilerParams(dimension_semantics=("arbitrary", "arbitrary")),
        cost_estimate=pl.CostEstimate(
            flops=heads * rows * key_count * 16 * HEAD_SIZE,
            bytes_accessed=2 * (2 * q.size + kv.size),
            transcendentals=heads * rows * key_count * 2,
        ),
    )(q, kv)


def local(
    queries,
    keys,
    values,
    q_gain,
    key_norm_gain,
    out_weight,
    residual,
    ln1_gain,
    ln1_bias,
    up_weight,
    down_weight,
    ln2_gain,
    ln2_bias,
):
    tok_rows = queries.shape[0]
    n_a, n_tp = lax.axis_size("a"), lax.axis_size("tp")
    grid_places = lax.axis_index(("a", "w")) * tok_rows + jnp.arange(tok_rows, dtype=jnp.int32)
    kv_heads = keys.shape[1] // HEAD_SIZE
    q_count = queries.shape[1] // HEAD_SIZE
    own_heads = kv_heads // n_a
    query_rows = prepare_inputs(
        queries.reshape(tok_rows, q_count, HEAD_SIZE), q_gain, grid_places, HEAD_SIZE ** (-0.5)
    ).reshape(tok_rows, kv_heads, 2 * HEAD_SIZE)
    key_rows = prepare_inputs(
        keys.reshape(tok_rows, kv_heads, HEAD_SIZE), key_norm_gain, grid_places, 1.0
    )
    value_rows = values.reshape(tok_rows, kv_heads, HEAD_SIZE)
    packed = jnp.concatenate([query_rows, key_rows, value_rows], -1)
    packed = jnp.transpose(packed, (1, 0, 2)).reshape(n_a, own_heads, tok_rows, 4 * HEAD_SIZE)
    packed = lax.all_to_all(packed, "a", 0, 0, tiled=True)
    packed = jnp.transpose(packed, (1, 0, 2, 3)).reshape(
        own_heads, n_a * tok_rows, 4 * HEAD_SIZE
    )
    q = packed[..., : 2 * HEAD_SIZE]
    kv = lax.all_gather(packed[..., 2 * HEAD_SIZE :], "w", axis=1, tiled=True)
    kv, down_weight = lax.optimization_barrier((kv, down_weight))

    out_full = line_gather(out_weight, "tp").reshape(-1, D)
    up_own = lax.all_to_all(up_weight, "a", 1, 0, tiled=True)
    up_full = lax.all_gather(up_own, "w", axis=0, tiled=True)
    down_own = swap_blocks(down_weight.reshape(n_a, -1, down_weight.shape[1]), "a")
    down_own = down_own.swapaxes(0, 1).reshape(down_weight.shape[0] // n_a, -1)

    attended = attend(q, kv)
    rows = tok_rows // n_tp
    sent = attended.reshape(own_heads, n_a * n_tp, rows, 2 * HEAD_SIZE)
    sent = jnp.transpose(sent, (1, 0, 2, 3))
    got = lax.all_to_all(sent, ("a", "tp"), 0, 0, tiled=True)
    got, down_own = lax.optimization_barrier((got, down_own))
    down_full = lax.all_gather(down_own, "w", axis=0)
    got = got.reshape(n_a, n_tp, own_heads, rows, 2 * HEAD_SIZE)
    group_cols = jnp.transpose(got, (1, 3, 0, 2, 4)).reshape(n_tp, rows, -1)
    out_groups = out_full.reshape(2, -1, D)
    both = jnp.transpose(group_cols, (1, 0, 2)).reshape(rows, 2, -1)
    mixed = sum(
        jnp.dot(both[:, g], out_groups[g], preferred_element_type=jnp.float32)
        .astype(jnp.bfloat16)
        .astype(jnp.float32)
        for g in range(2)
    )
    own_residual = lax.dynamic_slice_in_dim(residual, lax.axis_index("tp") * rows, rows, 0)
    normed = layer_norm(
        ALPHA * own_residual.astype(jnp.float32) + mixed, ln1_gain, ln1_bias
    ).astype(jnp.bfloat16)
    n_w = lax.axis_size("w")
    turned = turn_cols(normed, n_a, n_w)
    full_rows = line_gather(line_gather(turned, "a"), "tp").reshape(-1, D)
    up_acts = jnp.dot(full_rows, up_full, preferred_element_type=jnp.float32)
    hidden = jnp.square(jnp.maximum(up_acts, 0.0)).astype(jnp.bfloat16)
    partial_ffn = jnp.concatenate(
        [
            jnp.dot(hidden, down_full[i], preferred_element_type=jnp.float32).astype(jnp.bfloat16)
            for i in range(down_full.shape[0])
        ],
        -1,
    )
    ffn_out = lax.psum_scatter(partial_ffn, "tp", scatter_dimension=0, tiled=True)
    ffn_out = lax.psum_scatter(ffn_out, "a", scatter_dimension=0, tiled=True)
    ffn_out = (
        ffn_out.reshape(rows, n_w, n_a, -1).swapaxes(1, 2).reshape(rows, D).astype(jnp.float32)
    )
    encoded = layer_norm(
        ALPHA * normed.astype(jnp.float32) + ffn_out, ln2_gain, ln2_bias
    ).astype(jnp.bfloat16)
    return lax.all_to_all(encoded, "tp", 1, 0, tiled=True)


MESH = pl.DeviceIdType.MESH
BF16, F32 = jnp.bfloat16, jnp.float32


def scaled(index, size):
    return pl.ds(pl.multiple_of(index * size, size), size)


def layer_kernel(
    n_a,
    n_w,
    q_in,
    k_in,
    v_in,
    q_gain,
    k_gain,
    up_own,
    down_own,
    out_own,
    res_all,
    gain1,
    bias1,
    gain2,
    bias2,
    out,
    packed,
    qkv,
    kv,
    vals,
    q_held,
    att_out,
    att_in,
    out_full,
    res,
    mixed,
    up,
    down,
    toks,
    hid,
    part,
    sib_out,
    sib_in,
    rs_out,
    rs_in,
    enc_out,
    loc_sem,
    qkv_s,
    qkv_r,
    kv_s,
    kv_r,
    att_s,
    att_r,
    wz_s,
    wz_r,
    wf_s,
    wf_r,
    wd_s,
    wd_r,
    tz_s,
    tz_r,
    pair_s,
    pair_r,
    sib_s,
    sib_r,
    rs_s,
    rs_r,
):
    place, core = lax.axis_index("sp"), lax.axis_index("tp")
    a, w = place // n_w, place % n_w
    other = 1 - core
    x_side = w + 1 - 2 * (w % 2)
    y_side = w + 2 - 4 * (w // 2)
    sides = (x_side, y_side)
    rows = toks.shape[2]
    tok_rows = 2 * rows
    width = 2 * HEAD_SIZE
    up_rows, up_cols = up_own.shape[0], up.shape[1]
    down_rows, down_cols = down.shape[0], down_own.shape[1]

    def at(a_, w_, core_):
        return (a_ * n_w + w_, core_)

    sibling = at(a, w, other)

    def remote(src, dst, send, recv, target):
        return pltpu.make_async_remote_copy(
            src_ref=src,
            dst_ref=dst,
            send_sem=send,
            recv_sem=recv,
            device_id=target,
            device_id_type=MESH,
        )

    def landed(dst, recv, send):
        remote(dst, dst, send, recv, sibling).wait_recv()

    def sent(src, send, recv):
        remote(src, src, send, recv, sibling).wait_send()

    def cyc(k):
        return lax.rem(a + k + 2 * n_a, n_a)

    turns = (0, 1, 2, 3)
    mates = [a, a + 1 - 2 * (a % 2), a + 2 - 4 * (a // 2), n_a - 1 - a]

    def mate(k):
        return mates[turns[k]]

    def turn(k):
        found = turns[0]
        for j in range(1, n_a):
            found = jnp.where(k == j, turns[j], found)
        return found

    def w_slot(kind, a_, w_):
        if kind == 0:
            return up.at[scaled(a_ * n_w + w_, up_rows), :]
        return down.at[:, scaled(a_ * n_w + w_, down_cols)]

    def w_half(kind, a_, w_, h):
        if kind == 0:
            half = up_rows // 2
            return up.at[scaled((a_ * n_w + w_) * 2 + h, half), :]
        half = down_rows // 2
        return down.at[pl.ds(h * half, half), scaled(a_ * n_w + w_, down_cols)]

    def w_src(kind, a_):
        if kind == 0:
            return up_own.at[:, scaled(a_, up_cols)]
        return down_own.at[scaled(a_, down_rows), :]

    def w_exchange(kind, to):
        remote(
            w_src(kind, to),
            w_slot(kind, a, w),
            wz_s.at[kind, to],
            wz_r.at[kind, a],
            at(to, w, core),
        ).start()

    def w_forward(kind, frm):
        for j in range(2):
            remote(
                w_slot(kind, frm, w),
                w_slot(kind, frm, w),
                wf_s.at[kind, frm, j],
                wf_r.at[kind, frm, j],
                at(a, sides[j], core),
            ).start()

    def w_arrive(kind, frm):
        landed(w_slot(kind, frm, w), wz_r.at[kind, frm], wz_s.at[kind, frm])

    def w_pass(kind, frm):
        w_arrive(kind, frm)
        w_forward(kind, frm)

    def w_corner(kind, frm):
        for j in range(2):
            landed(w_slot(kind, frm, sides[j]), wf_r.at[kind, frm, j], wf_s.at[kind, frm, j])
            part_ref = w_half(kind, frm, sides[j], j)
            remote(
                part_ref,
                part_ref,
                wd_s.at[kind, frm, j],
                wd_r.at[kind, frm, j],
                at(a, sides[1 - j], core),
            ).start()

    def w_finish(kind, frm):
        for j in range(2):
            landed(
                w_half(kind, frm, n_w - 1 - w, j), wd_r.at[kind, frm, j], wd_s.at[kind, frm, j]
            )

    def w_complete(kind):
        for k in range(n_a):
            w_finish(kind, mate(k))

    def w_drain(kind):
        for k in range(1, n_a):
            to = mate(k)
            sent(w_src(kind, to), wz_s.at[kind, to], wz_r.at[kind, to])
        for k in range(n_a):
            frm = mate(k)
            for j in range(2):
                sent(w_slot(kind, frm, w), wf_s.at[kind, frm, j], wf_r.at[kind, frm, j])
                sent(w_half(kind, frm, sides[j], j), wd_s.at[kind, frm, j], wd_r.at[kind, frm, j])

    local_copies = [
        pltpu.make_async_copy(up_own.at[:, scaled(a, up_cols)], w_slot(0, a, w), loc_sem.at[0]),
        pltpu.make_async_copy(
            down_own.at[scaled(a, down_rows), :], w_slot(1, a, w), loc_sem.at[1]
        ),
        pltpu.make_async_copy(out_own, out_full.at[core], loc_sem.at[2]),
        pltpu.make_async_copy(res_all.at[scaled(core, rows), :], res, loc_sem.at[3]),
    ]
    for copy in local_copies:
        copy.start()

    barrier = pltpu.get_barrier_semaphore()
    w_peers = (x_side, y_side, n_w - 1 - w)
    peers = [at(cyc(k), w, core) for k in range(1, n_a)] + [sibling]
    peers += [at(a, side, core_) for side in w_peers for core_ in (core, other)]
    for peer in peers:
        pl.semaphore_signal(barrier, inc=1, device_id=peer, device_id_type=MESH)
    pl.semaphore_wait(barrier, len(peers))

    w_exchange(0, mate(1))
    remote(out_own, out_full.at[core], pair_s.at[0], pair_r.at[0], sibling).start()

    half_head, quarter = HEAD_SIZE // 2, HEAD_SIZE // 4
    lane = lax.broadcasted_iota(jnp.int32, (tok_rows, width), 1)
    token = lax.broadcasted_iota(jnp.int32, (tok_rows, width), 0) + place * tok_rows
    coord = jnp.where(lane % HEAD_SIZE < half_head, token // GRID_W, token % GRID_W)
    power = (lane % quarter).astype(F32) * (-math.log(ROTARY_BASE) / quarter)
    angle = coord.astype(F32) * jnp.exp(power)
    tail = lane % half_head >= quarter
    cos_val, sin_val = jnp.cos(angle), jnp.sin(angle)
    sin_val = jnp.where(tail, sin_val, -sin_val)
    first_head = lane < HEAD_SIZE

    def prepared(group, gain):
        squares = group * group
        low_sum = jnp.sum(jnp.where(first_head, squares, 0.0), -1, keepdims=True)
        high_sum = jnp.sum(jnp.where(first_head, 0.0, squares), -1, keepdims=True)
        mean = jnp.where(first_head, low_sum, high_sum) * (1.0 / HEAD_SIZE)
        unit = group * lax.rsqrt(mean + RMS_EPSILON) * gain
        partner = jnp.where(
            tail, pltpu.roll(unit, quarter, 1), pltpu.roll(unit, width - quarter, 1)
        )
        return unit * cos_val + partner * sin_val

    q_both, k_both = (jnp.concatenate([g[...], g[...]], -1) for g in (q_gain, k_gain))
    for h in range(n_w):
        q_group = q_in[:, h * width : (h + 1) * width].astype(F32)
        packed[h, :, :width] = (
            prepared(q_group, q_both) * (HEAD_SIZE ** (-0.5))
        ).astype(BF16)
    for h in range(0, n_w, 2):
        cols = slice(h // 2 * width, (h // 2 + 1) * width)
        k_group = prepared(k_in[:, cols].astype(F32), k_both)
        v_group = v_in[:, cols].astype(F32)
        packed[h, :, width:] = jnp.where(
            first_head, k_group, pltpu.roll(v_group, HEAD_SIZE, 1)
        ).astype(BF16)
        packed[h + 1, :, width:] = jnp.where(
            first_head, pltpu.roll(k_group, HEAD_SIZE, 1), v_group
        ).astype(BF16)

    for j, peer in enumerate(w_peers):
        remote(
            packed.at[peer], qkv.at[w], qkv_s.at[j], qkv_r.at[j], at(a, peer, core)
        ).start()
    local_copies[0].wait()
    w_forward(0, a)
    local_copies[1].wait()
    w_forward(1, a)
    qkv[w] = packed[w]

    last = n_a - 1
    low = jnp.minimum(a, last - a)
    toward = jnp.where(2 * a < n_a, 1, -1)

    def order(k):
        near = a + toward * jnp.where(k % 2 == 1, 1, -1) * ((k + 1) // 2)
        return jnp.where(k <= 2 * low, near, a + toward * (k - low))

    def kv_slot(b, w_):
        return kv.at[b, scaled(w_, tok_rows), :]

    def kv_send(src, b, w_, dest, way):
        remote(
            src, kv_slot(b, w_), kv_s.at[b, w_, way], kv_r.at[b, w_], at(dest, w, core)
        ).start()

    for j, frm in enumerate((w, *w_peers)):
        if j:
            landed(qkv.at[frm], qkv_r.at[j - 1], qkv_s.at[j - 1])
        mine = qkv.at[frm, :, pl.ds(width, width)]

        @pl.when(a < last)
        def _(mine=mine, frm=frm):
            kv_send(mine, a, frm, a + 1, 0)

        @pl.when(a > 0)
        def _(mine=mine, frm=frm):
            kv_send(mine, a, frm, a - 1, 1)

        kv[a, scaled(frm, tok_rows), :] = qkv[frm, :, width:]
        both = qkv[frm, :, :width].astype(F32)
        for head in range(2):
            own = both if head == 0 else pltpu.roll(both, HEAD_SIZE, 1)
            q_held[frm, head] = jnp.where(first_head, own, 0.0).astype(BF16)

    def kv_relay(k):
        b = order(k)

        @pl.loop(0, n_w)
        def _(w_):
            landed(kv_slot(b, w_), kv_r.at[b, w_], kv_s.at[b, w_, 0])

            @pl.when((b > a) & (a > 0))
            def _():
                kv_send(kv_slot(b, w_), b, w_, a - 1, 1)

            @pl.when((b < a) & (a < last))
            def _():
                kv_send(kv_slot(b, w_), b, w_, a + 1, 0)

    w_exchange(0, mate(2))
    kv_relay(1)
    w_pass(0, mate(1))
    kv_relay(2)
    w_corner(0, a)
    kv_relay(3)
    w_exchange(0, mate(3))
    w_corner(1, a)
    w_pass(0, mate(2))
    @pl.loop(0, n_a)
    def _(b):
        @pl.loop(0, n_w)
        def _(w_):
            r = scaled(w_, tok_rows)
            vals[b, r, :] = jnp.where(first_head, 1.0, kv[b, r, :].astype(F32)).astype(BF16)

    chunks = 2
    per = n_a // chunks

    @pl.loop(0, n_w)
    def _(i):
        block = lax.rem(w + 1 + i, n_w)
        results = []
        for head in range(2):
            top = None
            for c in range(chunks):
                planes = pl.ds(c * per, per)
                scores = lax.dot_general(
                    q_held[block, head],
                    kv[planes].reshape(-1, width),
                    (((1,), (1,)), ((), ())),
                    preferred_element_type=F32,
                )
                peak = jnp.max(scores, -1, keepdims=True)
                new_top = peak if top is None else jnp.maximum(top, peak)
                weights = jnp.exp(scores - new_top).astype(BF16)
                add = jnp.dot(
                    weights, vals[planes].reshape(-1, width), preferred_element_type=F32
                )
                total = add if top is None else total * jnp.exp(top - new_top) + add
                top = new_top
            results.append(total)
        first, second = (t / pltpu.roll(t, HEAD_SIZE, 1) for t in results)
        att_out[block] = jnp.where(
            first_head, pltpu.roll(first, HEAD_SIZE, 1), second
        ).astype(BF16)
        mine = core * n_w + w
        remote(
            att_out.at[block, scaled(other, rows), :],
            att_in.at[mine],
            att_s.at[block, 0],
            att_r.at[mine],
            at(a, block, other),
        ).start()

        @pl.when(i < n_w - 1)
        def _():
            remote(
                att_out.at[block, scaled(core, rows), :],
                att_in.at[mine],
                att_s.at[block, 1],
                att_r.at[mine],
                at(a, block, core),
            ).start()

        @pl.when(i < n_a - 1)
        def _():
            w_exchange(1, jnp.where(i == 0, mate(1), jnp.where(i == 1, mate(2), mate(3))))

        @pl.when(i == 0)
        def _():
            w_corner(0, mate(1))

        @pl.when(i == 2)
        def _():
            w_corner(0, mate(2))

        @pl.when(i == 3)
        def _():
            w_pass(0, mate(3))


    att_in[core * n_w + w] = att_out[w, scaled(core, rows), :]
    local_copies[2].wait()
    local_copies[3].wait()
    landed(out_full.at[other], pair_r.at[0], pair_s.at[0])
    for core_ in (core, other):
        for frm in (w, *w_peers):
            if frm is w and core_ is core:
                continue
            frm_slot = core_ * n_w + frm
            landed(att_in.at[frm_slot], att_r.at[frm_slot], att_s.at[frm, 0])

    tile = 256

    @pl.loop(0, D // tile)
    def _(t):
        cols = scaled(t, tile)
        total = None
        for g in range(2):
            lhs = jnp.concatenate([att_in[g * n_w + k] for k in range(n_w)], -1)
            add = jnp.dot(lhs, out_full[g, :, cols], preferred_element_type=F32)
            add = add.astype(BF16).astype(F32)
            total = add if total is None else total + add
        mixed[:, cols] = total

    step = 32

    @pl.loop(0, rows // step)
    def _(t):
        r = scaled(t, step)
        toks[a, 0, r, :] = layer_norm(
            ALPHA * res[r, :].astype(F32) + mixed[r, :], gain1[...], bias1[...]
        ).astype(BF16)

    def tok_send(b, dest, way):
        remote(
            toks.at[b, 0], toks.at[b, 0], tz_s.at[b, way], tz_r.at[b], at(dest, w, core)
        ).start()

    def tok_pair(b):
        remote(toks.at[b, 0], toks.at[b, 1], pair_s.at[1 + b], pair_r.at[1 + b], sibling).start()

    @pl.when(a < last)
    def _():
        tok_send(a, a + 1, 0)

    @pl.when(a > 0)
    def _():
        tok_send(a, a - 1, 1)

    tok_pair(a)

    def relay(k):
        b = order(k)
        landed(toks.at[b, 0], tz_r.at[b], tz_s.at[b, 0])

        @pl.when((b > a) & (a > 0))
        def _():
            tok_send(b, a - 1, 1)

        @pl.when((b < a) & (a < last))
        def _():
            tok_send(b, a + 1, 0)

        tok_pair(b)

    def up_part(k):
        b = order(k)
        landed(toks.at[b, 1], pair_r.at[1 + b], pair_s.at[1 + b])

        @pl.loop(0, up_cols // tile)
        def _(t):
            cols = scaled(t, tile)
            acts = jnp.dot(
                toks[b].reshape(tok_rows, D), up[:, cols], preferred_element_type=F32
            )
            hid[b, :, cols] = jnp.square(jnp.maximum(acts, 0.0)).astype(BF16)

    groups = n_a
    g_cols = D // groups

    def piece(ref, g):
        return ref.at[:, scaled(g, g_cols)]

    def group_of(b, k):
        return jnp.where(b > a, turn(k), n_a - 1 - turn(k))

    def down_part(b, g):
        @pl.loop(0, g_cols // tile)
        def _(t):
            cols = scaled(g * (g_cols // tile) + t, tile)
            acts = jnp.dot(hid[b], down[:, cols], preferred_element_type=F32)
            part[b, :, cols] = acts[:rows]
            sib_out[b, :, cols] = acts[rows:].astype(BF16)

        remote(
            piece(sib_out.at[b], g),
            piece(sib_in.at[b], g),
            sib_s.at[b, g],
            sib_r.at[b, g],
            sibling,
        ).start()

    def pass_on(b, g):
        cols = scaled(g, g_cols)
        landed(piece(sib_in.at[b], g), sib_r.at[b, g], sib_s.at[b, g])

        @pl.when(low > 0)
        def _():
            landed(piece(rs_in.at[b], g), rs_r.at[b, g], rs_s.at[b, g])

        @pl.loop(0, rows // step)
        def _(t):
            r = scaled(t, step)
            total = part[b, r, cols] + sib_in[b, r, cols].astype(F32)
            total = jnp.where(low > 0, total + rs_in[b, r, cols].astype(F32), total)
            rs_out[b, r, cols] = total.astype(BF16)

        p = a + jnp.where(b > a, 1, -1)
        slot = jnp.where((b == p) & (p < a), n_a, b)
        remote(
            piece(rs_out.at[b], g),
            piece(rs_in.at[slot], g),
            rs_s.at[b, g],
            rs_r.at[slot, g],
            at(p, w, core),
        ).start()

    def early(k):
        w_finish(1, mate(k))
        down_part(a + toward, mate(k))
        pass_on(a + toward, mate(k))

    w_pass(1, mate(1))
    w_pass(1, mate(2))
    w_corner(0, mate(3))
    w_corner(1, mate(1))
    w_complete(0)
    up_part(0)
    w_pass(1, mate(3))
    relay(1)

    @pl.when(low > 0)
    def _():
        relay(2)

    w_corner(1, mate(2))
    up_part(1)

    @pl.when(low == 0)
    def _():
        early(0)
        early(1)

    @pl.when(low > 0)
    def _():
        up_part(2)

    w_corner(1, mate(3))

    @pl.when(low == 0)
    def _():
        early(2)
        relay(2)
        up_part(2)
        early(3)

    @pl.when(low > 0)
    def _():
        relay(3)
        up_part(3)
        w_complete(1)

    def target(i):
        paired = (low > 0) & (i >= groups)
        later = jnp.where(i % 2 == 0, a + 2 * toward, a - toward)
        b = jnp.where(paired, later, a + toward)
        b = jnp.where(low > 0, b, a + toward * (2 + i // groups))
        b = jnp.where(i < last * groups, b, a)
        k = jnp.where(paired & (i < last * groups), (i - groups) // 2, i % groups)
        return b, group_of(b, k)

    def active(i):
        return (low > 0) | (i < 2 * groups) | (i >= last * groups)

    @pl.loop(0, n_a * groups + 1)
    def _(i):
        @pl.when((low == 0) & (i == groups))
        def _():
            relay(3)
            up_part(3)

        @pl.when((i < n_a * groups) & active(i))
        def _():
            down_part(*target(i))

        @pl.when((i > 0) & (i <= last * groups) & active(i - 1))
        def _():
            pass_on(*target(i - 1))

    for g in range(groups):
        landed(piece(sib_in.at[a], g), sib_r.at[a, g], sib_s.at[a, g])

        @pl.when(a > 0)
        def _(g=g):
            landed(piece(rs_in.at[a], g), rs_r.at[a, g], rs_s.at[a, g])

        @pl.when(a < last)
        def _(g=g):
            landed(piece(rs_in.at[n_a], g), rs_r.at[n_a, g], rs_s.at[a, g])

    half = D // 2

    @pl.loop(0, rows // step)
    def _(t):
        r = scaled(t, step)
        total = part[a, r, :] + sib_in[a, r, :].astype(F32)
        total = jnp.where(a > 0, total + rs_in[a, r, :].astype(F32), total)
        total = jnp.where(a < last, total + rs_in[n_a, r, :].astype(F32), total)
        encoded = layer_norm(
            ALPHA * toks[a, 0, r, :].astype(F32) + total, gain2[...], bias2[...]
        )
        left, right = encoded[:, :half].astype(BF16), encoded[:, half:].astype(BF16)
        out[pl.ds(pl.multiple_of(core * rows + t * step, step), step), :] = jnp.where(
            core == 0, left, right
        )
        enc_out[r, :] = jnp.where(core == 0, right, left)

    swap = remote(enc_out, out.at[scaled(core, rows), :], pair_s.at[n_a + 1], pair_r.at[n_a + 1], sibling)
    swap.start()
    for j, peer in enumerate(w_peers):
        sent(packed.at[peer], qkv_s.at[j], qkv_r.at[j])
        for core_way in range(2):
            sent(att_out.at[peer, pl.ds(0, rows), :], att_s.at[peer, core_way], att_r.at[peer])
    sent(att_out.at[w, pl.ds(0, rows), :], att_s.at[w, 0], att_r.at[w])
    sent(out_own, pair_s.at[0], pair_r.at[0])
    for kind in range(2):
        w_drain(kind)
    for k in range(n_a):
        b = cyc(k)
        if k:
            for g in range(groups):
                sent(piece(rs_out.at[b], g), rs_s.at[b, g], rs_r.at[b, g])
        for g in range(groups):
            sent(piece(sib_out.at[b], g), sib_s.at[b, g], sib_r.at[b, g])
        sent(toks.at[b, 0], pair_s.at[1 + b], pair_r.at[1 + b])

        @pl.when((a < last) & (b <= a))
        def _():
            for w_ in range(n_w):
                sent(kv_slot(b, w_), kv_s.at[b, w_, 0], kv_r.at[b, w_])
            sent(toks.at[b, 0], tz_s.at[b, 0], tz_r.at[b])

        @pl.when((a > 0) & (b >= a))
        def _():
            for w_ in range(n_w):
                sent(kv_slot(b, w_), kv_s.at[b, w_, 1], kv_r.at[b, w_])
            sent(toks.at[b, 0], tz_s.at[b, 1], tz_r.at[b])

    swap.wait_send()
    landed(out.at[scaled(other, rows), :], pair_r.at[n_a + 1], pair_s.at[n_a + 1])


def fused(n_a, n_w, *args):
    (queries, keys, values, q_gain, key_norm_gain, out_weight, residual, *rest) = args
    ln1_gain, ln1_bias, up_weight, down_weight, ln2_gain, ln2_bias = rest
    tok_rows = queries.shape[0]
    rows = tok_rows // 2
    width = 2 * HEAD_SIZE
    up_cols = up_weight.shape[1] // n_a
    down_rows = down_weight.shape[0] // n_a
    dma, vmem = pltpu.SemaphoreType.DMA, pltpu.VMEM
    whole, hbm = pl.BlockSpec(memory_space=pltpu.VMEM), pl.BlockSpec(memory_space=pl.ANY)
    return pl.pallas_call(
        functools.partial(layer_kernel, n_a, n_w),
        out_shape=jax.ShapeDtypeStruct((tok_rows, D // 2), BF16),
        in_specs=[whole] * 5 + [hbm] * 4 + [whole] * 4,
        out_specs=whole,
        scratch_shapes=[
            vmem((n_w, tok_rows, 2 * width), BF16),
            vmem((n_w, tok_rows, 2 * width), BF16),
            vmem((n_a, n_w * tok_rows, width), BF16),
            vmem((n_a, n_w * tok_rows, width), BF16),
            vmem((n_w, 2, tok_rows, width), BF16),
            vmem((n_w, tok_rows, width), BF16),
            vmem((2 * n_w, rows, width), BF16),
            vmem((2, *out_weight.shape), BF16),
            vmem((rows, D), BF16),
            vmem((rows, D), F32),
            vmem((D, up_cols), BF16),
            vmem((down_rows, D), BF16),
            vmem((n_a, 2, rows, D), BF16),
            vmem((n_a, tok_rows, up_cols), BF16),
            vmem((n_a, rows, D), F32),
            vmem((n_a, rows, D), BF16),
            vmem((n_a, rows, D), BF16),
            vmem((n_a, rows, D), BF16),
            vmem((n_a + 1, rows, D), BF16),
            vmem((rows, D // 2), BF16),
            dma((4,)),
            dma((n_w - 1,)),
            dma((n_w - 1,)),
            dma((n_a, n_w, 2)),
            dma((n_a, n_w)),
            dma((n_w, 2)),
            dma((2 * n_w,)),
            dma((2, n_a)),
            dma((2, n_a)),
            dma((2, n_a, 2)),
            dma((2, n_a, 2)),
            dma((2, n_a, 2)),
            dma((2, n_a, 2)),
            dma((n_a, 2)),
            dma((n_a,)),
            dma((n_a + 2,)),
            dma((n_a + 2,)),
            dma((n_a, n_a)),
            dma((n_a, n_a)),
            dma((n_a, n_a)),
            dma((n_a + 1, n_a)),
        ],
        compiler_params=pltpu.CompilerParams(
            collective_id=0, has_side_effects=True, vmem_limit_bytes=60 * 2**20
        ),
    )(
        queries,
        keys,
        values,
        q_gain.reshape(1, HEAD_SIZE),
        key_norm_gain.reshape(1, HEAD_SIZE),
        up_weight,
        down_weight,
        out_weight,
        residual,
        *(v.reshape(1, D) for v in (ln1_gain, ln1_bias, ln2_gain, ln2_bias)),
    )


def solution(mesh):
    n_sp, n_tp = mesh.shape["sp"], mesh.shape["tp"]

    def layer(queries, keys, *others):
        n_a = math.gcd(n_sp, keys.shape[1] // (HEAD_SIZE * n_tp))
        n_w = n_sp // n_a
        sp = ("a", "w")
        if n_tp == 2 and n_w == n_a == 4 and keys.shape[1] == n_w * HEAD_SIZE * n_tp:
            cut = P("sp", "tp")
            return jax.shard_map(
                functools.partial(fused, n_a, n_w),
                mesh=mesh,
                in_specs=(cut, cut, cut, P(), P(), P("tp", None), P("sp", None), P(), P())
                + (cut, P("tp", "sp"), P(), P()),
                out_specs=cut,
                check_vma=False,
            )(queries, keys, *others)
        groups = Mesh(mesh.devices.reshape(n_a, n_w, n_tp), ("a", "w", "tp"))
        cut = P(sp, "tp")
        return jax.shard_map(
            local,
            mesh=groups,
            in_specs=(cut, cut, cut, P(), P(), P("tp", None), P(sp, None), P(), P())
            + (cut, P("tp", sp), P(), P()),
            out_specs=cut,
            check_vma=False,
        )(queries, keys, *others)

    return layer
```

```python
import functools
import math

import jax
import jax.numpy as jnp
from jax import lax
from jax.experimental import pallas as pl
from jax.experimental.pallas import tpu as pltpu
from jax.sharding import Mesh, PartitionSpec as P

D = 2048
HEAD_SIZE = 64
GRID_W = 64


ALPHA = 8.0**0.25
ROTARY_BASE = 10000.0
RMS_EPSILON = 1e-06
NORM_EPSILON = 1e-05


def rotate_grid(heads_in, grid_places):
    half_dim = heads_in.shape[-1] // 2
    quarter = half_dim // 2
    inverse = ROTARY_BASE ** (-jnp.arange(quarter, dtype=jnp.float32) / quarter)

    def spin(segment, coords):
        angles = coords.astype(jnp.float32)[:, None] * inverse[None, :]
        cos_val = jnp.cos(angles)[:, None, :]
        sin_val = jnp.sin(angles)[:, None, :]
        lead_half = segment[..., :quarter]
        tail_half = segment[..., quarter:]
        return jnp.concatenate(
            [lead_half * cos_val - tail_half * sin_val, tail_half * cos_val + lead_half * sin_val],
            -1,
        )

    return jnp.concatenate(
        [
            spin(heads_in[..., :half_dim], grid_places // GRID_W),
            spin(heads_in[..., half_dim:], grid_places % GRID_W),
        ],
        -1,
    )


def prepare_inputs(heads_in, gain_vec, grid_places, factor):
    values32 = heads_in.astype(jnp.float32)
    normed = (
        values32
        * lax.rsqrt(jnp.mean(values32 * values32, -1, keepdims=True) + RMS_EPSILON)
        * gain_vec
    )
    return (rotate_grid(normed, grid_places) * factor).astype(jnp.bfloat16)


def layer_norm(pre_norm, gain_vec, bias_vec):
    row_mean = jnp.mean(pre_norm, -1, keepdims=True)
    centred = pre_norm - row_mean
    spread = jnp.mean(centred * centred, -1, keepdims=True)
    return centred * lax.rsqrt(spread + NORM_EPSILON) * gain_vec + bias_vec


def line_gather(block, axis):
    n, me = lax.axis_size(axis), lax.axis_index(axis)
    up = [(i, i + 1) for i in range(n - 1)]
    down = [(i + 1, i) for i in range(n - 1)]
    from_left, from_right = [block], [block]
    for _ in range(n - 1):
        from_left.append(lax.ppermute(from_left[-1], axis, up))
        from_right.append(lax.ppermute(from_right[-1], axis, down))
    stacked = jnp.zeros((n, *block.shape), block.dtype)
    for k in range(n):
        piece = block if k == 0 else jnp.where(me >= k, from_left[k], from_right[n - k])
        stacked = lax.dynamic_update_index_in_dim(stacked, piece, (me - k + n) % n, 0)
    return stacked


def swap_blocks(blocks, axis):
    n, me = lax.axis_size(axis), lax.axis_index(axis)
    stacked = jnp.zeros_like(blocks)
    for k in range(n):
        piece = lax.dynamic_index_in_dim(blocks, (me + k) % n, 0, keepdims=False)
        if k:
            piece = lax.ppermute(piece, axis, [(i, (i + k) % n) for i in range(n)])
        stacked = lax.dynamic_update_index_in_dim(stacked, piece, (me - k + n) % n, 0)
    return stacked


def turn_cols(block, outer, inner):
    width = block.shape[1] // (outer * inner)
    starts = [(o * inner + i) * width for i in range(inner) for o in range(outer)]
    return jnp.concatenate([block[:, c : c + width] for c in starts], -1)


def attend_kernel(chunk, q_ref, kv_ref, out_ref, vals_ref):
    width = 2 * HEAD_SIZE
    key_count = kv_ref.shape[0]
    rows = q_ref.shape[0]

    @pl.when(pl.program_id(1) == 0)
    def _():
        lane_kv = lax.broadcasted_iota(jnp.int32, (chunk, width), 1)

        @pl.loop(0, key_count // chunk)
        def _(c):
            at = pl.ds(pl.multiple_of(c * chunk, chunk), chunk)
            vals_ref[at, :] = jnp.where(
                lane_kv < HEAD_SIZE, 1.0, kv_ref[at, :].astype(jnp.float32)
            ).astype(jnp.bfloat16)

    lane = lax.broadcasted_iota(jnp.int32, (rows, width), 1)
    both = q_ref[...].astype(jnp.float32)
    results = []
    for head in range(2):
        own = both if head == 0 else pltpu.roll(both, HEAD_SIZE, 1)
        q = jnp.where(lane < HEAD_SIZE, own, 0.0).astype(jnp.bfloat16)
        top = None
        for c in range(key_count // chunk):
            at = pl.ds(c * chunk, chunk)
            scores = lax.dot_general(
                q, kv_ref[at, :], (((1,), (1,)), ((), ())), preferred_element_type=jnp.float32
            )
            peak = jnp.max(scores, -1, keepdims=True)
            new_top = peak if top is None else jnp.maximum(top, peak)
            weights = jnp.exp(scores - new_top).astype(jnp.bfloat16)
            part = jnp.dot(weights, vals_ref[at, :], preferred_element_type=jnp.float32)
            total = part if top is None else total * jnp.exp(top - new_top) + part
            top = new_top
        results.append(total)
    first, second = (t / pltpu.roll(t, HEAD_SIZE, 1) for t in results)
    out_ref[...] = jnp.where(
        lane < HEAD_SIZE, pltpu.roll(first, HEAD_SIZE, 1), second
    ).astype(jnp.bfloat16)


def attend(q, kv, block=256, chunk=2048):
    heads, rows, width = q.shape
    key_count = kv.shape[1]
    block, chunk = math.gcd(rows, block), math.gcd(key_count, chunk)
    return pl.pallas_call(
        functools.partial(attend_kernel, chunk),
        grid=(heads, rows // block),
        in_specs=[
            pl.BlockSpec((None, block, width), lambda h, i: (h, i, 0)),
            pl.BlockSpec((None, key_count, width), lambda h, i: (h, 0, 0)),
        ],
        out_specs=pl.BlockSpec((None, block, width), lambda h, i: (h, i, 0)),
        out_shape=jax.ShapeDtypeStruct(q.shape, jnp.bfloat16),
        scratch_shapes=[pltpu.VMEM((key_count, width), jnp.bfloat16)],
        compiler_params=pltpu.CompilerParams(dimension_semantics=("arbitrary", "arbitrary")),
        cost_estimate=pl.CostEstimate(
            flops=heads * rows * key_count * 16 * HEAD_SIZE,
            bytes_accessed=2 * (2 * q.size + kv.size),
            transcendentals=heads * rows * key_count * 2,
        ),
    )(q, kv)


def local(
    queries,
    keys,
    values,
    q_gain,
    key_norm_gain,
    out_weight,
    residual,
    ln1_gain,
    ln1_bias,
    up_weight,
    down_weight,
    ln2_gain,
    ln2_bias,
):
    tok_rows = queries.shape[0]
    n_a, n_tp = lax.axis_size("a"), lax.axis_size("tp")
    grid_places = lax.axis_index(("a", "w")) * tok_rows + jnp.arange(tok_rows, dtype=jnp.int32)
    kv_heads = keys.shape[1] // HEAD_SIZE
    q_count = queries.shape[1] // HEAD_SIZE
    own_heads = kv_heads // n_a
    query_rows = prepare_inputs(
        queries.reshape(tok_rows, q_count, HEAD_SIZE), q_gain, grid_places, HEAD_SIZE ** (-0.5)
    ).reshape(tok_rows, kv_heads, 2 * HEAD_SIZE)
    key_rows = prepare_inputs(
        keys.reshape(tok_rows, kv_heads, HEAD_SIZE), key_norm_gain, grid_places, 1.0
    )
    value_rows = values.reshape(tok_rows, kv_heads, HEAD_SIZE)
    packed = jnp.concatenate([query_rows, key_rows, value_rows], -1)
    packed = jnp.transpose(packed, (1, 0, 2)).reshape(n_a, own_heads, tok_rows, 4 * HEAD_SIZE)
    packed = lax.all_to_all(packed, "a", 0, 0, tiled=True)
    packed = jnp.transpose(packed, (1, 0, 2, 3)).reshape(
        own_heads, n_a * tok_rows, 4 * HEAD_SIZE
    )
    q = packed[..., : 2 * HEAD_SIZE]
    kv = lax.all_gather(packed[..., 2 * HEAD_SIZE :], "w", axis=1, tiled=True)
    kv, down_weight = lax.optimization_barrier((kv, down_weight))

    out_full = line_gather(out_weight, "tp").reshape(-1, D)
    up_own = lax.all_to_all(up_weight, "a", 1, 0, tiled=True)
    up_full = lax.all_gather(up_own, "w", axis=0, tiled=True)
    down_own = swap_blocks(down_weight.reshape(n_a, -1, down_weight.shape[1]), "a")
    down_own = down_own.swapaxes(0, 1).reshape(down_weight.shape[0] // n_a, -1)

    attended = attend(q, kv)
    rows = tok_rows // n_tp
    sent = attended.reshape(own_heads, n_a * n_tp, rows, 2 * HEAD_SIZE)
    sent = jnp.transpose(sent, (1, 0, 2, 3))
    got = lax.all_to_all(sent, ("a", "tp"), 0, 0, tiled=True)
    got, down_own = lax.optimization_barrier((got, down_own))
    down_full = lax.all_gather(down_own, "w", axis=0)
    got = got.reshape(n_a, n_tp, own_heads, rows, 2 * HEAD_SIZE)
    group_cols = jnp.transpose(got, (1, 3, 0, 2, 4)).reshape(n_tp, rows, -1)
    out_groups = out_full.reshape(2, -1, D)
    both = jnp.transpose(group_cols, (1, 0, 2)).reshape(rows, 2, -1)
    mixed = sum(
        jnp.dot(both[:, g], out_groups[g], preferred_element_type=jnp.float32)
        .astype(jnp.bfloat16)
        .astype(jnp.float32)
        for g in range(2)
    )
    own_residual = lax.dynamic_slice_in_dim(residual, lax.axis_index("tp") * rows, rows, 0)
    normed = layer_norm(
        ALPHA * own_residual.astype(jnp.float32) + mixed, ln1_gain, ln1_bias
    ).astype(jnp.bfloat16)
    n_w = lax.axis_size("w")
    turned = turn_cols(normed, n_a, n_w)
    full_rows = line_gather(line_gather(turned, "a"), "tp").reshape(-1, D)
    up_acts = jnp.dot(full_rows, up_full, preferred_element_type=jnp.float32)
    hidden = jnp.square(jnp.maximum(up_acts, 0.0)).astype(jnp.bfloat16)
    partial_ffn = jnp.concatenate(
        [
            jnp.dot(hidden, down_full[i], preferred_element_type=jnp.float32).astype(jnp.bfloat16)
            for i in range(down_full.shape[0])
        ],
        -1,
    )
    ffn_out = lax.psum_scatter(partial_ffn, "tp", scatter_dimension=0, tiled=True)
    ffn_out = lax.psum_scatter(ffn_out, "a", scatter_dimension=0, tiled=True)
    ffn_out = (
        ffn_out.reshape(rows, n_w, n_a, -1).swapaxes(1, 2).reshape(rows, D).astype(jnp.float32)
    )
    encoded = layer_norm(
        ALPHA * normed.astype(jnp.float32) + ffn_out, ln2_gain, ln2_bias
    ).astype(jnp.bfloat16)
    return lax.all_to_all(encoded, "tp", 1, 0, tiled=True)


MESH = pl.DeviceIdType.MESH
BF16, F32 = jnp.bfloat16, jnp.float32


def scaled(index, size):
    return pl.ds(pl.multiple_of(index * size, size), size)


def layer_kernel(
    n_a,
    n_w,
    q_in,
    k_in,
    v_in,
    q_gain,
    k_gain,
    up_own,
    down_own,
    out_own,
    res_all,
    gain1,
    bias1,
    gain2,
    bias2,
    out,
    packed,
    qkv,
    kv,
    vals,
    q_held,
    att_out,
    att_in,
    out_full,
    res,
    mixed,
    up,
    down,
    toks,
    hid,
    part,
    sib_out,
    sib_in,
    rs_out,
    rs_in,
    enc_out,
    loc_sem,
    qkv_s,
    qkv_r,
    kv_s,
    kv_r,
    att_s,
    att_r,
    wz_s,
    wz_r,
    wf_s,
    wf_r,
    wd_s,
    wd_r,
    tz_s,
    tz_r,
    pair_s,
    pair_r,
    sib_s,
    sib_r,
    rs_s,
    rs_r,
):
    place, core = lax.axis_index("sp"), lax.axis_index("tp")
    a, w = place // n_w, place % n_w
    other = 1 - core
    x_side = w + 1 - 2 * (w % 2)
    y_side = w + 2 - 4 * (w // 2)
    sides = (x_side, y_side)
    rows = toks.shape[2]
    tok_rows = 2 * rows
    width = 2 * HEAD_SIZE
    up_rows, up_cols = up_own.shape[0], up.shape[1]
    down_rows, down_cols = down.shape[0], down_own.shape[1]

    def at(a_, w_, core_):
        return (a_ * n_w + w_, core_)

    sibling = at(a, w, other)

    def remote(src, dst, send, recv, target):
        return pltpu.make_async_remote_copy(
            src_ref=src,
            dst_ref=dst,
            send_sem=send,
            recv_sem=recv,
            device_id=target,
            device_id_type=MESH,
        )

    def landed(dst, recv, send):
        remote(dst, dst, send, recv, sibling).wait_recv()

    def sent(src, send, recv):
        remote(src, src, send, recv, sibling).wait_send()

    def cyc(k):
        return lax.rem(a + k + 2 * n_a, n_a)

    turns = (0, 1, 2, 3)
    mates = [a, a + 1 - 2 * (a % 2), a + 2 - 4 * (a // 2), n_a - 1 - a]

    def mate(k):
        return mates[turns[k]]

    def turn(k):
        found = turns[0]
        for j in range(1, n_a):
            found = jnp.where(k == j, turns[j], found)
        return found

    def w_slot(kind, a_, w_):
        if kind == 0:
            return up.at[scaled(a_ * n_w + w_, up_rows), :]
        return down.at[:, scaled(a_ * n_w + w_, down_cols)]

    def w_half(kind, a_, w_, h):
        if kind == 0:
            half = up_rows // 2
            return up.at[scaled((a_ * n_w + w_) * 2 + h, half), :]
        half = down_rows // 2
        return down.at[pl.ds(h * half, half), scaled(a_ * n_w + w_, down_cols)]

    def w_src(kind, a_):
        if kind == 0:
            return up_own.at[:, scaled(a_, up_cols)]
        return down_own.at[scaled(a_, down_rows), :]

    def w_exchange(kind, to):
        remote(
            w_src(kind, to),
            w_slot(kind, a, w),
            wz_s.at[kind, to],
            wz_r.at[kind, a],
            at(to, w, core),
        ).start()

    def w_forward(kind, frm):
        for j in range(2):
            remote(
                w_slot(kind, frm, w),
                w_slot(kind, frm, w),
                wf_s.at[kind, frm, j],
                wf_r.at[kind, frm, j],
                at(a, sides[j], core),
            ).start()

    def w_arrive(kind, frm):
        landed(w_slot(kind, frm, w), wz_r.at[kind, frm], wz_s.at[kind, frm])

    def w_pass(kind, frm):
        w_arrive(kind, frm)
        w_forward(kind, frm)

    def w_corner(kind, frm):
        for j in range(2):
            landed(w_slot(kind, frm, sides[j]), wf_r.at[kind, frm, j], wf_s.at[kind, frm, j])
            part_ref = w_half(kind, frm, sides[j], j)
            remote(
                part_ref,
                part_ref,
                wd_s.at[kind, frm, j],
                wd_r.at[kind, frm, j],
                at(a, sides[1 - j], core),
            ).start()

    def w_finish(kind, frm):
        for j in range(2):
            landed(
                w_half(kind, frm, n_w - 1 - w, j), wd_r.at[kind, frm, j], wd_s.at[kind, frm, j]
            )

    def w_complete(kind):
        for k in range(n_a):
            w_finish(kind, mate(k))

    def w_drain(kind):
        for k in range(1, n_a):
            to = mate(k)
            sent(w_src(kind, to), wz_s.at[kind, to], wz_r.at[kind, to])
        for k in range(n_a):
            frm = mate(k)
            for j in range(2):
                sent(w_slot(kind, frm, w), wf_s.at[kind, frm, j], wf_r.at[kind, frm, j])
                sent(w_half(kind, frm, sides[j], j), wd_s.at[kind, frm, j], wd_r.at[kind, frm, j])

    local_copies = [
        pltpu.make_async_copy(up_own.at[:, scaled(a, up_cols)], w_slot(0, a, w), loc_sem.at[0]),
        pltpu.make_async_copy(
            down_own.at[scaled(a, down_rows), :], w_slot(1, a, w), loc_sem.at[1]
        ),
        pltpu.make_async_copy(out_own, out_full.at[core], loc_sem.at[2]),
        pltpu.make_async_copy(res_all.at[scaled(core, rows), :], res, loc_sem.at[3]),
    ]
    for copy in local_copies:
        copy.start()

    barrier = pltpu.get_barrier_semaphore()
    w_peers = (x_side, y_side, n_w - 1 - w)
    peers = [at(cyc(k), w, core) for k in range(1, n_a)] + [sibling]
    peers += [at(a, side, core_) for side in w_peers for core_ in (core, other)]
    for peer in peers:
        pl.semaphore_signal(barrier, inc=1, device_id=peer, device_id_type=MESH)
    pl.semaphore_wait(barrier, len(peers))

    w_exchange(0, mate(1))
    remote(out_own, out_full.at[core], pair_s.at[0], pair_r.at[0], sibling).start()

    half_head, quarter = HEAD_SIZE // 2, HEAD_SIZE // 4
    lane = lax.broadcasted_iota(jnp.int32, (tok_rows, width), 1)
    token = lax.broadcasted_iota(jnp.int32, (tok_rows, width), 0) + place * tok_rows
    coord = jnp.where(lane % HEAD_SIZE < half_head, token // GRID_W, token % GRID_W)
    power = (lane % quarter).astype(F32) * (-math.log(ROTARY_BASE) / quarter)
    angle = coord.astype(F32) * jnp.exp(power)
    tail = lane % half_head >= quarter
    cos_val, sin_val = jnp.cos(angle), jnp.sin(angle)
    sin_val = jnp.where(tail, sin_val, -sin_val)
    first_head = lane < HEAD_SIZE

    def prepared(group, gain):
        squares = group * group
        low_sum = jnp.sum(jnp.where(first_head, squares, 0.0), -1, keepdims=True)
        high_sum = jnp.sum(jnp.where(first_head, 0.0, squares), -1, keepdims=True)
        mean = jnp.where(first_head, low_sum, high_sum) * (1.0 / HEAD_SIZE)
        unit = group * lax.rsqrt(mean + RMS_EPSILON) * gain
        partner = jnp.where(
            tail, pltpu.roll(unit, quarter, 1), pltpu.roll(unit, width - quarter, 1)
        )
        return unit * cos_val + partner * sin_val

    q_both, k_both = (jnp.concatenate([g[...], g[...]], -1) for g in (q_gain, k_gain))
    for h in range(n_w):
        q_group = q_in[:, h * width : (h + 1) * width].astype(F32)
        packed[h, :, :width] = (
            prepared(q_group, q_both) * (HEAD_SIZE ** (-0.5))
        ).astype(BF16)
    for h in range(0, n_w, 2):
        cols = slice(h // 2 * width, (h // 2 + 1) * width)
        k_group = prepared(k_in[:, cols].astype(F32), k_both)
        v_group = v_in[:, cols].astype(F32)
        packed[h, :, width:] = jnp.where(
            first_head, k_group, pltpu.roll(v_group, HEAD_SIZE, 1)
        ).astype(BF16)
        packed[h + 1, :, width:] = jnp.where(
            first_head, pltpu.roll(k_group, HEAD_SIZE, 1), v_group
        ).astype(BF16)

    for j, peer in enumerate(w_peers):
        remote(
            packed.at[peer], qkv.at[w], qkv_s.at[j], qkv_r.at[j], at(a, peer, core)
        ).start()
    local_copies[0].wait()
    w_forward(0, a)
    local_copies[1].wait()
    w_forward(1, a)
    qkv[w] = packed[w]

    last = n_a - 1
    low = jnp.minimum(a, last - a)
    toward = jnp.where(2 * a < n_a, 1, -1)

    def order(k):
        near = a + toward * jnp.where(k % 2 == 1, 1, -1) * ((k + 1) // 2)
        return jnp.where(k <= 2 * low, near, a + toward * (k - low))

    def kv_slot(b, w_):
        return kv.at[b, scaled(w_, tok_rows), :]

    def kv_send(src, b, w_, dest, way):
        remote(
            src, kv_slot(b, w_), kv_s.at[b, w_, way], kv_r.at[b, w_], at(dest, w, core)
        ).start()

    for j, frm in enumerate((w, *w_peers)):
        if j:
            landed(qkv.at[frm], qkv_r.at[j - 1], qkv_s.at[j - 1])
        mine = qkv.at[frm, :, pl.ds(width, width)]

        @pl.when(a < last)
        def _(mine=mine, frm=frm):
            kv_send(mine, a, frm, a + 1, 0)

        @pl.when(a > 0)
        def _(mine=mine, frm=frm):
            kv_send(mine, a, frm, a - 1, 1)

        kv[a, scaled(frm, tok_rows), :] = qkv[frm, :, width:]
        both = qkv[frm, :, :width].astype(F32)
        for head in range(2):
            own = both if head == 0 else pltpu.roll(both, HEAD_SIZE, 1)
            q_held[frm, head] = jnp.where(first_head, own, 0.0).astype(BF16)

    def kv_relay(k):
        b = order(k)

        @pl.loop(0, n_w)
        def _(w_):
            landed(kv_slot(b, w_), kv_r.at[b, w_], kv_s.at[b, w_, 0])

            @pl.when((b > a) & (a > 0))
            def _():
                kv_send(kv_slot(b, w_), b, w_, a - 1, 1)

            @pl.when((b < a) & (a < last))
            def _():
                kv_send(kv_slot(b, w_), b, w_, a + 1, 0)

    w_exchange(0, mate(2))
    kv_relay(1)
    w_pass(0, mate(1))
    kv_relay(2)
    w_corner(0, a)
    kv_relay(3)
    w_exchange(0, mate(3))
    w_corner(1, a)
    w_pass(0, mate(2))
    @pl.loop(0, n_a)
    def _(b):
        @pl.loop(0, n_w)
        def _(w_):
            r = scaled(w_, tok_rows)
            vals[b, r, :] = jnp.where(first_head, 1.0, kv[b, r, :].astype(F32)).astype(BF16)

    chunks = 2
    per = n_a // chunks

    @pl.loop(0, n_w)
    def _(i):
        block = lax.rem(w + 1 + i, n_w)
        results = []
        for head in range(2):
            top = None
            for c in range(chunks):
                planes = pl.ds(c * per, per)
                scores = lax.dot_general(
                    q_held[block, head],
                    kv[planes].reshape(-1, width),
                    (((1,), (1,)), ((), ())),
                    preferred_element_type=F32,
                )
                peak = jnp.max(scores, -1, keepdims=True)
                new_top = peak if top is None else jnp.maximum(top, peak)
                weights = jnp.exp(scores - new_top).astype(BF16)
                add = jnp.dot(
                    weights, vals[planes].reshape(-1, width), preferred_element_type=F32
                )
                total = add if top is None else total * jnp.exp(top - new_top) + add
                top = new_top
            results.append(total)
        first, second = (t / pltpu.roll(t, HEAD_SIZE, 1) for t in results)
        att_out[block] = jnp.where(
            first_head, pltpu.roll(first, HEAD_SIZE, 1), second
        ).astype(BF16)
        mine = core * n_w + w
        remote(
            att_out.at[block, scaled(other, rows), :],
            att_in.at[mine],
            att_s.at[block, 0],
            att_r.at[mine],
            at(a, block, other),
        ).start()

        @pl.when(i < n_w - 1)
        def _():
            remote(
                att_out.at[block, scaled(core, rows), :],
                att_in.at[mine],
                att_s.at[block, 1],
                att_r.at[mine],
                at(a, block, core),
            ).start()

        @pl.when(i < n_a - 1)
        def _():
            w_exchange(1, jnp.where(i == 0, mate(1), jnp.where(i == 1, mate(2), mate(3))))

        @pl.when(i == 0)
        def _():
            w_corner(0, mate(1))

        @pl.when(i == 2)
        def _():
            w_corner(0, mate(2))

        @pl.when(i == 3)
        def _():
            w_pass(0, mate(3))


    att_in[core * n_w + w] = att_out[w, scaled(core, rows), :]
    local_copies[2].wait()
    local_copies[3].wait()
    landed(out_full.at[other], pair_r.at[0], pair_s.at[0])
    for core_ in (core, other):
        for frm in (w, *w_peers):
            if frm is w and core_ is core:
                continue
            frm_slot = core_ * n_w + frm
            landed(att_in.at[frm_slot], att_r.at[frm_slot], att_s.at[frm, 0])

    tile = 256

    @pl.loop(0, D // tile)
    def _(t):
        cols = scaled(t, tile)
        total = None
        for g in range(2):
            lhs = jnp.concatenate([att_in[g * n_w + k] for k in range(n_w)], -1)
            add = jnp.dot(lhs, out_full[g, :, cols], preferred_element_type=F32)
            add = add.astype(BF16).astype(F32)
            total = add if total is None else total + add
        mixed[:, cols] = total

    step = 32

    @pl.loop(0, rows // step)
    def _(t):
        r = scaled(t, step)
        toks[a, 0, r, :] = layer_norm(
            ALPHA * res[r, :].astype(F32) + mixed[r, :], gain1[...], bias1[...]
        ).astype(BF16)

    def tok_send(b, dest, way):
        remote(
            toks.at[b, 0], toks.at[b, 0], tz_s.at[b, way], tz_r.at[b], at(dest, w, core)
        ).start()

    def tok_pair(b):
        remote(toks.at[b, 0], toks.at[b, 1], pair_s.at[1 + b], pair_r.at[1 + b], sibling).start()

    @pl.when(a < last)
    def _():
        tok_send(a, a + 1, 0)

    @pl.when(a > 0)
    def _():
        tok_send(a, a - 1, 1)

    tok_pair(a)

    def relay(k):
        b = order(k)
        landed(toks.at[b, 0], tz_r.at[b], tz_s.at[b, 0])

        @pl.when((b > a) & (a > 0))
        def _():
            tok_send(b, a - 1, 1)

        @pl.when((b < a) & (a < last))
        def _():
            tok_send(b, a + 1, 0)

        tok_pair(b)

    def up_part(k):
        b = order(k)
        landed(toks.at[b, 1], pair_r.at[1 + b], pair_s.at[1 + b])

        @pl.loop(0, up_cols // tile)
        def _(t):
            cols = scaled(t, tile)
            acts = jnp.dot(
                toks[b].reshape(tok_rows, D), up[:, cols], preferred_element_type=F32
            )
            hid[b, :, cols] = jnp.square(jnp.maximum(acts, 0.0)).astype(BF16)

    groups = n_a
    g_cols = D // groups

    def piece(ref, g):
        return ref.at[:, scaled(g, g_cols)]

    def group_of(b, k):
        return jnp.where(b > a, turn(k), n_a - 1 - turn(k))

    def down_part(b, g):
        @pl.loop(0, g_cols // tile)
        def _(t):
            cols = scaled(g * (g_cols // tile) + t, tile)
            acts = jnp.dot(hid[b], down[:, cols], preferred_element_type=F32)
            part[b, :, cols] = acts[:rows]
            sib_out[b, :, cols] = acts[rows:].astype(BF16)

        remote(
            piece(sib_out.at[b], g),
            piece(sib_in.at[b], g),
            sib_s.at[b, g],
            sib_r.at[b, g],
            sibling,
        ).start()

    def pass_on(b, g):
        cols = scaled(g, g_cols)
        landed(piece(sib_in.at[b], g), sib_r.at[b, g], sib_s.at[b, g])

        carried = (low > 0) & (b != a + 2 * toward)

        @pl.when(carried)
        def _():
            landed(piece(rs_in.at[b], g), rs_r.at[b, g], rs_s.at[b, g])

        @pl.loop(0, rows // step)
        def _(t):
            r = scaled(t, step)
            total = part[b, r, cols] + sib_in[b, r, cols].astype(F32)
            total = jnp.where(carried, total + rs_in[b, r, cols].astype(F32), total)
            rs_out[b, r, cols] = total.astype(BF16)

        across = b == a + last * toward
        p = jnp.where(across, b, a + jnp.where(b > a, 1, -1))
        slot = jnp.where((b == p) & (p < a), n_a, b)
        slot = jnp.where(across, n_a + 1, slot)
        remote(
            piece(rs_out.at[b], g),
            piece(rs_in.at[slot], g),
            rs_s.at[b, g],
            rs_r.at[slot, g],
            at(p, w, core),
        ).start()

    def early(k):
        w_finish(1, mate(k))
        down_part(a + toward, mate(k))
        pass_on(a + toward, mate(k))

    w_pass(1, mate(1))
    w_pass(1, mate(2))
    w_corner(0, mate(3))
    w_corner(1, mate(1))
    w_complete(0)
    up_part(0)
    w_pass(1, mate(3))
    relay(1)

    @pl.when(low > 0)
    def _():
        relay(2)

    w_corner(1, mate(2))
    up_part(1)

    @pl.when(low == 0)
    def _():
        early(0)
        early(1)

    @pl.when(low > 0)
    def _():
        up_part(2)

    w_corner(1, mate(3))

    @pl.when(low == 0)
    def _():
        early(2)
        relay(2)
        up_part(2)
        early(3)

    @pl.when(low > 0)
    def _():
        relay(3)
        up_part(3)
        w_complete(1)

    def target(i):
        turn_ = i // groups
        b = a + jnp.where(turn_ == 0, 2, jnp.where(turn_ == 1, -1, 1)) * toward
        b = jnp.where(low > 0, b, a + toward * (2 + turn_))
        b = jnp.where(i < last * groups, b, a)
        return b, group_of(b, i % groups)

    def active(i):
        return (low > 0) | (i < 2 * groups) | (i >= last * groups)

    @pl.loop(0, n_a * groups + 1)
    def _(i):
        @pl.when((low == 0) & (i == groups))
        def _():
            relay(3)
            up_part(3)

        @pl.when((i < n_a * groups) & active(i))
        def _():
            down_part(*target(i))

        @pl.when((i > 0) & (i <= last * groups) & active(i - 1))
        def _():
            pass_on(*target(i - 1))

    for g in range(groups):
        landed(piece(sib_in.at[a], g), sib_r.at[a, g], sib_s.at[a, g])

        @pl.when(a > 0)
        def _(g=g):
            landed(piece(rs_in.at[a], g), rs_r.at[a, g], rs_s.at[a, g])

        @pl.when(a < last)
        def _(g=g):
            landed(piece(rs_in.at[n_a], g), rs_r.at[n_a, g], rs_s.at[a, g])

        @pl.when(low == 0)
        def _(g=g):
            landed(piece(rs_in.at[n_a + 1], g), rs_r.at[n_a + 1, g], rs_s.at[a, g])

    half = D // 2

    @pl.loop(0, rows // step)
    def _(t):
        r = scaled(t, step)
        total = part[a, r, :] + sib_in[a, r, :].astype(F32)
        total = jnp.where(a > 0, total + rs_in[a, r, :].astype(F32), total)
        total = jnp.where(a < last, total + rs_in[n_a, r, :].astype(F32), total)
        total = jnp.where(low == 0, total + rs_in[n_a + 1, r, :].astype(F32), total)
        encoded = layer_norm(
            ALPHA * toks[a, 0, r, :].astype(F32) + total, gain2[...], bias2[...]
        )
        left, right = encoded[:, :half].astype(BF16), encoded[:, half:].astype(BF16)
        out[pl.ds(pl.multiple_of(core * rows + t * step, step), step), :] = jnp.where(
            core == 0, left, right
        )
        enc_out[r, :] = jnp.where(core == 0, right, left)

    swap = remote(enc_out, out.at[scaled(core, rows), :], pair_s.at[n_a + 1], pair_r.at[n_a + 1], sibling)
    swap.start()
    for j, peer in enumerate(w_peers):
        sent(packed.at[peer], qkv_s.at[j], qkv_r.at[j])
        for core_way in range(2):
            sent(att_out.at[peer, pl.ds(0, rows), :], att_s.at[peer, core_way], att_r.at[peer])
    sent(att_out.at[w, pl.ds(0, rows), :], att_s.at[w, 0], att_r.at[w])
    sent(out_own, pair_s.at[0], pair_r.at[0])
    for kind in range(2):
        w_drain(kind)
    for k in range(n_a):
        b = cyc(k)
        if k:
            for g in range(groups):
                sent(piece(rs_out.at[b], g), rs_s.at[b, g], rs_r.at[b, g])
        for g in range(groups):
            sent(piece(sib_out.at[b], g), sib_s.at[b, g], sib_r.at[b, g])
        sent(toks.at[b, 0], pair_s.at[1 + b], pair_r.at[1 + b])

        @pl.when((a < last) & (b <= a))
        def _():
            for w_ in range(n_w):
                sent(kv_slot(b, w_), kv_s.at[b, w_, 0], kv_r.at[b, w_])
            sent(toks.at[b, 0], tz_s.at[b, 0], tz_r.at[b])

        @pl.when((a > 0) & (b >= a))
        def _():
            for w_ in range(n_w):
                sent(kv_slot(b, w_), kv_s.at[b, w_, 1], kv_r.at[b, w_])
            sent(toks.at[b, 0], tz_s.at[b, 1], tz_r.at[b])

    swap.wait_send()
    landed(out.at[scaled(other, rows), :], pair_r.at[n_a + 1], pair_s.at[n_a + 1])


def fused(n_a, n_w, *args):
    (queries, keys, values, q_gain, key_norm_gain, out_weight, residual, *rest) = args
    ln1_gain, ln1_bias, up_weight, down_weight, ln2_gain, ln2_bias = rest
    tok_rows = queries.shape[0]
    rows = tok_rows // 2
    width = 2 * HEAD_SIZE
    up_cols = up_weight.shape[1] // n_a
    down_rows = down_weight.shape[0] // n_a
    dma, vmem = pltpu.SemaphoreType.DMA, pltpu.VMEM
    whole, hbm = pl.BlockSpec(memory_space=pltpu.VMEM), pl.BlockSpec(memory_space=pl.ANY)
    return pl.pallas_call(
        functools.partial(layer_kernel, n_a, n_w),
        out_shape=jax.ShapeDtypeStruct((tok_rows, D // 2), BF16),
        in_specs=[whole] * 5 + [hbm] * 4 + [whole] * 4,
        out_specs=whole,
        scratch_shapes=[
            vmem((n_w, tok_rows, 2 * width), BF16),
            vmem((n_w, tok_rows, 2 * width), BF16),
            vmem((n_a, n_w * tok_rows, width), BF16),
            vmem((n_a, n_w * tok_rows, width), BF16),
            vmem((n_w, 2, tok_rows, width), BF16),
            vmem((n_w, tok_rows, width), BF16),
            vmem((2 * n_w, rows, width), BF16),
            vmem((2, *out_weight.shape), BF16),
            vmem((rows, D), BF16),
            vmem((rows, D), F32),
            vmem((D, up_cols), BF16),
            vmem((down_rows, D), BF16),
            vmem((n_a, 2, rows, D), BF16),
            vmem((n_a, tok_rows, up_cols), BF16),
            vmem((n_a, rows, D), F32),
            vmem((n_a, rows, D), BF16),
            vmem((n_a, rows, D), BF16),
            vmem((n_a, rows, D), BF16),
            vmem((n_a + 2, rows, D), BF16),
            vmem((rows, D // 2), BF16),
            dma((4,)),
            dma((n_w - 1,)),
            dma((n_w - 1,)),
            dma((n_a, n_w, 2)),
            dma((n_a, n_w)),
            dma((n_w, 2)),
            dma((2 * n_w,)),
            dma((2, n_a)),
            dma((2, n_a)),
            dma((2, n_a, 2)),
            dma((2, n_a, 2)),
            dma((2, n_a, 2)),
            dma((2, n_a, 2)),
            dma((n_a, 2)),
            dma((n_a,)),
            dma((n_a + 2,)),
            dma((n_a + 2,)),
            dma((n_a, n_a)),
            dma((n_a, n_a)),
            dma((n_a, n_a)),
            dma((n_a + 2, n_a)),
        ],
        compiler_params=pltpu.CompilerParams(
            collective_id=0, has_side_effects=True, vmem_limit_bytes=60 * 2**20
        ),
    )(
        queries,
        keys,
        values,
        q_gain.reshape(1, HEAD_SIZE),
        key_norm_gain.reshape(1, HEAD_SIZE),
        up_weight,
        down_weight,
        out_weight,
        residual,
        *(v.reshape(1, D) for v in (ln1_gain, ln1_bias, ln2_gain, ln2_bias)),
    )


def solution(mesh):
    n_sp, n_tp = mesh.shape["sp"], mesh.shape["tp"]

    def layer(queries, keys, *others):
        n_a = math.gcd(n_sp, keys.shape[1] // (HEAD_SIZE * n_tp))
        n_w = n_sp // n_a
        sp = ("a", "w")
        if n_tp == 2 and n_w == n_a == 4 and keys.shape[1] == n_w * HEAD_SIZE * n_tp:
            cut = P("sp", "tp")
            return jax.shard_map(
                functools.partial(fused, n_a, n_w),
                mesh=mesh,
                in_specs=(cut, cut, cut, P(), P(), P("tp", None), P("sp", None), P(), P())
                + (cut, P("tp", "sp"), P(), P()),
                out_specs=cut,
                check_vma=False,
            )(queries, keys, *others)
        groups = Mesh(mesh.devices.reshape(n_a, n_w, n_tp), ("a", "w", "tp"))
        cut = P(sp, "tp")
        return jax.shard_map(
            local,
            mesh=groups,
            in_specs=(cut, cut, cut, P(), P(), P("tp", None), P(sp, None), P(), P())
            + (cut, P("tp", sp), P(), P()),
            out_specs=cut,
            check_vma=False,
        )(queries, keys, *others)

    return layer
```

```python
import functools
import math

import jax
import jax.numpy as jnp
from jax import lax
from jax.experimental import pallas as pl
from jax.experimental.pallas import tpu as pltpu
from jax.sharding import Mesh, PartitionSpec as P

D = 2048
HEAD_SIZE = 64
GRID_W = 64


ALPHA = 8.0**0.25
ROTARY_BASE = 10000.0
RMS_EPSILON = 1e-06
NORM_EPSILON = 1e-05


def rotate_grid(heads_in, grid_places):
    half_dim = heads_in.shape[-1] // 2
    quarter = half_dim // 2
    inverse = ROTARY_BASE ** (-jnp.arange(quarter, dtype=jnp.float32) / quarter)

    def spin(segment, coords):
        angles = coords.astype(jnp.float32)[:, None] * inverse[None, :]
        cos_val = jnp.cos(angles)[:, None, :]
        sin_val = jnp.sin(angles)[:, None, :]
        lead_half = segment[..., :quarter]
        tail_half = segment[..., quarter:]
        return jnp.concatenate(
            [lead_half * cos_val - tail_half * sin_val, tail_half * cos_val + lead_half * sin_val],
            -1,
        )

    return jnp.concatenate(
        [
            spin(heads_in[..., :half_dim], grid_places // GRID_W),
            spin(heads_in[..., half_dim:], grid_places % GRID_W),
        ],
        -1,
    )


def prepare_inputs(heads_in, gain_vec, grid_places, factor):
    values32 = heads_in.astype(jnp.float32)
    normed = (
        values32
        * lax.rsqrt(jnp.mean(values32 * values32, -1, keepdims=True) + RMS_EPSILON)
        * gain_vec
    )
    return (rotate_grid(normed, grid_places) * factor).astype(jnp.bfloat16)


def layer_norm(pre_norm, gain_vec, bias_vec):
    row_mean = jnp.mean(pre_norm, -1, keepdims=True)
    centred = pre_norm - row_mean
    spread = jnp.mean(centred * centred, -1, keepdims=True)
    return centred * lax.rsqrt(spread + NORM_EPSILON) * gain_vec + bias_vec


def line_gather(block, axis):
    n, me = lax.axis_size(axis), lax.axis_index(axis)
    up = [(i, i + 1) for i in range(n - 1)]
    down = [(i + 1, i) for i in range(n - 1)]
    from_left, from_right = [block], [block]
    for _ in range(n - 1):
        from_left.append(lax.ppermute(from_left[-1], axis, up))
        from_right.append(lax.ppermute(from_right[-1], axis, down))
    stacked = jnp.zeros((n, *block.shape), block.dtype)
    for k in range(n):
        piece = block if k == 0 else jnp.where(me >= k, from_left[k], from_right[n - k])
        stacked = lax.dynamic_update_index_in_dim(stacked, piece, (me - k + n) % n, 0)
    return stacked


def swap_blocks(blocks, axis):
    n, me = lax.axis_size(axis), lax.axis_index(axis)
    stacked = jnp.zeros_like(blocks)
    for k in range(n):
        piece = lax.dynamic_index_in_dim(blocks, (me + k) % n, 0, keepdims=False)
        if k:
            piece = lax.ppermute(piece, axis, [(i, (i + k) % n) for i in range(n)])
        stacked = lax.dynamic_update_index_in_dim(stacked, piece, (me - k + n) % n, 0)
    return stacked


def turn_cols(block, outer, inner):
    width = block.shape[1] // (outer * inner)
    starts = [(o * inner + i) * width for i in range(inner) for o in range(outer)]
    return jnp.concatenate([block[:, c : c + width] for c in starts], -1)


def attend_kernel(chunk, q_ref, kv_ref, out_ref, vals_ref):
    width = 2 * HEAD_SIZE
    key_count = kv_ref.shape[0]
    rows = q_ref.shape[0]

    @pl.when(pl.program_id(1) == 0)
    def _():
        lane_kv = lax.broadcasted_iota(jnp.int32, (chunk, width), 1)

        @pl.loop(0, key_count // chunk)
        def _(c):
            at = pl.ds(pl.multiple_of(c * chunk, chunk), chunk)
            vals_ref[at, :] = jnp.where(
                lane_kv < HEAD_SIZE, 1.0, kv_ref[at, :].astype(jnp.float32)
            ).astype(jnp.bfloat16)

    lane = lax.broadcasted_iota(jnp.int32, (rows, width), 1)
    both = q_ref[...].astype(jnp.float32)
    results = []
    for head in range(2):
        own = both if head == 0 else pltpu.roll(both, HEAD_SIZE, 1)
        q = jnp.where(lane < HEAD_SIZE, own, 0.0).astype(jnp.bfloat16)
        top = None
        for c in range(key_count // chunk):
            at = pl.ds(c * chunk, chunk)
            scores = lax.dot_general(
                q, kv_ref[at, :], (((1,), (1,)), ((), ())), preferred_element_type=jnp.float32
            )
            peak = jnp.max(scores, -1, keepdims=True)
            new_top = peak if top is None else jnp.maximum(top, peak)
            weights = jnp.exp(scores - new_top).astype(jnp.bfloat16)
            part = jnp.dot(weights, vals_ref[at, :], preferred_element_type=jnp.float32)
            total = part if top is None else total * jnp.exp(top - new_top) + part
            top = new_top
        results.append(total)
    first, second = (t / pltpu.roll(t, HEAD_SIZE, 1) for t in results)
    out_ref[...] = jnp.where(
        lane < HEAD_SIZE, pltpu.roll(first, HEAD_SIZE, 1), second
    ).astype(jnp.bfloat16)


def attend(q, kv, block=256, chunk=2048):
    heads, rows, width = q.shape
    key_count = kv.shape[1]
    block, chunk = math.gcd(rows, block), math.gcd(key_count, chunk)
    return pl.pallas_call(
        functools.partial(attend_kernel, chunk),
        grid=(heads, rows // block),
        in_specs=[
            pl.BlockSpec((None, block, width), lambda h, i: (h, i, 0)),
            pl.BlockSpec((None, key_count, width), lambda h, i: (h, 0, 0)),
        ],
        out_specs=pl.BlockSpec((None, block, width), lambda h, i: (h, i, 0)),
        out_shape=jax.ShapeDtypeStruct(q.shape, jnp.bfloat16),
        scratch_shapes=[pltpu.VMEM((key_count, width), jnp.bfloat16)],
        compiler_params=pltpu.CompilerParams(dimension_semantics=("arbitrary", "arbitrary")),
        cost_estimate=pl.CostEstimate(
            flops=heads * rows * key_count * 16 * HEAD_SIZE,
            bytes_accessed=2 * (2 * q.size + kv.size),
            transcendentals=heads * rows * key_count * 2,
        ),
    )(q, kv)


def local(
    queries,
    keys,
    values,
    q_gain,
    key_norm_gain,
    out_weight,
    residual,
    ln1_gain,
    ln1_bias,
    up_weight,
    down_weight,
    ln2_gain,
    ln2_bias,
):
    tok_rows = queries.shape[0]
    n_a, n_tp = lax.axis_size("a"), lax.axis_size("tp")
    grid_places = lax.axis_index(("a", "w")) * tok_rows + jnp.arange(tok_rows, dtype=jnp.int32)
    kv_heads = keys.shape[1] // HEAD_SIZE
    q_count = queries.shape[1] // HEAD_SIZE
    own_heads = kv_heads // n_a
    query_rows = prepare_inputs(
        queries.reshape(tok_rows, q_count, HEAD_SIZE), q_gain, grid_places, HEAD_SIZE ** (-0.5)
    ).reshape(tok_rows, kv_heads, 2 * HEAD_SIZE)
    key_rows = prepare_inputs(
        keys.reshape(tok_rows, kv_heads, HEAD_SIZE), key_norm_gain, grid_places, 1.0
    )
    value_rows = values.reshape(tok_rows, kv_heads, HEAD_SIZE)
    packed = jnp.concatenate([query_rows, key_rows, value_rows], -1)
    packed = jnp.transpose(packed, (1, 0, 2)).reshape(n_a, own_heads, tok_rows, 4 * HEAD_SIZE)
    packed = lax.all_to_all(packed, "a", 0, 0, tiled=True)
    packed = jnp.transpose(packed, (1, 0, 2, 3)).reshape(
        own_heads, n_a * tok_rows, 4 * HEAD_SIZE
    )
    q = packed[..., : 2 * HEAD_SIZE]
    kv = lax.all_gather(packed[..., 2 * HEAD_SIZE :], "w", axis=1, tiled=True)
    kv, down_weight = lax.optimization_barrier((kv, down_weight))

    out_full = line_gather(out_weight, "tp").reshape(-1, D)
    up_own = lax.all_to_all(up_weight, "a", 1, 0, tiled=True)
    up_full = lax.all_gather(up_own, "w", axis=0, tiled=True)
    down_own = swap_blocks(down_weight.reshape(n_a, -1, down_weight.shape[1]), "a")
    down_own = down_own.swapaxes(0, 1).reshape(down_weight.shape[0] // n_a, -1)

    attended = attend(q, kv)
    rows = tok_rows // n_tp
    sent = attended.reshape(own_heads, n_a * n_tp, rows, 2 * HEAD_SIZE)
    sent = jnp.transpose(sent, (1, 0, 2, 3))
    got = lax.all_to_all(sent, ("a", "tp"), 0, 0, tiled=True)
    got, down_own = lax.optimization_barrier((got, down_own))
    down_full = lax.all_gather(down_own, "w", axis=0)
    got = got.reshape(n_a, n_tp, own_heads, rows, 2 * HEAD_SIZE)
    group_cols = jnp.transpose(got, (1, 3, 0, 2, 4)).reshape(n_tp, rows, -1)
    out_groups = out_full.reshape(2, -1, D)
    both = jnp.transpose(group_cols, (1, 0, 2)).reshape(rows, 2, -1)
    mixed = sum(
        jnp.dot(both[:, g], out_groups[g], preferred_element_type=jnp.float32)
        .astype(jnp.bfloat16)
        .astype(jnp.float32)
        for g in range(2)
    )
    own_residual = lax.dynamic_slice_in_dim(residual, lax.axis_index("tp") * rows, rows, 0)
    normed = layer_norm(
        ALPHA * own_residual.astype(jnp.float32) + mixed, ln1_gain, ln1_bias
    ).astype(jnp.bfloat16)
    n_w = lax.axis_size("w")
    turned = turn_cols(normed, n_a, n_w)
    full_rows = line_gather(line_gather(turned, "a"), "tp").reshape(-1, D)
    up_acts = jnp.dot(full_rows, up_full, preferred_element_type=jnp.float32)
    hidden = jnp.square(jnp.maximum(up_acts, 0.0)).astype(jnp.bfloat16)
    partial_ffn = jnp.concatenate(
        [
            jnp.dot(hidden, down_full[i], preferred_element_type=jnp.float32).astype(jnp.bfloat16)
            for i in range(down_full.shape[0])
        ],
        -1,
    )
    ffn_out = lax.psum_scatter(partial_ffn, "tp", scatter_dimension=0, tiled=True)
    ffn_out = lax.psum_scatter(ffn_out, "a", scatter_dimension=0, tiled=True)
    ffn_out = (
        ffn_out.reshape(rows, n_w, n_a, -1).swapaxes(1, 2).reshape(rows, D).astype(jnp.float32)
    )
    encoded = layer_norm(
        ALPHA * normed.astype(jnp.float32) + ffn_out, ln2_gain, ln2_bias
    ).astype(jnp.bfloat16)
    return lax.all_to_all(encoded, "tp", 1, 0, tiled=True)


MESH = pl.DeviceIdType.MESH
BF16, F32 = jnp.bfloat16, jnp.float32


def scaled(index, size):
    return pl.ds(pl.multiple_of(index * size, size), size)


def layer_kernel(
    n_a,
    n_w,
    q_all,
    k_all,
    v_all,
    q_gain,
    k_gain,
    up_own,
    down_own,
    out_own,
    res_all,
    gain1,
    bias1,
    gain2,
    bias2,
    out,
    q_own,
    kv_own,
    q_got,
    q_in,
    k_in,
    v_in,
    kv,
    vals,
    q_held,
    att_out,
    att_in,
    out_full,
    res,
    mixed,
    up,
    down,
    toks,
    hid,
    part,
    sib_out,
    sib_in,
    rs_out,
    rs_in,
    enc_out,
    loc_sem,
    q_s,
    q_r,
    side_s,
    side_r,
    kv_s,
    kv_r,
    att_s,
    att_r,
    wz_s,
    wz_r,
    wf_s,
    wf_r,
    wd_s,
    wd_r,
    tz_s,
    tz_r,
    pair_s,
    pair_r,
    sib_s,
    sib_r,
    rs_s,
    rs_r,
):
    place, core = lax.axis_index("sp"), lax.axis_index("tp")
    a, w = place // n_w, place % n_w
    other = 1 - core
    x_side = w + 1 - 2 * (w % 2)
    y_side = w + 2 - 4 * (w // 2)
    sides = (x_side, y_side)
    rows = toks.shape[2]
    tok_rows = 2 * rows
    width = 2 * HEAD_SIZE
    up_rows, up_cols = up_own.shape[0], up.shape[1]
    down_rows, down_cols = down.shape[0], down_own.shape[1]

    def at(a_, w_, core_):
        return (a_ * n_w + w_, core_)

    sibling = at(a, w, other)

    def remote(src, dst, send, recv, target):
        return pltpu.make_async_remote_copy(
            src_ref=src,
            dst_ref=dst,
            send_sem=send,
            recv_sem=recv,
            device_id=target,
            device_id_type=MESH,
        )

    def landed(dst, recv, send):
        remote(dst, dst, send, recv, sibling).wait_recv()

    def sent(src, send, recv):
        remote(src, src, send, recv, sibling).wait_send()

    def cyc(k):
        return lax.rem(a + k + 2 * n_a, n_a)

    turns = (0, 1, 2, 3)
    mates = [a, a + 1 - 2 * (a % 2), a + 2 - 4 * (a // 2), n_a - 1 - a]

    def mate(k):
        return mates[turns[k]]

    def turn(k):
        found = turns[0]
        for j in range(1, n_a):
            found = jnp.where(k == j, turns[j], found)
        return found

    def w_slot(kind, a_, w_):
        if kind == 0:
            return up.at[scaled(a_ * n_w + w_, up_rows), :]
        return down.at[:, scaled(a_ * n_w + w_, down_cols)]

    def w_half(kind, a_, w_, h):
        if kind == 0:
            half = up_rows // 2
            return up.at[scaled((a_ * n_w + w_) * 2 + h, half), :]
        half = down_rows // 2
        return down.at[pl.ds(h * half, half), scaled(a_ * n_w + w_, down_cols)]

    def w_src(kind, a_):
        if kind == 0:
            return up_own.at[:, scaled(a_, up_cols)]
        return down_own.at[scaled(a_, down_rows), :]

    def w_exchange(kind, to):
        remote(
            w_src(kind, to),
            w_slot(kind, a, w),
            wz_s.at[kind, to],
            wz_r.at[kind, a],
            at(to, w, core),
        ).start()

    def w_forward(kind, frm):
        for j in range(2):
            remote(
                w_slot(kind, frm, w),
                w_slot(kind, frm, w),
                wf_s.at[kind, frm, j],
                wf_r.at[kind, frm, j],
                at(a, sides[j], core),
            ).start()

    def w_arrive(kind, frm):
        landed(w_slot(kind, frm, w), wz_r.at[kind, frm], wz_s.at[kind, frm])

    def w_pass(kind, frm):
        w_arrive(kind, frm)
        w_forward(kind, frm)

    def w_corner(kind, frm):
        for j in range(2):
            landed(w_slot(kind, frm, sides[j]), wf_r.at[kind, frm, j], wf_s.at[kind, frm, j])
            part_ref = w_half(kind, frm, sides[j], j)
            remote(
                part_ref,
                part_ref,
                wd_s.at[kind, frm, j],
                wd_r.at[kind, frm, j],
                at(a, sides[1 - j], core),
            ).start()

    def w_finish(kind, frm):
        for j in range(2):
            landed(
                w_half(kind, frm, n_w - 1 - w, j), wd_r.at[kind, frm, j], wd_s.at[kind, frm, j]
            )

    def w_complete(kind):
        for k in range(n_a):
            w_finish(kind, mate(k))

    def w_drain(kind):
        for k in range(1, n_a):
            to = mate(k)
            sent(w_src(kind, to), wz_s.at[kind, to], wz_r.at[kind, to])
        for k in range(n_a):
            frm = mate(k)
            for j in range(2):
                sent(w_slot(kind, frm, w), wf_s.at[kind, frm, j], wf_r.at[kind, frm, j])
                sent(w_half(kind, frm, sides[j], j), wd_s.at[kind, frm, j], wd_r.at[kind, frm, j])

    entry_copies = [
        pltpu.make_async_copy(src, dst, loc_sem.at[4 + j])
        for j, (src, dst) in enumerate(((k_all, k_in), (v_all, v_in), (q_all, q_in)))
    ]
    for copy in entry_copies:
        copy.start()
    local_copies = [
        pltpu.make_async_copy(up_own.at[:, scaled(a, up_cols)], w_slot(0, a, w), loc_sem.at[0]),
        pltpu.make_async_copy(
            down_own.at[scaled(a, down_rows), :], w_slot(1, a, w), loc_sem.at[1]
        ),
        pltpu.make_async_copy(out_own, out_full.at[core], loc_sem.at[2]),
        pltpu.make_async_copy(res_all.at[scaled(core, rows), :], res, loc_sem.at[3]),
    ]
    for copy in local_copies:
        copy.start()

    barrier = pltpu.get_barrier_semaphore()
    w_peers = (x_side, y_side, n_w - 1 - w)
    peers = [at(cyc(k), w, core) for k in range(1, n_a)] + [sibling]
    peers += [at(a, side, core_) for side in w_peers for core_ in (core, other)]
    for peer in peers:
        pl.semaphore_signal(barrier, inc=1, device_id=peer, device_id_type=MESH)
    pl.semaphore_wait(barrier, len(peers))

    w_exchange(0, mate(1))
    remote(out_own, out_full.at[core], pair_s.at[0], pair_r.at[0], sibling).start()

    half_head, quarter = HEAD_SIZE // 2, HEAD_SIZE // 4
    lane = lax.broadcasted_iota(jnp.int32, (tok_rows, width), 1)
    token = lax.broadcasted_iota(jnp.int32, (tok_rows, width), 0) + place * tok_rows
    coord = jnp.where(lane % HEAD_SIZE < half_head, token // GRID_W, token % GRID_W)
    power = (lane % quarter).astype(F32) * (-math.log(ROTARY_BASE) / quarter)
    angle = coord.astype(F32) * jnp.exp(power)
    tail = lane % half_head >= quarter
    cos_val, sin_val = jnp.cos(angle), jnp.sin(angle)
    sin_val = jnp.where(tail, sin_val, -sin_val)
    first_head = lane < HEAD_SIZE

    def prepared(group, gain):
        squares = group * group
        low_sum = jnp.sum(jnp.where(first_head, squares, 0.0), -1, keepdims=True)
        high_sum = jnp.sum(jnp.where(first_head, 0.0, squares), -1, keepdims=True)
        mean = jnp.where(first_head, low_sum, high_sum) * (1.0 / HEAD_SIZE)
        unit = group * lax.rsqrt(mean + RMS_EPSILON) * gain
        partner = jnp.where(
            tail, pltpu.roll(unit, quarter, 1), pltpu.roll(unit, width - quarter, 1)
        )
        return unit * cos_val + partner * sin_val

    q_both, k_both = (jnp.concatenate([g[...], g[...]], -1) for g in (q_gain, k_gain))
    def kv_slot(b, w_):
        return kv.at[b, scaled(w_, tok_rows), :]

    entry_copies[0].wait()
    entry_copies[1].wait()
    for h in range(0, n_w, 2):
        cols = slice(h // 2 * width, (h // 2 + 1) * width)
        k_group = prepared(k_in[:, cols].astype(F32), k_both)
        v_group = v_in[:, cols].astype(F32)
        kv_own[h] = jnp.where(first_head, k_group, pltpu.roll(v_group, HEAD_SIZE, 1)).astype(BF16)
        kv_own[h + 1] = jnp.where(
            first_head, pltpu.roll(k_group, HEAD_SIZE, 1), v_group
        ).astype(BF16)
    for j, peer in enumerate(w_peers):
        remote(
            kv_own.at[peer], kv_slot(a, w), side_s.at[j], side_r.at[j], at(a, peer, core)
        ).start()
    kv[a, scaled(w, tok_rows), :] = kv_own[w]
    entry_copies[2].wait()
    for h in range(n_w):
        q_group = q_in[:, h * width : (h + 1) * width].astype(F32)
        q_own[h] = (prepared(q_group, q_both) * (HEAD_SIZE ** (-0.5))).astype(BF16)

    for j, peer in enumerate(w_peers):
        remote(q_own.at[peer], q_got.at[w], q_s.at[j], q_r.at[j], at(a, peer, core)).start()
    local_copies[0].wait()
    w_forward(0, a)
    local_copies[1].wait()
    w_forward(1, a)
    q_got[w] = q_own[w]

    last = n_a - 1
    low = jnp.minimum(a, last - a)
    toward = jnp.where(2 * a < n_a, 1, -1)

    def order(k):
        near = a + toward * jnp.where(k % 2 == 1, 1, -1) * ((k + 1) // 2)
        return jnp.where(k <= 2 * low, near, a + toward * (k - low))

    def kv_send(src, b, w_, dest, way):
        remote(
            src, kv_slot(b, w_), kv_s.at[b, w_, way], kv_r.at[b, w_], at(dest, w, core)
        ).start()

    for j, frm in enumerate((w, *w_peers)):
        if j:
            landed(kv_slot(a, frm), side_r.at[j - 1], side_s.at[j - 1])

        @pl.when(a < last)
        def _(frm=frm):
            kv_send(kv_slot(a, frm), a, frm, a + 1, 0)

        @pl.when(a > 0)
        def _(frm=frm):
            kv_send(kv_slot(a, frm), a, frm, a - 1, 1)

    def kv_relay(k):
        b = order(k)

        @pl.loop(0, n_w)
        def _(w_):
            landed(kv_slot(b, w_), kv_r.at[b, w_], kv_s.at[b, w_, 0])

            @pl.when((b > a) & (a > 0))
            def _():
                kv_send(kv_slot(b, w_), b, w_, a - 1, 1)

            @pl.when((b < a) & (a < last))
            def _():
                kv_send(kv_slot(b, w_), b, w_, a + 1, 0)

    w_exchange(0, mate(2))
    kv_relay(1)
    w_pass(0, mate(1))
    kv_relay(2)
    w_corner(0, a)
    kv_relay(3)
    w_exchange(0, mate(3))
    w_corner(1, a)
    w_pass(0, mate(2))
    for j, frm in enumerate((w, *w_peers)):
        if j:
            landed(q_got.at[frm], q_r.at[j - 1], q_s.at[j - 1])
        both = q_got[frm].astype(F32)
        for head in range(2):
            own = both if head == 0 else pltpu.roll(both, HEAD_SIZE, 1)
            q_held[frm, head] = jnp.where(first_head, own, 0.0).astype(BF16)

    @pl.loop(0, n_a)
    def _(b):
        @pl.loop(0, n_w)
        def _(w_):
            r = scaled(w_, tok_rows)
            vals[b, r, :] = jnp.where(first_head, 1.0, kv[b, r, :].astype(F32)).astype(BF16)

    chunks = 2
    per = n_a // chunks

    @pl.loop(0, n_w)
    def _(i):
        block = lax.rem(w + 1 + i, n_w)
        results = []
        for head in range(2):
            top = None
            for c in range(chunks):
                planes = pl.ds(c * per, per)
                scores = lax.dot_general(
                    q_held[block, head],
                    kv[planes].reshape(-1, width),
                    (((1,), (1,)), ((), ())),
                    preferred_element_type=F32,
                )
                peak = jnp.max(scores, -1, keepdims=True)
                new_top = peak if top is None else jnp.maximum(top, peak)
                weights = jnp.exp(scores - new_top).astype(BF16)
                add = jnp.dot(
                    weights, vals[planes].reshape(-1, width), preferred_element_type=F32
                )
                total = add if top is None else total * jnp.exp(top - new_top) + add
                top = new_top
            results.append(total)
        first, second = (t / pltpu.roll(t, HEAD_SIZE, 1) for t in results)
        att_out[block] = jnp.where(
            first_head, pltpu.roll(first, HEAD_SIZE, 1), second
        ).astype(BF16)
        mine = core * n_w + w
        remote(
            att_out.at[block, scaled(other, rows), :],
            att_in.at[mine],
            att_s.at[block, 0],
            att_r.at[mine],
            at(a, block, other),
        ).start()

        @pl.when(i < n_w - 1)
        def _():
            remote(
                att_out.at[block, scaled(core, rows), :],
                att_in.at[mine],
                att_s.at[block, 1],
                att_r.at[mine],
                at(a, block, core),
            ).start()

        @pl.when(i < n_a - 1)
        def _():
            w_exchange(1, jnp.where(i == 0, mate(1), jnp.where(i == 1, mate(2), mate(3))))

        @pl.when(i == 0)
        def _():
            w_corner(0, mate(1))

        @pl.when(i == 2)
        def _():
            w_corner(0, mate(2))

        @pl.when(i == 3)
        def _():
            w_pass(0, mate(3))


    att_in[core * n_w + w] = att_out[w, scaled(core, rows), :]
    local_copies[2].wait()
    local_copies[3].wait()
    landed(out_full.at[other], pair_r.at[0], pair_s.at[0])
    for core_ in (core, other):
        for frm in (w, *w_peers):
            if frm is w and core_ is core:
                continue
            frm_slot = core_ * n_w + frm
            landed(att_in.at[frm_slot], att_r.at[frm_slot], att_s.at[frm, 0])

    tile = 256

    @pl.loop(0, D // tile)
    def _(t):
        cols = scaled(t, tile)
        total = None
        for g in range(2):
            lhs = jnp.concatenate([att_in[g * n_w + k] for k in range(n_w)], -1)
            add = jnp.dot(lhs, out_full[g, :, cols], preferred_element_type=F32)
            add = add.astype(BF16).astype(F32)
            total = add if total is None else total + add
        mixed[:, cols] = total

    step = 32

    @pl.loop(0, rows // step)
    def _(t):
        r = scaled(t, step)
        toks[a, 0, r, :] = layer_norm(
            ALPHA * res[r, :].astype(F32) + mixed[r, :], gain1[...], bias1[...]
        ).astype(BF16)

    def tok_send(b, dest, way):
        remote(
            toks.at[b, 0], toks.at[b, 0], tz_s.at[b, way], tz_r.at[b], at(dest, w, core)
        ).start()

    def tok_pair(b):
        remote(toks.at[b, 0], toks.at[b, 1], pair_s.at[1 + b], pair_r.at[1 + b], sibling).start()

    @pl.when(a < last)
    def _():
        tok_send(a, a + 1, 0)

    @pl.when(a > 0)
    def _():
        tok_send(a, a - 1, 1)

    tok_pair(a)

    def relay(k):
        b = order(k)
        landed(toks.at[b, 0], tz_r.at[b], tz_s.at[b, 0])

        @pl.when((b > a) & (a > 0))
        def _():
            tok_send(b, a - 1, 1)

        @pl.when((b < a) & (a < last))
        def _():
            tok_send(b, a + 1, 0)

        tok_pair(b)

    def up_part(k):
        b = order(k)
        landed(toks.at[b, 1], pair_r.at[1 + b], pair_s.at[1 + b])

        @pl.loop(0, up_cols // tile)
        def _(t):
            cols = scaled(t, tile)
            acts = jnp.dot(
                toks[b].reshape(tok_rows, D), up[:, cols], preferred_element_type=F32
            )
            hid[b, :, cols] = jnp.square(jnp.maximum(acts, 0.0)).astype(BF16)

    groups = n_a
    g_cols = D // groups

    def piece(ref, g):
        return ref.at[:, scaled(g, g_cols)]

    def group_of(b, k):
        return jnp.where(b > a, turn(k), n_a - 1 - turn(k))

    def down_part(b, g):
        @pl.loop(0, g_cols // tile)
        def _(t):
            cols = scaled(g * (g_cols // tile) + t, tile)
            acts = jnp.dot(hid[b], down[:, cols], preferred_element_type=F32)
            part[b, :, cols] = acts[:rows]
            sib_out[b, :, cols] = acts[rows:].astype(BF16)

        remote(
            piece(sib_out.at[b], g),
            piece(sib_in.at[b], g),
            sib_s.at[b, g],
            sib_r.at[b, g],
            sibling,
        ).start()

    def pass_on(b, g):
        cols = scaled(g, g_cols)
        landed(piece(sib_in.at[b], g), sib_r.at[b, g], sib_s.at[b, g])

        carried = (low > 0) & (b != a + 2 * toward)

        @pl.when(carried)
        def _():
            landed(piece(rs_in.at[b], g), rs_r.at[b, g], rs_s.at[b, g])

        @pl.loop(0, rows // step)
        def _(t):
            r = scaled(t, step)
            total = part[b, r, cols] + sib_in[b, r, cols].astype(F32)
            total = jnp.where(carried, total + rs_in[b, r, cols].astype(F32), total)
            rs_out[b, r, cols] = total.astype(BF16)

        across = b == a + last * toward
        p = jnp.where(across, b, a + jnp.where(b > a, 1, -1))
        slot = jnp.where((b == p) & (p < a), n_a, b)
        slot = jnp.where(across, n_a + 1, slot)
        remote(
            piece(rs_out.at[b], g),
            piece(rs_in.at[slot], g),
            rs_s.at[b, g],
            rs_r.at[slot, g],
            at(p, w, core),
        ).start()

    def early(k):
        w_finish(1, mate(k))
        down_part(a + toward, mate(k))
        pass_on(a + toward, mate(k))

    w_pass(1, mate(1))
    w_pass(1, mate(2))
    w_corner(0, mate(3))
    w_corner(1, mate(1))
    w_complete(0)
    up_part(0)
    w_pass(1, mate(3))
    relay(1)

    @pl.when(low > 0)
    def _():
        relay(2)

    w_corner(1, mate(2))
    up_part(1)

    @pl.when(low == 0)
    def _():
        early(0)
        early(1)

    @pl.when(low > 0)
    def _():
        up_part(2)

    w_corner(1, mate(3))

    @pl.when(low == 0)
    def _():
        early(2)
        relay(2)
        up_part(2)
        early(3)

    @pl.when(low > 0)
    def _():
        relay(3)
        up_part(3)
        w_complete(1)

    def target(i):
        turn_ = i // groups
        b = a + jnp.where(turn_ == 0, 2, jnp.where(turn_ == 1, -1, 1)) * toward
        b = jnp.where(low > 0, b, a + toward * (2 + turn_))
        b = jnp.where(i < last * groups, b, a)
        return b, group_of(b, i % groups)

    def active(i):
        return (low > 0) | (i < 2 * groups) | (i >= last * groups)

    @pl.loop(0, n_a * groups + 1)
    def _(i):
        @pl.when((low == 0) & (i == groups))
        def _():
            relay(3)
            up_part(3)

        @pl.when((i < n_a * groups) & active(i))
        def _():
            down_part(*target(i))

        @pl.when((i > 0) & (i <= last * groups) & active(i - 1))
        def _():
            pass_on(*target(i - 1))

    for g in range(groups):
        landed(piece(sib_in.at[a], g), sib_r.at[a, g], sib_s.at[a, g])

        @pl.when(a > 0)
        def _(g=g):
            landed(piece(rs_in.at[a], g), rs_r.at[a, g], rs_s.at[a, g])

        @pl.when(a < last)
        def _(g=g):
            landed(piece(rs_in.at[n_a], g), rs_r.at[n_a, g], rs_s.at[a, g])

        @pl.when(low == 0)
        def _(g=g):
            landed(piece(rs_in.at[n_a + 1], g), rs_r.at[n_a + 1, g], rs_s.at[a, g])

    half = D // 2

    @pl.loop(0, rows // step)
    def _(t):
        r = scaled(t, step)
        total = part[a, r, :] + sib_in[a, r, :].astype(F32)
        total = jnp.where(a > 0, total + rs_in[a, r, :].astype(F32), total)
        total = jnp.where(a < last, total + rs_in[n_a, r, :].astype(F32), total)
        total = jnp.where(low == 0, total + rs_in[n_a + 1, r, :].astype(F32), total)
        encoded = layer_norm(
            ALPHA * toks[a, 0, r, :].astype(F32) + total, gain2[...], bias2[...]
        )
        left, right = encoded[:, :half].astype(BF16), encoded[:, half:].astype(BF16)
        out[pl.ds(pl.multiple_of(core * rows + t * step, step), step), :] = jnp.where(
            core == 0, left, right
        )
        enc_out[r, :] = jnp.where(core == 0, right, left)

    swap = remote(enc_out, out.at[scaled(core, rows), :], pair_s.at[n_a + 1], pair_r.at[n_a + 1], sibling)
    swap.start()
    for j, peer in enumerate(w_peers):
        sent(q_own.at[peer], q_s.at[j], q_r.at[j])
        sent(kv_own.at[peer], side_s.at[j], side_r.at[j])
        for core_way in range(2):
            sent(att_out.at[peer, pl.ds(0, rows), :], att_s.at[peer, core_way], att_r.at[peer])
    sent(att_out.at[w, pl.ds(0, rows), :], att_s.at[w, 0], att_r.at[w])
    sent(out_own, pair_s.at[0], pair_r.at[0])
    for kind in range(2):
        w_drain(kind)
    for k in range(n_a):
        b = cyc(k)
        if k:
            for g in range(groups):
                sent(piece(rs_out.at[b], g), rs_s.at[b, g], rs_r.at[b, g])
        for g in range(groups):
            sent(piece(sib_out.at[b], g), sib_s.at[b, g], sib_r.at[b, g])
        sent(toks.at[b, 0], pair_s.at[1 + b], pair_r.at[1 + b])

        @pl.when((a < last) & (b <= a))
        def _():
            for w_ in range(n_w):
                sent(kv_slot(b, w_), kv_s.at[b, w_, 0], kv_r.at[b, w_])
            sent(toks.at[b, 0], tz_s.at[b, 0], tz_r.at[b])

        @pl.when((a > 0) & (b >= a))
        def _():
            for w_ in range(n_w):
                sent(kv_slot(b, w_), kv_s.at[b, w_, 1], kv_r.at[b, w_])
            sent(toks.at[b, 0], tz_s.at[b, 1], tz_r.at[b])

    swap.wait_send()
    landed(out.at[scaled(other, rows), :], pair_r.at[n_a + 1], pair_s.at[n_a + 1])


def fused(n_a, n_w, *args):
    (queries, keys, values, q_gain, key_norm_gain, out_weight, residual, *rest) = args
    ln1_gain, ln1_bias, up_weight, down_weight, ln2_gain, ln2_bias = rest
    tok_rows = queries.shape[0]
    rows = tok_rows // 2
    width = 2 * HEAD_SIZE
    up_cols = up_weight.shape[1] // n_a
    down_rows = down_weight.shape[0] // n_a
    dma, vmem = pltpu.SemaphoreType.DMA, pltpu.VMEM
    whole, hbm = pl.BlockSpec(memory_space=pltpu.VMEM), pl.BlockSpec(memory_space=pl.ANY)
    return pl.pallas_call(
        functools.partial(layer_kernel, n_a, n_w),
        out_shape=jax.ShapeDtypeStruct((tok_rows, D // 2), BF16),
        in_specs=[hbm] * 3 + [whole] * 2 + [hbm] * 4 + [whole] * 4,
        out_specs=whole,
        scratch_shapes=[
            vmem((n_w, tok_rows, width), BF16),
            vmem((n_w, tok_rows, width), BF16),
            vmem((n_w, tok_rows, width), BF16),
            vmem(queries.shape, BF16),
            vmem(keys.shape, BF16),
            vmem(values.shape, BF16),
            vmem((n_a, n_w * tok_rows, width), BF16),
            vmem((n_a, n_w * tok_rows, width), BF16),
            vmem((n_w, 2, tok_rows, width), BF16),
            vmem((n_w, tok_rows, width), BF16),
            vmem((2 * n_w, rows, width), BF16),
            vmem((2, *out_weight.shape), BF16),
            vmem((rows, D), BF16),
            vmem((rows, D), F32),
            vmem((D, up_cols), BF16),
            vmem((down_rows, D), BF16),
            vmem((n_a, 2, rows, D), BF16),
            vmem((n_a, tok_rows, up_cols), BF16),
            vmem((n_a, rows, D), F32),
            vmem((n_a, rows, D), BF16),
            vmem((n_a, rows, D), BF16),
            vmem((n_a, rows, D), BF16),
            vmem((n_a + 2, rows, D), BF16),
            vmem((rows, D // 2), BF16),
            dma((7,)),
            dma((n_w - 1,)),
            dma((n_w - 1,)),
            dma((n_w - 1,)),
            dma((n_w - 1,)),
            dma((n_a, n_w, 2)),
            dma((n_a, n_w)),
            dma((n_w, 2)),
            dma((2 * n_w,)),
            dma((2, n_a)),
            dma((2, n_a)),
            dma((2, n_a, 2)),
            dma((2, n_a, 2)),
            dma((2, n_a, 2)),
            dma((2, n_a, 2)),
            dma((n_a, 2)),
            dma((n_a,)),
            dma((n_a + 2,)),
            dma((n_a + 2,)),
            dma((n_a, n_a)),
            dma((n_a, n_a)),
            dma((n_a, n_a)),
            dma((n_a + 2, n_a)),
        ],
        compiler_params=pltpu.CompilerParams(
            collective_id=0, has_side_effects=True, vmem_limit_bytes=60 * 2**20
        ),
    )(
        queries,
        keys,
        values,
        q_gain.reshape(1, HEAD_SIZE),
        key_norm_gain.reshape(1, HEAD_SIZE),
        up_weight,
        down_weight,
        out_weight,
        residual,
        *(v.reshape(1, D) for v in (ln1_gain, ln1_bias, ln2_gain, ln2_bias)),
    )


def solution(mesh):
    n_sp, n_tp = mesh.shape["sp"], mesh.shape["tp"]

    def layer(queries, keys, *others):
        n_a = math.gcd(n_sp, keys.shape[1] // (HEAD_SIZE * n_tp))
        n_w = n_sp // n_a
        sp = ("a", "w")
        if n_tp == 2 and n_w == n_a == 4 and keys.shape[1] == n_w * HEAD_SIZE * n_tp:
            cut = P("sp", "tp")
            return jax.shard_map(
                functools.partial(fused, n_a, n_w),
                mesh=mesh,
                in_specs=(cut, cut, cut, P(), P(), P("tp", None), P("sp", None), P(), P())
                + (cut, P("tp", "sp"), P(), P()),
                out_specs=cut,
                check_vma=False,
            )(queries, keys, *others)
        groups = Mesh(mesh.devices.reshape(n_a, n_w, n_tp), ("a", "w", "tp"))
        cut = P(sp, "tp")
        return jax.shard_map(
            local,
            mesh=groups,
            in_specs=(cut, cut, cut, P(), P(), P("tp", None), P(sp, None), P(), P())
            + (cut, P("tp", sp), P(), P()),
            out_specs=cut,
            check_vma=False,
        )(queries, keys, *others)

    return layer
```

```python
import functools
import math

import jax
import jax.numpy as jnp
from jax import lax
from jax.experimental import pallas as pl
from jax.experimental.pallas import tpu as pltpu
from jax.sharding import Mesh, PartitionSpec as P

D = 2048
HEAD_SIZE = 64
GRID_W = 64


ALPHA = 8.0**0.25
ROTARY_BASE = 10000.0
RMS_EPSILON = 1e-06
NORM_EPSILON = 1e-05


def rotate_grid(heads_in, grid_places):
    half_dim = heads_in.shape[-1] // 2
    quarter = half_dim // 2
    inverse = ROTARY_BASE ** (-jnp.arange(quarter, dtype=jnp.float32) / quarter)

    def spin(segment, coords):
        angles = coords.astype(jnp.float32)[:, None] * inverse[None, :]
        cos_val = jnp.cos(angles)[:, None, :]
        sin_val = jnp.sin(angles)[:, None, :]
        lead_half = segment[..., :quarter]
        tail_half = segment[..., quarter:]
        return jnp.concatenate(
            [lead_half * cos_val - tail_half * sin_val, tail_half * cos_val + lead_half * sin_val],
            -1,
        )

    return jnp.concatenate(
        [
            spin(heads_in[..., :half_dim], grid_places // GRID_W),
            spin(heads_in[..., half_dim:], grid_places % GRID_W),
        ],
        -1,
    )


def prepare_inputs(heads_in, gain_vec, grid_places, factor):
    values32 = heads_in.astype(jnp.float32)
    normed = (
        values32
        * lax.rsqrt(jnp.mean(values32 * values32, -1, keepdims=True) + RMS_EPSILON)
        * gain_vec
    )
    return (rotate_grid(normed, grid_places) * factor).astype(jnp.bfloat16)


def layer_norm(pre_norm, gain_vec, bias_vec):
    row_mean = jnp.mean(pre_norm, -1, keepdims=True)
    centred = pre_norm - row_mean
    spread = jnp.mean(centred * centred, -1, keepdims=True)
    return centred * lax.rsqrt(spread + NORM_EPSILON) * gain_vec + bias_vec


def line_gather(block, axis):
    n, me = lax.axis_size(axis), lax.axis_index(axis)
    up = [(i, i + 1) for i in range(n - 1)]
    down = [(i + 1, i) for i in range(n - 1)]
    from_left, from_right = [block], [block]
    for _ in range(n - 1):
        from_left.append(lax.ppermute(from_left[-1], axis, up))
        from_right.append(lax.ppermute(from_right[-1], axis, down))
    stacked = jnp.zeros((n, *block.shape), block.dtype)
    for k in range(n):
        piece = block if k == 0 else jnp.where(me >= k, from_left[k], from_right[n - k])
        stacked = lax.dynamic_update_index_in_dim(stacked, piece, (me - k + n) % n, 0)
    return stacked


def swap_blocks(blocks, axis):
    n, me = lax.axis_size(axis), lax.axis_index(axis)
    stacked = jnp.zeros_like(blocks)
    for k in range(n):
        piece = lax.dynamic_index_in_dim(blocks, (me + k) % n, 0, keepdims=False)
        if k:
            piece = lax.ppermute(piece, axis, [(i, (i + k) % n) for i in range(n)])
        stacked = lax.dynamic_update_index_in_dim(stacked, piece, (me - k + n) % n, 0)
    return stacked


def turn_cols(block, outer, inner):
    width = block.shape[1] // (outer * inner)
    starts = [(o * inner + i) * width for i in range(inner) for o in range(outer)]
    return jnp.concatenate([block[:, c : c + width] for c in starts], -1)


def attend_kernel(chunk, q_ref, kv_ref, out_ref, vals_ref):
    width = 2 * HEAD_SIZE
    key_count = kv_ref.shape[0]
    rows = q_ref.shape[0]

    @pl.when(pl.program_id(1) == 0)
    def _():
        lane_kv = lax.broadcasted_iota(jnp.int32, (chunk, width), 1)

        @pl.loop(0, key_count // chunk)
        def _(c):
            at = pl.ds(pl.multiple_of(c * chunk, chunk), chunk)
            vals_ref[at, :] = jnp.where(
                lane_kv < HEAD_SIZE, 1.0, kv_ref[at, :].astype(jnp.float32)
            ).astype(jnp.bfloat16)

    lane = lax.broadcasted_iota(jnp.int32, (rows, width), 1)
    both = q_ref[...].astype(jnp.float32)
    results = []
    for head in range(2):
        own = both if head == 0 else pltpu.roll(both, HEAD_SIZE, 1)
        q = jnp.where(lane < HEAD_SIZE, own, 0.0).astype(jnp.bfloat16)
        top = None
        for c in range(key_count // chunk):
            at = pl.ds(c * chunk, chunk)
            scores = lax.dot_general(
                q, kv_ref[at, :], (((1,), (1,)), ((), ())), preferred_element_type=jnp.float32
            )
            peak = jnp.max(scores, -1, keepdims=True)
            new_top = peak if top is None else jnp.maximum(top, peak)
            weights = jnp.exp(scores - new_top).astype(jnp.bfloat16)
            part = jnp.dot(weights, vals_ref[at, :], preferred_element_type=jnp.float32)
            total = part if top is None else total * jnp.exp(top - new_top) + part
            top = new_top
        results.append(total)
    first, second = (t / pltpu.roll(t, HEAD_SIZE, 1) for t in results)
    out_ref[...] = jnp.where(
        lane < HEAD_SIZE, pltpu.roll(first, HEAD_SIZE, 1), second
    ).astype(jnp.bfloat16)


def attend(q, kv, block=256, chunk=2048):
    heads, rows, width = q.shape
    key_count = kv.shape[1]
    block, chunk = math.gcd(rows, block), math.gcd(key_count, chunk)
    return pl.pallas_call(
        functools.partial(attend_kernel, chunk),
        grid=(heads, rows // block),
        in_specs=[
            pl.BlockSpec((None, block, width), lambda h, i: (h, i, 0)),
            pl.BlockSpec((None, key_count, width), lambda h, i: (h, 0, 0)),
        ],
        out_specs=pl.BlockSpec((None, block, width), lambda h, i: (h, i, 0)),
        out_shape=jax.ShapeDtypeStruct(q.shape, jnp.bfloat16),
        scratch_shapes=[pltpu.VMEM((key_count, width), jnp.bfloat16)],
        compiler_params=pltpu.CompilerParams(dimension_semantics=("arbitrary", "arbitrary")),
        cost_estimate=pl.CostEstimate(
            flops=heads * rows * key_count * 16 * HEAD_SIZE,
            bytes_accessed=2 * (2 * q.size + kv.size),
            transcendentals=heads * rows * key_count * 2,
        ),
    )(q, kv)


def local(
    queries,
    keys,
    values,
    q_gain,
    key_norm_gain,
    out_weight,
    residual,
    ln1_gain,
    ln1_bias,
    up_weight,
    down_weight,
    ln2_gain,
    ln2_bias,
):
    tok_rows = queries.shape[0]
    n_a, n_tp = lax.axis_size("a"), lax.axis_size("tp")
    grid_places = lax.axis_index(("a", "w")) * tok_rows + jnp.arange(tok_rows, dtype=jnp.int32)
    kv_heads = keys.shape[1] // HEAD_SIZE
    q_count = queries.shape[1] // HEAD_SIZE
    own_heads = kv_heads // n_a
    query_rows = prepare_inputs(
        queries.reshape(tok_rows, q_count, HEAD_SIZE), q_gain, grid_places, HEAD_SIZE ** (-0.5)
    ).reshape(tok_rows, kv_heads, 2 * HEAD_SIZE)
    key_rows = prepare_inputs(
        keys.reshape(tok_rows, kv_heads, HEAD_SIZE), key_norm_gain, grid_places, 1.0
    )
    value_rows = values.reshape(tok_rows, kv_heads, HEAD_SIZE)
    packed = jnp.concatenate([query_rows, key_rows, value_rows], -1)
    packed = jnp.transpose(packed, (1, 0, 2)).reshape(n_a, own_heads, tok_rows, 4 * HEAD_SIZE)
    packed = lax.all_to_all(packed, "a", 0, 0, tiled=True)
    packed = jnp.transpose(packed, (1, 0, 2, 3)).reshape(
        own_heads, n_a * tok_rows, 4 * HEAD_SIZE
    )
    q = packed[..., : 2 * HEAD_SIZE]
    kv = lax.all_gather(packed[..., 2 * HEAD_SIZE :], "w", axis=1, tiled=True)
    kv, down_weight = lax.optimization_barrier((kv, down_weight))

    out_full = line_gather(out_weight, "tp").reshape(-1, D)
    up_own = lax.all_to_all(up_weight, "a", 1, 0, tiled=True)
    up_full = lax.all_gather(up_own, "w", axis=0, tiled=True)
    down_own = swap_blocks(down_weight.reshape(n_a, -1, down_weight.shape[1]), "a")
    down_own = down_own.swapaxes(0, 1).reshape(down_weight.shape[0] // n_a, -1)

    attended = attend(q, kv)
    rows = tok_rows // n_tp
    sent = attended.reshape(own_heads, n_a * n_tp, rows, 2 * HEAD_SIZE)
    sent = jnp.transpose(sent, (1, 0, 2, 3))
    got = lax.all_to_all(sent, ("a", "tp"), 0, 0, tiled=True)
    got, down_own = lax.optimization_barrier((got, down_own))
    down_full = lax.all_gather(down_own, "w", axis=0)
    got = got.reshape(n_a, n_tp, own_heads, rows, 2 * HEAD_SIZE)
    group_cols = jnp.transpose(got, (1, 3, 0, 2, 4)).reshape(n_tp, rows, -1)
    out_groups = out_full.reshape(2, -1, D)
    both = jnp.transpose(group_cols, (1, 0, 2)).reshape(rows, 2, -1)
    mixed = sum(
        jnp.dot(both[:, g], out_groups[g], preferred_element_type=jnp.float32)
        .astype(jnp.bfloat16)
        .astype(jnp.float32)
        for g in range(2)
    )
    own_residual = lax.dynamic_slice_in_dim(residual, lax.axis_index("tp") * rows, rows, 0)
    normed = layer_norm(
        ALPHA * own_residual.astype(jnp.float32) + mixed, ln1_gain, ln1_bias
    ).astype(jnp.bfloat16)
    n_w = lax.axis_size("w")
    turned = turn_cols(normed, n_a, n_w)
    full_rows = line_gather(line_gather(turned, "a"), "tp").reshape(-1, D)
    up_acts = jnp.dot(full_rows, up_full, preferred_element_type=jnp.float32)
    hidden = jnp.square(jnp.maximum(up_acts, 0.0)).astype(jnp.bfloat16)
    partial_ffn = jnp.concatenate(
        [
            jnp.dot(hidden, down_full[i], preferred_element_type=jnp.float32).astype(jnp.bfloat16)
            for i in range(down_full.shape[0])
        ],
        -1,
    )
    ffn_out = lax.psum_scatter(partial_ffn, "tp", scatter_dimension=0, tiled=True)
    ffn_out = lax.psum_scatter(ffn_out, "a", scatter_dimension=0, tiled=True)
    ffn_out = (
        ffn_out.reshape(rows, n_w, n_a, -1).swapaxes(1, 2).reshape(rows, D).astype(jnp.float32)
    )
    encoded = layer_norm(
        ALPHA * normed.astype(jnp.float32) + ffn_out, ln2_gain, ln2_bias
    ).astype(jnp.bfloat16)
    return lax.all_to_all(encoded, "tp", 1, 0, tiled=True)


MESH = pl.DeviceIdType.MESH
BF16, F32 = jnp.bfloat16, jnp.float32


def scaled(index, size):
    return pl.ds(pl.multiple_of(index * size, size), size)


def layer_kernel(
    n_a,
    n_w,
    q_all,
    k_all,
    v_all,
    q_gain,
    k_gain,
    up_own,
    down_own,
    out_own,
    res_all,
    gain1,
    bias1,
    gain2,
    bias2,
    out,
    q_own,
    kv_own,
    q_got,
    q_in,
    k_in,
    v_in,
    kv,
    vals,
    q_held,
    att_out,
    att_in,
    out_full,
    res,
    mixed,
    up,
    down,
    toks,
    hid,
    part,
    sib_out,
    sib_in,
    rs_out,
    rs_in,
    enc_out,
    loc_sem,
    q_s,
    q_r,
    side_s,
    side_r,
    kv_s,
    kv_r,
    att_s,
    att_r,
    wz_s,
    wz_r,
    wf_s,
    wf_r,
    wd_s,
    wd_r,
    tz_s,
    tz_r,
    pair_s,
    pair_r,
    sib_s,
    sib_r,
    rs_s,
    rs_r,
):
    place, core = lax.axis_index("sp"), lax.axis_index("tp")
    a, w = place // n_w, place % n_w
    other = 1 - core
    x_side = w + 1 - 2 * (w % 2)
    y_side = w + 2 - 4 * (w // 2)
    sides = (x_side, y_side)
    rows = toks.shape[2]
    tok_rows = 2 * rows
    width = 2 * HEAD_SIZE
    up_rows, up_cols = up_own.shape[0], up.shape[1]
    down_rows, down_cols = down.shape[0], down_own.shape[1]

    def at(a_, w_, core_):
        return (a_ * n_w + w_, core_)

    sibling = at(a, w, other)

    def remote(src, dst, send, recv, target):
        return pltpu.make_async_remote_copy(
            src_ref=src,
            dst_ref=dst,
            send_sem=send,
            recv_sem=recv,
            device_id=target,
            device_id_type=MESH,
        )

    def landed(dst, recv, send):
        remote(dst, dst, send, recv, sibling).wait_recv()

    def sent(src, send, recv):
        remote(src, src, send, recv, sibling).wait_send()

    def cyc(k):
        return lax.rem(a + k + 2 * n_a, n_a)

    turns = (0, 1, 2, 3)
    mates = [a, a + 1 - 2 * (a % 2), a + 2 - 4 * (a // 2), n_a - 1 - a]

    def mate(k):
        return mates[turns[k]]

    def turn(k):
        found = turns[0]
        for j in range(1, n_a):
            found = jnp.where(k == j, turns[j], found)
        return found

    def w_slot(kind, a_, w_):
        if kind == 0:
            return up.at[scaled(a_ * n_w + w_, up_rows), :]
        return down.at[:, scaled(a_ * n_w + w_, down_cols)]

    def w_half(kind, a_, w_, h):
        if kind == 0:
            half = up_rows // 2
            return up.at[scaled((a_ * n_w + w_) * 2 + h, half), :]
        half = down_rows // 2
        return down.at[pl.ds(h * half, half), scaled(a_ * n_w + w_, down_cols)]

    def w_src(kind, a_):
        if kind == 0:
            return up_own.at[:, scaled(a_, up_cols)]
        return down_own.at[scaled(a_, down_rows), :]

    def w_exchange(kind, to):
        remote(
            w_src(kind, to),
            w_slot(kind, a, w),
            wz_s.at[kind, to],
            wz_r.at[kind, a],
            at(to, w, core),
        ).start()

    def w_forward(kind, frm):
        for j in range(2):
            remote(
                w_slot(kind, frm, w),
                w_slot(kind, frm, w),
                wf_s.at[kind, frm, j],
                wf_r.at[kind, frm, j],
                at(a, sides[j], core),
            ).start()

    def w_arrive(kind, frm):
        landed(w_slot(kind, frm, w), wz_r.at[kind, frm], wz_s.at[kind, frm])

    def w_pass(kind, frm):
        w_arrive(kind, frm)
        w_forward(kind, frm)

    def w_corner(kind, frm):
        for j in range(2):
            landed(w_slot(kind, frm, sides[j]), wf_r.at[kind, frm, j], wf_s.at[kind, frm, j])
            part_ref = w_half(kind, frm, sides[j], j)
            remote(
                part_ref,
                part_ref,
                wd_s.at[kind, frm, j],
                wd_r.at[kind, frm, j],
                at(a, sides[1 - j], core),
            ).start()

    def w_finish(kind, frm):
        for j in range(2):
            landed(
                w_half(kind, frm, n_w - 1 - w, j), wd_r.at[kind, frm, j], wd_s.at[kind, frm, j]
            )

    def w_complete(kind):
        for k in range(n_a):
            w_finish(kind, mate(k))

    def w_drain(kind):
        for k in range(1, n_a):
            to = mate(k)
            sent(w_src(kind, to), wz_s.at[kind, to], wz_r.at[kind, to])
        for k in range(n_a):
            frm = mate(k)
            for j in range(2):
                sent(w_slot(kind, frm, w), wf_s.at[kind, frm, j], wf_r.at[kind, frm, j])
                sent(w_half(kind, frm, sides[j], j), wd_s.at[kind, frm, j], wd_r.at[kind, frm, j])

    entry_copies = [
        pltpu.make_async_copy(src, dst, loc_sem.at[4 + j])
        for j, (src, dst) in enumerate(((k_all, k_in), (v_all, v_in), (q_all, q_in)))
    ]
    for copy in entry_copies:
        copy.start()
    local_copies = [
        pltpu.make_async_copy(up_own.at[:, scaled(a, up_cols)], w_slot(0, a, w), loc_sem.at[0]),
        pltpu.make_async_copy(
            down_own.at[scaled(a, down_rows), :], w_slot(1, a, w), loc_sem.at[1]
        ),
        pltpu.make_async_copy(out_own, out_full.at[core], loc_sem.at[2]),
        pltpu.make_async_copy(res_all.at[scaled(core, rows), :], res, loc_sem.at[3]),
    ]
    for copy in local_copies:
        copy.start()

    barrier = pltpu.get_barrier_semaphore()
    w_peers = (x_side, y_side, n_w - 1 - w)
    peers = [at(cyc(k), w, core) for k in range(1, n_a)] + [sibling]
    peers += [at(a, side, core_) for side in w_peers for core_ in (core, other)]
    for peer in peers:
        pl.semaphore_signal(barrier, inc=1, device_id=peer, device_id_type=MESH)
    pl.semaphore_wait(barrier, len(peers))

    w_exchange(0, mate(1))
    remote(out_own, out_full.at[core], pair_s.at[0], pair_r.at[0], sibling).start()

    half_head, quarter = HEAD_SIZE // 2, HEAD_SIZE // 4
    lane = lax.broadcasted_iota(jnp.int32, (tok_rows, width), 1)
    token = lax.broadcasted_iota(jnp.int32, (tok_rows, width), 0) + place * tok_rows
    coord = jnp.where(lane % HEAD_SIZE < half_head, token // GRID_W, token % GRID_W)
    power = (lane % quarter).astype(F32) * (-math.log(ROTARY_BASE) / quarter)
    angle = coord.astype(F32) * jnp.exp(power)
    tail = lane % half_head >= quarter
    cos_val, sin_val = jnp.cos(angle), jnp.sin(angle)
    sin_val = jnp.where(tail, sin_val, -sin_val)
    first_head = lane < HEAD_SIZE

    def prepared(group, gain):
        squares = group * group
        low_sum = jnp.sum(jnp.where(first_head, squares, 0.0), -1, keepdims=True)
        high_sum = jnp.sum(jnp.where(first_head, 0.0, squares), -1, keepdims=True)
        mean = jnp.where(first_head, low_sum, high_sum) * (1.0 / HEAD_SIZE)
        unit = group * lax.rsqrt(mean + RMS_EPSILON) * gain
        partner = jnp.where(
            tail, pltpu.roll(unit, quarter, 1), pltpu.roll(unit, width - quarter, 1)
        )
        return unit * cos_val + partner * sin_val

    q_both, k_both = (jnp.concatenate([g[...], g[...]], -1) for g in (q_gain, k_gain))
    def kv_slot(b, w_):
        return kv.at[b, scaled(w_, tok_rows), :]

    last = n_a - 1
    low = jnp.minimum(a, last - a)
    toward = jnp.where(2 * a < n_a, 1, -1)

    def kv_send(src, b, w_, dest, way):
        remote(
            src, kv_slot(b, w_), kv_s.at[b, w_, way], kv_r.at[b, w_], at(dest, w, core)
        ).start()

    def kv_out(frm):
        @pl.when(a < last)
        def _():
            kv_send(kv_slot(a, frm), a, frm, a + 1, 0)

        @pl.when(a > 0)
        def _():
            kv_send(kv_slot(a, frm), a, frm, a - 1, 1)

    entry_copies[0].wait()
    entry_copies[1].wait()
    for h in range(0, n_w, 2):
        cols = slice(h // 2 * width, (h // 2 + 1) * width)
        k_group = prepared(k_in[:, cols].astype(F32), k_both)
        v_group = v_in[:, cols].astype(F32)
        kv_own[h] = jnp.where(first_head, k_group, pltpu.roll(v_group, HEAD_SIZE, 1)).astype(BF16)
        kv_own[h + 1] = jnp.where(
            first_head, pltpu.roll(k_group, HEAD_SIZE, 1), v_group
        ).astype(BF16)
    for j, peer in enumerate(w_peers):
        remote(
            kv_own.at[peer], kv_slot(a, w), side_s.at[j], side_r.at[j], at(a, peer, core)
        ).start()
    kv[a, scaled(w, tok_rows), :] = kv_own[w]
    kv_out(w)
    entry_copies[2].wait()
    for h in range(n_w):
        q_group = q_in[:, h * width : (h + 1) * width].astype(F32)
        q_own[h] = (prepared(q_group, q_both) * (HEAD_SIZE ** (-0.5))).astype(BF16)

    for j, peer in enumerate(w_peers):
        remote(q_own.at[peer], q_got.at[w], q_s.at[j], q_r.at[j], at(a, peer, core)).start()
    local_copies[0].wait()
    w_forward(0, a)
    local_copies[1].wait()
    w_forward(1, a)
    q_got[w] = q_own[w]


    def order(k):
        near = a + toward * jnp.where(k % 2 == 1, 1, -1) * ((k + 1) // 2)
        return jnp.where(k <= 2 * low, near, a + toward * (k - low))

    for j, frm in enumerate(w_peers):
        landed(kv_slot(a, frm), side_r.at[j], side_s.at[j])
        kv_out(frm)

    def kv_relay(k):
        b = order(k)

        @pl.loop(0, n_w)
        def _(w_):
            landed(kv_slot(b, w_), kv_r.at[b, w_], kv_s.at[b, w_, 0])

            @pl.when((b > a) & (a > 0))
            def _():
                kv_send(kv_slot(b, w_), b, w_, a - 1, 1)

            @pl.when((b < a) & (a < last))
            def _():
                kv_send(kv_slot(b, w_), b, w_, a + 1, 0)

    w_exchange(0, mate(2))
    kv_relay(1)
    w_pass(0, mate(1))
    kv_relay(2)
    w_corner(0, a)
    kv_relay(3)
    w_exchange(0, mate(3))
    w_corner(1, a)
    w_pass(0, mate(2))
    for j, frm in enumerate((w, *w_peers)):
        if j:
            landed(q_got.at[frm], q_r.at[j - 1], q_s.at[j - 1])
        both = q_got[frm].astype(F32)
        for head in range(2):
            own = both if head == 0 else pltpu.roll(both, HEAD_SIZE, 1)
            q_held[frm, head] = jnp.where(first_head, own, 0.0).astype(BF16)

    @pl.loop(0, n_a)
    def _(b):
        @pl.loop(0, n_w)
        def _(w_):
            r = scaled(w_, tok_rows)
            vals[b, r, :] = jnp.where(first_head, 1.0, kv[b, r, :].astype(F32)).astype(BF16)

    chunks = 2
    per = n_a // chunks

    @pl.loop(0, n_w)
    def _(i):
        block = lax.rem(w + 1 + i, n_w)
        results = []
        for head in range(2):
            top = None
            for c in range(chunks):
                planes = pl.ds(c * per, per)
                scores = lax.dot_general(
                    q_held[block, head],
                    kv[planes].reshape(-1, width),
                    (((1,), (1,)), ((), ())),
                    preferred_element_type=F32,
                )
                peak = jnp.max(scores, -1, keepdims=True)
                new_top = peak if top is None else jnp.maximum(top, peak)
                weights = jnp.exp(scores - new_top).astype(BF16)
                add = jnp.dot(
                    weights, vals[planes].reshape(-1, width), preferred_element_type=F32
                )
                total = add if top is None else total * jnp.exp(top - new_top) + add
                top = new_top
            results.append(total)
        first, second = (t / pltpu.roll(t, HEAD_SIZE, 1) for t in results)
        att_out[block] = jnp.where(
            first_head, pltpu.roll(first, HEAD_SIZE, 1), second
        ).astype(BF16)
        mine = core * n_w + w
        remote(
            att_out.at[block, scaled(other, rows), :],
            att_in.at[mine],
            att_s.at[block, 0],
            att_r.at[mine],
            at(a, block, other),
        ).start()

        @pl.when(i < n_w - 1)
        def _():
            remote(
                att_out.at[block, scaled(core, rows), :],
                att_in.at[mine],
                att_s.at[block, 1],
                att_r.at[mine],
                at(a, block, core),
            ).start()

        @pl.when(i < n_a - 1)
        def _():
            w_exchange(1, jnp.where(i == 0, mate(1), jnp.where(i == 1, mate(2), mate(3))))

        @pl.when(i == 0)
        def _():
            w_corner(0, mate(1))

        @pl.when(i == 2)
        def _():
            w_corner(0, mate(2))

        @pl.when(i == 3)
        def _():
            w_pass(0, mate(3))


    att_in[core * n_w + w] = att_out[w, scaled(core, rows), :]
    local_copies[2].wait()
    local_copies[3].wait()
    landed(out_full.at[other], pair_r.at[0], pair_s.at[0])
    for core_ in (core, other):
        for frm in (w, *w_peers):
            if frm is w and core_ is core:
                continue
            frm_slot = core_ * n_w + frm
            landed(att_in.at[frm_slot], att_r.at[frm_slot], att_s.at[frm, 0])

    tile = 256

    @pl.loop(0, D // tile)
    def _(t):
        cols = scaled(t, tile)
        total = None
        for g in range(2):
            lhs = jnp.concatenate([att_in[g * n_w + k] for k in range(n_w)], -1)
            add = jnp.dot(lhs, out_full[g, :, cols], preferred_element_type=F32)
            add = add.astype(BF16).astype(F32)
            total = add if total is None else total + add
        mixed[:, cols] = total

    step = 32

    @pl.loop(0, rows // step)
    def _(t):
        r = scaled(t, step)
        toks[a, 0, r, :] = layer_norm(
            ALPHA * res[r, :].astype(F32) + mixed[r, :], gain1[...], bias1[...]
        ).astype(BF16)

    def tok_send(b, dest, way):
        remote(
            toks.at[b, 0], toks.at[b, 0], tz_s.at[b, way], tz_r.at[b], at(dest, w, core)
        ).start()

    def tok_pair(b):
        remote(toks.at[b, 0], toks.at[b, 1], pair_s.at[1 + b], pair_r.at[1 + b], sibling).start()

    @pl.when(a < last)
    def _():
        tok_send(a, a + 1, 0)

    @pl.when(a > 0)
    def _():
        tok_send(a, a - 1, 1)

    tok_pair(a)

    def relay(k):
        b = order(k)
        landed(toks.at[b, 0], tz_r.at[b], tz_s.at[b, 0])

        @pl.when((b > a) & (a > 0))
        def _():
            tok_send(b, a - 1, 1)

        @pl.when((b < a) & (a < last))
        def _():
            tok_send(b, a + 1, 0)

        tok_pair(b)

    def up_part(k):
        b = order(k)
        landed(toks.at[b, 1], pair_r.at[1 + b], pair_s.at[1 + b])

        @pl.loop(0, up_cols // tile)
        def _(t):
            cols = scaled(t, tile)
            acts = jnp.dot(
                toks[b].reshape(tok_rows, D), up[:, cols], preferred_element_type=F32
            )
            hid[b, :, cols] = jnp.square(jnp.maximum(acts, 0.0)).astype(BF16)

    groups = n_a
    g_cols = D // groups

    def piece(ref, g):
        return ref.at[:, scaled(g, g_cols)]

    def group_of(b, k):
        return jnp.where(b > a, turn(k), n_a - 1 - turn(k))

    def down_part(b, g):
        @pl.loop(0, g_cols // tile)
        def _(t):
            cols = scaled(g * (g_cols // tile) + t, tile)
            acts = jnp.dot(hid[b], down[:, cols], preferred_element_type=F32)
            part[b, :, cols] = acts[:rows]
            sib_out[b, :, cols] = acts[rows:].astype(BF16)

        remote(
            piece(sib_out.at[b], g),
            piece(sib_in.at[b], g),
            sib_s.at[b, g],
            sib_r.at[b, g],
            sibling,
        ).start()

    def pass_on(b, g):
        cols = scaled(g, g_cols)
        landed(piece(sib_in.at[b], g), sib_r.at[b, g], sib_s.at[b, g])

        carried = (low > 0) & (b != a + 2 * toward)

        @pl.when(carried)
        def _():
            landed(piece(rs_in.at[b], g), rs_r.at[b, g], rs_s.at[b, g])

        @pl.loop(0, rows // step)
        def _(t):
            r = scaled(t, step)
            total = part[b, r, cols] + sib_in[b, r, cols].astype(F32)
            total = jnp.where(carried, total + rs_in[b, r, cols].astype(F32), total)
            rs_out[b, r, cols] = total.astype(BF16)

        across = b == a + last * toward
        p = jnp.where(across, b, a + jnp.where(b > a, 1, -1))
        slot = jnp.where((b == p) & (p < a), n_a, b)
        slot = jnp.where(across, n_a + 1, slot)
        remote(
            piece(rs_out.at[b], g),
            piece(rs_in.at[slot], g),
            rs_s.at[b, g],
            rs_r.at[slot, g],
            at(p, w, core),
        ).start()

    def early(k):
        w_finish(1, mate(k))
        down_part(a + toward, mate(k))
        pass_on(a + toward, mate(k))

    w_pass(1, mate(1))
    w_pass(1, mate(2))
    w_corner(0, mate(3))
    w_corner(1, mate(1))
    w_complete(0)
    up_part(0)
    w_pass(1, mate(3))
    relay(1)

    @pl.when(low > 0)
    def _():
        relay(2)

    w_corner(1, mate(2))
    up_part(1)

    @pl.when(low == 0)
    def _():
        early(0)
        early(1)

    @pl.when(low > 0)
    def _():
        up_part(2)

    w_corner(1, mate(3))

    @pl.when(low == 0)
    def _():
        early(2)
        relay(2)
        up_part(2)
        early(3)

    @pl.when(low > 0)
    def _():
        relay(3)
        up_part(3)
        w_complete(1)

    def target(i):
        turn_ = i // groups
        b = a + jnp.where(turn_ == 0, 2, jnp.where(turn_ == 1, -1, 1)) * toward
        b = jnp.where(low > 0, b, a + toward * (2 + turn_))
        b = jnp.where(i < last * groups, b, a)
        return b, group_of(b, i % groups)

    def active(i):
        return (low > 0) | (i < 2 * groups) | (i >= last * groups)

    @pl.loop(0, n_a * groups + 1)
    def _(i):
        @pl.when((low == 0) & (i == groups))
        def _():
            relay(3)
            up_part(3)

        @pl.when((i < n_a * groups) & active(i))
        def _():
            down_part(*target(i))

        @pl.when((i > 0) & (i <= last * groups) & active(i - 1))
        def _():
            pass_on(*target(i - 1))

    for g in range(groups):
        landed(piece(sib_in.at[a], g), sib_r.at[a, g], sib_s.at[a, g])

        @pl.when(a > 0)
        def _(g=g):
            landed(piece(rs_in.at[a], g), rs_r.at[a, g], rs_s.at[a, g])

        @pl.when(a < last)
        def _(g=g):
            landed(piece(rs_in.at[n_a], g), rs_r.at[n_a, g], rs_s.at[a, g])

        @pl.when(low == 0)
        def _(g=g):
            landed(piece(rs_in.at[n_a + 1], g), rs_r.at[n_a + 1, g], rs_s.at[a, g])

    half = D // 2

    @pl.loop(0, rows // step)
    def _(t):
        r = scaled(t, step)
        total = part[a, r, :] + sib_in[a, r, :].astype(F32)
        total = jnp.where(a > 0, total + rs_in[a, r, :].astype(F32), total)
        total = jnp.where(a < last, total + rs_in[n_a, r, :].astype(F32), total)
        total = jnp.where(low == 0, total + rs_in[n_a + 1, r, :].astype(F32), total)
        encoded = layer_norm(
            ALPHA * toks[a, 0, r, :].astype(F32) + total, gain2[...], bias2[...]
        )
        left, right = encoded[:, :half].astype(BF16), encoded[:, half:].astype(BF16)
        out[pl.ds(pl.multiple_of(core * rows + t * step, step), step), :] = jnp.where(
            core == 0, left, right
        )
        enc_out[r, :] = jnp.where(core == 0, right, left)

    swap = remote(enc_out, out.at[scaled(core, rows), :], pair_s.at[n_a + 1], pair_r.at[n_a + 1], sibling)
    swap.start()
    for j, peer in enumerate(w_peers):
        sent(q_own.at[peer], q_s.at[j], q_r.at[j])
        sent(kv_own.at[peer], side_s.at[j], side_r.at[j])
        for core_way in range(2):
            sent(att_out.at[peer, pl.ds(0, rows), :], att_s.at[peer, core_way], att_r.at[peer])
    sent(att_out.at[w, pl.ds(0, rows), :], att_s.at[w, 0], att_r.at[w])
    sent(out_own, pair_s.at[0], pair_r.at[0])
    for kind in range(2):
        w_drain(kind)
    for k in range(n_a):
        b = cyc(k)
        if k:
            for g in range(groups):
                sent(piece(rs_out.at[b], g), rs_s.at[b, g], rs_r.at[b, g])
        for g in range(groups):
            sent(piece(sib_out.at[b], g), sib_s.at[b, g], sib_r.at[b, g])
        sent(toks.at[b, 0], pair_s.at[1 + b], pair_r.at[1 + b])

        @pl.when((a < last) & (b <= a))
        def _():
            for w_ in range(n_w):
                sent(kv_slot(b, w_), kv_s.at[b, w_, 0], kv_r.at[b, w_])
            sent(toks.at[b, 0], tz_s.at[b, 0], tz_r.at[b])

        @pl.when((a > 0) & (b >= a))
        def _():
            for w_ in range(n_w):
                sent(kv_slot(b, w_), kv_s.at[b, w_, 1], kv_r.at[b, w_])
            sent(toks.at[b, 0], tz_s.at[b, 1], tz_r.at[b])

    swap.wait_send()
    landed(out.at[scaled(other, rows), :], pair_r.at[n_a + 1], pair_s.at[n_a + 1])


def fused(n_a, n_w, *args):
    (queries, keys, values, q_gain, key_norm_gain, out_weight, residual, *rest) = args
    ln1_gain, ln1_bias, up_weight, down_weight, ln2_gain, ln2_bias = rest
    tok_rows = queries.shape[0]
    rows = tok_rows // 2
    width = 2 * HEAD_SIZE
    up_cols = up_weight.shape[1] // n_a
    down_rows = down_weight.shape[0] // n_a
    dma, vmem = pltpu.SemaphoreType.DMA, pltpu.VMEM
    whole, hbm = pl.BlockSpec(memory_space=pltpu.VMEM), pl.BlockSpec(memory_space=pl.ANY)
    return pl.pallas_call(
        functools.partial(layer_kernel, n_a, n_w),
        out_shape=jax.ShapeDtypeStruct((tok_rows, D // 2), BF16),
        in_specs=[hbm] * 3 + [whole] * 2 + [hbm] * 4 + [whole] * 4,
        out_specs=whole,
        scratch_shapes=[
            vmem((n_w, tok_rows, width), BF16),
            vmem((n_w, tok_rows, width), BF16),
            vmem((n_w, tok_rows, width), BF16),
            vmem(queries.shape, BF16),
            vmem(keys.shape, BF16),
            vmem(values.shape, BF16),
            vmem((n_a, n_w * tok_rows, width), BF16),
            vmem((n_a, n_w * tok_rows, width), BF16),
            vmem((n_w, 2, tok_rows, width), BF16),
            vmem((n_w, tok_rows, width), BF16),
            vmem((2 * n_w, rows, width), BF16),
            vmem((2, *out_weight.shape), BF16),
            vmem((rows, D), BF16),
            vmem((rows, D), F32),
            vmem((D, up_cols), BF16),
            vmem((down_rows, D), BF16),
            vmem((n_a, 2, rows, D), BF16),
            vmem((n_a, tok_rows, up_cols), BF16),
            vmem((n_a, rows, D), F32),
            vmem((n_a, rows, D), BF16),
            vmem((n_a, rows, D), BF16),
            vmem((n_a, rows, D), BF16),
            vmem((n_a + 2, rows, D), BF16),
            vmem((rows, D // 2), BF16),
            dma((7,)),
            dma((n_w - 1,)),
            dma((n_w - 1,)),
            dma((n_w - 1,)),
            dma((n_w - 1,)),
            dma((n_a, n_w, 2)),
            dma((n_a, n_w)),
            dma((n_w, 2)),
            dma((2 * n_w,)),
            dma((2, n_a)),
            dma((2, n_a)),
            dma((2, n_a, 2)),
            dma((2, n_a, 2)),
            dma((2, n_a, 2)),
            dma((2, n_a, 2)),
            dma((n_a, 2)),
            dma((n_a,)),
            dma((n_a + 2,)),
            dma((n_a + 2,)),
            dma((n_a, n_a)),
            dma((n_a, n_a)),
            dma((n_a, n_a)),
            dma((n_a + 2, n_a)),
        ],
        compiler_params=pltpu.CompilerParams(
            collective_id=0, has_side_effects=True, vmem_limit_bytes=60 * 2**20
        ),
    )(
        queries,
        keys,
        values,
        q_gain.reshape(1, HEAD_SIZE),
        key_norm_gain.reshape(1, HEAD_SIZE),
        up_weight,
        down_weight,
        out_weight,
        residual,
        *(v.reshape(1, D) for v in (ln1_gain, ln1_bias, ln2_gain, ln2_bias)),
    )


def solution(mesh):
    n_sp, n_tp = mesh.shape["sp"], mesh.shape["tp"]

    def layer(queries, keys, *others):
        n_a = math.gcd(n_sp, keys.shape[1] // (HEAD_SIZE * n_tp))
        n_w = n_sp // n_a
        sp = ("a", "w")
        if n_tp == 2 and n_w == n_a == 4 and keys.shape[1] == n_w * HEAD_SIZE * n_tp:
            cut = P("sp", "tp")
            return jax.shard_map(
                functools.partial(fused, n_a, n_w),
                mesh=mesh,
                in_specs=(cut, cut, cut, P(), P(), P("tp", None), P("sp", None), P(), P())
                + (cut, P("tp", "sp"), P(), P()),
                out_specs=cut,
                check_vma=False,
            )(queries, keys, *others)
        groups = Mesh(mesh.devices.reshape(n_a, n_w, n_tp), ("a", "w", "tp"))
        cut = P(sp, "tp")
        return jax.shard_map(
            local,
            mesh=groups,
            in_specs=(cut, cut, cut, P(), P(), P("tp", None), P(sp, None), P(), P())
            + (cut, P("tp", sp), P(), P()),
            out_specs=cut,
            check_vma=False,
        )(queries, keys, *others)

    return layer
```
